32 devices in a mesh: sp: 8 (over z, x), tp: 4 (over y, core).
Axes of the slice: x: 2, y: 2, z: 4, core: 2. Of those that a mesh axis runs over, the one named last changes fastest.
Arguments:
- tokens: bfloat16 [8192, 2048], P('sp', 'tp'), may hold values from -70 to 70
- w_query: bfloat16 [2048, 1024], P(None, 'tp'), may hold values from -0.125 to 0.125
- w_key: bfloat16 [2048, 1024], P(None, 'tp'), may hold values from -0.125 to 0.125
- w_value: bfloat16 [2048, 1024], P(None, 'tp'), may hold values from -0.125 to 0.125
- w_delta_gate: bfloat16 [2048, 1024], P(None, 'tp'), may hold values from -0.125 to 0.125
- w_glu_value: bfloat16 [2048, 1024], P(None, 'tp'), may hold values from -0.125 to 0.125
- w_glu_gate: bfloat16 [2048, 1024], P(None, 'tp'), may hold values from -0.125 to 0.125
- w_conv_gate: bfloat16 [2048, 1024], P(None, 'tp'), may hold values from -0.125 to 0.125
- w_beta: bfloat16 [2048, 8], replicated, may hold values from -0.125 to 0.125
- w_decay: bfloat16 [2048, 8], replicated, may hold values from -0.125 to 0.125
- decay_log: float32 [8], replicated, may hold values from -12 to -3
- head_gain: float32 [128], replicated, may hold values from 0.1 to 1.9
- conv_taps: bfloat16 [31, 1024], P(None, 'tp'), may hold values from -2.5 to 2.5
- ln_gain: float32 [1024], P('tp'), may hold values from 0.1 to 1.9
- ln_shift: float32 [1024], P('tp'), may hold values from -3 to 3
- out_delta: bfloat16 [1024, 2048], P('tp'), may hold values from -0.125 to 0.125
- out_conv: bfloat16 [1024, 2048], P('tp'), may hold values from -0.125 to 0.125
Outputs:
- mixed_out: bfloat16 [8192, 2048], P(('sp', 'tp'))
The draws below stay inside these ranges and needn't reach their ends.
All inputs are finite; a program needn't handle non-finite values.
Results may differ from the reference program's by a relative error of at most 0.024.
Values may be sent and summed in bfloat16 or wider, within the bound.
A program may use at most 64 MiB of HBM per device.

```python
import jax
import jax.numpy as jnp
from jax import lax

D = 2048
HEADS = 8
DK = 128
CV = 1024
KERNEL = 31
SPAN = 64
TOKENS = 8192
N_TP = 4


def draw_tokens(key, part):
    keys = jax.random.split(key, 3)
    span_rows = 4 * SPAN
    groups = (TOKENS + span_rows - 1) // span_rows
    shifts = jnp.clip(jax.random.normal(keys[1], (groups, D), jnp.float32), -6.0, 6.0) * 1.5
    shifts = jnp.repeat(shifts, span_rows, axis=0)[:TOKENS]
    noise = jnp.clip(jax.random.normal(keys[0], (TOKENS, D), jnp.float32), -6.0, 6.0)
    spread = 0.7
    scales = jnp.exp(jax.random.uniform(keys[2], (TOKENS, 1), jnp.float32, -spread, spread))
    return ((noise + shifts) * scales).astype(jnp.bfloat16)


def draw_decay_log(key, part):
    keys = jax.random.split(key, 3)
    order = jax.random.permutation(keys[0], HEADS)
    fast_heads = HEADS // 2
    slow_rate = jax.random.uniform(keys[1], (HEADS,), jnp.float32, 0.3, 1.0) * 2.3 / TOKENS
    fast_rate = jax.random.uniform(keys[2], (HEADS,), jnp.float32, 0.015, 0.04)
    return jnp.log(jnp.where(order < fast_heads, fast_rate, slow_rate)).astype(jnp.float32)


def draw_conv_taps(key, part):
    keys = jax.random.split(key, 2)
    noise = jnp.clip(jax.random.normal(keys[0], (KERNEL, CV), jnp.float32), -4.0, 4.0)
    spread = 1.2
    levels = jnp.exp(jax.random.uniform(keys[1], (16,), jnp.float32, -spread, spread))
    group_ids = jnp.arange(CV) * 16 // CV
    column_scale = jnp.take(levels, group_ids)
    return (noise * column_scale[None, :] * KERNEL ** (-0.5)).astype(jnp.bfloat16)


def level_of(key, shape, shards, smallest, high):
    def one(axis_at, shards_of):
        heights = jax.random.uniform(jax.random.fold_in(jax.random.fold_in(key, 6), axis_at), (shards_of,), jnp.float32, smallest / len(shards), high / len(shards))
        return jnp.repeat(jnp.exp(heights), shape[axis_at] // shards_of).reshape((-1,) + (1,) * (len(shape) - axis_at - 1))

    loudness = one(*shards[0])
    for cut in shards[1:]:
        loudness = loudness * one(*cut)
    return loudness


def gaussian(own_key, shape, scale, reach, shards=(), kind=jnp.bfloat16):
    entries = scale * jax.random.normal(own_key, shape, jnp.float32)
    if shards:
        entries = entries * level_of(own_key, shape, shards, -0.22, 0.18)
    return jnp.clip(entries, -reach, reach).astype(kind)


def setup_inputs(seed: int = 0) -> dict:
    splits = jax.random.split(jax.random.key(seed), 18)
    tokens = draw_tokens(jax.random.fold_in(splits[17], 71), 0)
    w_query = gaussian(splits[1], (D, HEADS * DK), D ** -0.5, 0.125, ((1, 4),))
    w_key = gaussian(splits[2], (D, HEADS * DK), D ** -0.5, 0.125, ((1, 4),))
    w_value = gaussian(splits[3], (D, HEADS * DK), D ** -0.5, 0.125, ((1, 4),))
    w_delta_gate = gaussian(splits[4], (D, HEADS * DK), D ** -0.5, 0.125, ((1, 4),))
    w_glu_value = gaussian(splits[5], (D, CV), D ** -0.5, 0.125, ((1, 4),))
    w_glu_gate = gaussian(splits[6], (D, CV), D ** -0.5, 0.125, ((1, 4),))
    w_conv_gate = gaussian(splits[7], (D, CV), D ** -0.5, 0.125, ((1, 4),))
    w_beta = gaussian(splits[8], (D, HEADS), D ** -0.5, 0.125)
    w_decay = gaussian(splits[9], (D, HEADS), D ** -0.5, 0.125)
    decay_log = draw_decay_log(jax.random.fold_in(splits[17], 71), 0)
    head_gain = jnp.clip(1.0 + 0.18 * jax.random.normal(splits[11], (DK,), jnp.float32), 0.1, 1.9)
    conv_taps = draw_conv_taps(jax.random.fold_in(splits[17], 71), 0)
    ln_gain = jnp.clip(1.0 + 0.18 * jax.random.normal(splits[13], (CV,), jnp.float32), 0.1, 1.9)
    ln_shift = gaussian(splits[14], (CV,), 0.5, 3.0, ((0, 4),), jnp.float32)
    out_delta = gaussian(splits[15], (HEADS * DK, D), (HEADS * DK + CV) ** -0.5, 0.125, ((0, 4),))
    out_conv = gaussian(splits[16], (CV, D), (HEADS * DK + CV) ** -0.5, 0.125, ((0, 4),))
    return {"tokens": tokens, "w_query": w_query, "w_key": w_key, "w_value": w_value, "w_delta_gate": w_delta_gate, "w_glu_value": w_glu_value, "w_glu_gate": w_glu_gate, "w_conv_gate": w_conv_gate, "w_beta": w_beta, "w_decay": w_decay, "decay_log": decay_log, "head_gain": head_gain, "conv_taps": conv_taps, "ln_gain": ln_gain, "ln_shift": ln_shift, "out_delta": out_delta, "out_conv": out_conv}


TINY_NORM = 1e-06
TINY_VAR = 1e-05
HIGHEST = lax.Precision.HIGHEST

def head_rule(query, keys, values, strength, log_decay):
    blocks = query.shape[0] // SPAN

    def split_blocks(array):
        return array.reshape((blocks, SPAN) + array.shape[1:])
    query, keys, values = (split_blocks(query), split_blocks(keys), split_blocks(values))
    strength, log_decay = (split_blocks(strength), split_blocks(log_decay))
    log_sum = jnp.cumsum(log_decay, axis=-1)
    offsets = jnp.arange(SPAN)
    causal = offsets[:, None] >= offsets[None, :]
    strict = offsets[:, None] > offsets[None, :]
    spread = log_sum[:, :, None] - log_sum[:, None, :]
    damping = jnp.where(causal, jnp.exp(jnp.where(causal, spread, 0.0)), 0.0)
    scaled_keys = keys * strength[..., None]
    lower = jnp.where(strict, jnp.einsum('nid,njd->nij', scaled_keys, keys, precision=HIGHEST) * damping, 0.0)
    identity = jnp.eye(SPAN, dtype=jnp.float32)
    right = jnp.concatenate([values * strength[..., None], scaled_keys * jnp.exp(log_sum)[..., None]], axis=-1)
    solved = jax.scipy.linalg.solve_triangular(identity + lower, right, lower=True, unit_diagonal=True)
    width = values.shape[-1]
    corrected = solved[..., :width]
    key_terms = solved[..., width:]
    scores = jnp.einsum('nid,njd->nij', query, keys, precision=HIGHEST) * damping

    def advance(memory, inputs):
        query_block, keys_block, corrected_block, terms_block, scores_block, log_block = inputs
        fresh = corrected_block - jnp.dot(terms_block, memory, precision=HIGHEST)
        output = jnp.dot(query_block * jnp.exp(log_block)[:, None], memory, precision=HIGHEST)
        output = output + jnp.dot(scores_block, fresh, precision=HIGHEST)
        tail_log = log_block[-1]
        weighted = keys_block * jnp.exp(tail_log - log_block)[:, None]
        memory = memory * jnp.exp(tail_log) + jnp.dot(weighted.T, fresh, precision=HIGHEST)
        return (memory, output)
    start = jnp.zeros((keys.shape[-1], width), jnp.float32)
    ignored, outputs = lax.scan(advance, start, (query, keys, corrected, key_terms, scores, log_sum))
    return outputs.reshape(blocks * SPAN, width)

def reference(tokens, w_query, w_key, w_value, w_delta_gate, w_glu_value, w_glu_gate, w_conv_gate, w_beta, w_decay, decay_log, head_gain, conv_taps, ln_gain, ln_shift, out_delta, out_conv):
    length = tokens.shape[0]
    floats = tokens.astype(jnp.float32)
    inv_rms = lax.rsqrt(lax.optimization_barrier(jnp.mean(floats * floats, axis=1, keepdims=True)) + TINY_NORM)

    def project(weight):
        return jnp.dot(tokens.astype(jnp.float32), weight.astype(jnp.float32), preferred_element_type=jnp.float32) * inv_rms
    query_raw = project(w_query).astype(jnp.bfloat16)
    key_raw = project(w_key).astype(jnp.bfloat16)
    value_raw = project(w_value).astype(jnp.bfloat16)
    delta_gate_raw = project(w_delta_gate).astype(jnp.bfloat16)
    glu_value_raw = project(w_glu_value).astype(jnp.bfloat16)
    glu_gate_raw = project(w_glu_gate).astype(jnp.bfloat16)
    conv_gate_raw = project(w_conv_gate).astype(jnp.bfloat16)
    strength = jax.nn.sigmoid(project(w_beta))
    log_decay = -jnp.exp(decay_log)[None, :] * jax.nn.softplus(project(w_decay))

    def to_heads(raw):
        return raw.astype(jnp.float32).reshape(length, HEADS, DK)

    def unit_rows(array):
        return array * lax.rsqrt(lax.optimization_barrier(jnp.sum(array * array, axis=-1, keepdims=True)) + TINY_NORM)
    query = unit_rows(to_heads(query_raw)) * DK ** (-0.5)
    keys = unit_rows(to_heads(key_raw))
    values = to_heads(value_raw)
    heads_out = lax.map(lambda inputs: head_rule(*inputs), (jnp.moveaxis(query, 1, 0), jnp.moveaxis(keys, 1, 0), jnp.moveaxis(values, 1, 0), strength.T, log_decay.T))
    output = jnp.moveaxis(heads_out, 0, 1)
    output = output * lax.rsqrt(lax.optimization_barrier(jnp.mean(output * output, axis=-1, keepdims=True)) + TINY_NORM) * head_gain
    delta_mixed = (output.reshape(length, HEADS * DK) * jax.nn.silu(delta_gate_raw.astype(jnp.float32))).astype(jnp.bfloat16)
    gated_units = (glu_value_raw.astype(jnp.float32) * jax.nn.sigmoid(glu_gate_raw.astype(jnp.float32))).astype(jnp.bfloat16)
    padded = jnp.concatenate([jnp.zeros((KERNEL - 1, CV), jnp.bfloat16), gated_units], axis=0)
    filtered = jnp.zeros((length, CV), jnp.float32)
    for offset in range(KERNEL):
        filtered = filtered + padded[offset:offset + length].astype(jnp.float32) * conv_taps[offset].astype(jnp.float32)
    center = lax.optimization_barrier(jnp.sum(filtered, axis=1)) / CV
    variance = jnp.maximum(lax.optimization_barrier(jnp.sum(filtered * filtered, axis=1)) / CV - center * center, 0.0)
    normed = (filtered - center[:, None]) * lax.rsqrt(variance + TINY_VAR)[:, None] * ln_gain + ln_shift
    conv_mixed = (jax.nn.silu(normed) * jax.nn.silu(conv_gate_raw.astype(jnp.float32))).astype(jnp.bfloat16)
    head_block = HEADS * DK // N_TP
    chan_block = CV // N_TP
    summed = jnp.zeros((length, D), jnp.float32)
    for group in range(N_TP):
        partial_value = jnp.dot(delta_mixed[:, group * head_block:(group + 1) * head_block].astype(jnp.float32), out_delta[group * head_block:(group + 1) * head_block].astype(jnp.float32), preferred_element_type=jnp.float32)
        partial_value = partial_value + jnp.dot(conv_mixed[:, group * chan_block:(group + 1) * chan_block].astype(jnp.float32), out_conv[group * chan_block:(group + 1) * chan_block].astype(jnp.float32), preferred_element_type=jnp.float32)
        partial_value = lax.optimization_barrier(partial_value.astype(jnp.bfloat16))
        summed = summed + partial_value.astype(jnp.float32)
    return summed.astype(jnp.bfloat16)
```

```python
import functools

import jax
import jax.numpy as jnp
from jax import lax
from jax.experimental import pallas as pl
from jax.experimental.pallas import tpu as pltpu
from jax.sharding import PartitionSpec as P

BLOCK = 128
CHUNKS = 8
TOGETHER = 8
CUTS = 8


TINY_NORM = 1e-06
TINY_VAR = 1e-05
HIGHEST = lax.Precision.HIGHEST


def nt(a, b):
    return lax.dot_general(a, b, (((1,), (1,)), ((), ())), preferred_element_type=jnp.float32)


def mm(a, b):
    return jnp.dot(
        a.astype(jnp.bfloat16), b.astype(jnp.bfloat16), preferred_element_type=jnp.float32
    )


def delta_kernel(
    heads, width, q_ref, k_ref, v_ref, g_ref, outa_ref, outb_ref, final_ref,
    lhs_s, corr_s, score_s, wt_s, tail_s, state_ref,
):
    rows = q_ref.shape[0]
    blocks = rows // BLOCK
    row_id = lax.broadcasted_iota(jnp.int32, (BLOCK, BLOCK), 0)
    col_id = lax.broadcasted_iota(jnp.int32, (BLOCK, BLOCK), 1)
    causal = row_id >= col_id
    strict = row_id > col_id
    differ = row_id ^ col_id
    eye = jnp.where(row_id == col_id, 1.0, 0.0)
    tril = jnp.where(causal, 1.0, 0.0)

    def prepare(c):
        at = pl.ds(pl.multiple_of(c * BLOCK, BLOCK), BLOCK)
        gates = g_ref[at, :]
        sums = jnp.dot(tril, gates, precision=HIGHEST, preferred_element_type=jnp.float32)
        chains = []
        for h in range(heads):
            lanes = slice(h * width, (h + 1) * width)
            k, q = k_ref[at, lanes], q_ref[at, lanes]
            v = v_ref[at, lanes].astype(jnp.float32)
            kf, qf = k.astype(jnp.float32), q.astype(jnp.float32)
            ik = lax.rsqrt(jnp.sum(kf * kf, axis=-1, keepdims=True) + TINY_NORM)
            iq = lax.rsqrt(jnp.sum(qf * qf, axis=-1, keepdims=True) + TINY_NORM)
            iq = iq * width ** (-0.5)
            beta = gates[:, h : h + 1]
            log_sum = sums[:, heads + h : heads + h + 1]
            log_full = jnp.broadcast_to(log_sum, (BLOCK, BLOCK))
            spread = log_full - log_full.T
            damp = jnp.where(causal, jnp.exp(jnp.where(causal, spread, 0.0)), 0.0)
            damp = damp * jnp.broadcast_to(ik, (BLOCK, BLOCK)).T
            lower = jnp.where(strict, nt(k, k) * damp * (beta * ik), 0.0)
            score_s[h, at, :] = (nt(q, k) * damp * iq).astype(jnp.bfloat16)
            grow = jnp.exp(log_sum)
            right = jnp.concatenate([v * beta, kf * (beta * ik * grow)], axis=1)
            tail = log_full[BLOCK - 1 : BLOCK, :]
            weighted = kf * (ik * jnp.exp(tail[:, :1] - log_sum))
            wt_s[h, c] = weighted.T.astype(jnp.bfloat16)
            tail_s[h, c] = jnp.broadcast_to(jnp.exp(tail), (8, BLOCK))
            lhs_s[h, c, BLOCK:, :] = (qf * (iq * grow)).astype(jnp.bfloat16)
            chains.append([h, lower, right, eye - jnp.where(differ == 1, lower, 0.0)])
        return at, c, chains

    def pair(p, carry):
        prepared = [prepare(p * TOGETHER + i) for i in range(TOGETHER)]
        size = 2
        while size < BLOCK:
            level = (differ >= size) & (differ < 2 * size)
            parts = [
                [mm(jnp.where(level, ch[1], 0.0), ch[3]) for ch in item[2]] for item in prepared
            ]
            for item, part in zip(prepared, parts):
                for ch, moved in zip(item[2], part):
                    ch[3] = ch[3] - mm(ch[3], moved)
            size *= 2
        for at, c, chains in prepared:
            for h, lower, right, inverse in chains:
                solved = mm(inverse, right)
                corr_s[h, at, :] = solved[:, :width]
                lhs_s[h, c, :BLOCK, :] = solved[:, width:].astype(jnp.bfloat16)
        return carry

    lax.fori_loop(0, blocks // TOGETHER, pair, 0)
    for h in range(heads):
        state_ref[h] = jnp.concatenate([eye, jnp.zeros((width, width), jnp.float32)], axis=1)

    def advance(c, carry):
        at = pl.ds(pl.multiple_of(c * BLOCK, BLOCK), BLOCK)
        boths = [mm(lhs_s[h, c], state_ref[h]) for h in range(heads)]
        fresh = []
        for h in range(heads):
            first = boths[h][:BLOCK]
            fresh.append(
                jnp.concatenate(
                    [-first[:, :width], corr_s[h, at, :] - first[:, width:]], axis=1
                ).astype(jnp.bfloat16)
            )
        for h in range(heads):
            decay = tail_s[h, c][:1, :]
            decay = jnp.concatenate([decay, decay], axis=1)
            state_ref[h] = state_ref[h] * decay + mm(wt_s[h, c], fresh[h])
        for h in range(heads):
            out = boths[h][BLOCK:] + mm(score_s[h, at, :], fresh[h])
            outa_ref[h, at, :] = out[:, :width].astype(jnp.bfloat16)
            outb_ref[h, at, :] = out[:, width:]
        return carry

    lax.fori_loop(0, blocks, advance, 0)
    final_ref[...] = state_ref[...].astype(jnp.bfloat16)


def delta_rule(query_raw, key_raw, value_raw, gates, heads, width):
    rows = query_raw.shape[0]
    blocks = rows // BLOCK
    vm = pl.BlockSpec(memory_space=pltpu.VMEM)
    return pl.pallas_call(
        functools.partial(delta_kernel, heads, width),
        out_shape=(
            jax.ShapeDtypeStruct((heads, rows, width), jnp.bfloat16),
            jax.ShapeDtypeStruct((heads, rows, width), jnp.float32),
            jax.ShapeDtypeStruct((heads, width, 2 * width), jnp.bfloat16),
        ),
        in_specs=[vm] * 4,
        out_specs=(vm, vm, vm),
        scratch_shapes=[
            pltpu.VMEM((heads, blocks, 2 * BLOCK, width), jnp.bfloat16),
            pltpu.VMEM((heads, rows, width), jnp.float32),
            pltpu.VMEM((heads, rows, BLOCK), jnp.bfloat16),
            pltpu.VMEM((heads, blocks, width, BLOCK), jnp.bfloat16),
            pltpu.VMEM((heads, blocks, 8, BLOCK), jnp.float32),
            pltpu.VMEM((heads, width, 2 * width), jnp.float32),
        ],
        compiler_params=pltpu.CompilerParams(
            vmem_limit_bytes=40 * 1024 * 1024
        ),
        cost_estimate=pl.CostEstimate(
            flops=10_000_000_000, bytes_accessed=4_000_000, transcendentals=0
        ),
        name="delta_rule",
    )(query_raw, key_raw, value_raw, gates)


MESH = pl.DeviceIdType.MESH


def sharded_place():
    tp = lax.axis_size("tp")
    me = lax.axis_index("tp")
    core = lax.rem(me, 2)
    return tp // 2, me, core, me // 2, me + 1 - 2 * core


def greet(chips, core, chip, sibling):
    barrier = pltpu.get_barrier_semaphore()
    pl.semaphore_signal(barrier, inc=1, device_id={"tp": sibling}, device_id_type=MESH)
    for o in range(1, chips):
        there = lax.rem(chip + o, chips) * 2 + core
        pl.semaphore_signal(barrier, inc=1, device_id={"tp": there}, device_id_type=MESH)
    pl.semaphore_wait(barrier, chips)


def project_kernel(heads, *refs):
    count = 7
    tok_ref, far_refs, wg_ref, rate_ref = refs[0], refs[1 : 1 + count], refs[8], refs[9]
    out_refs, gates_ref = refs[10 : 10 + count], refs[17]
    full, y_send, y_recv, own_send, own_recv, fwd_send, fwd_recv, w_sem = refs[18:26]
    w_refs = refs[26:]
    rows, part = tok_ref.shape
    step = rows // CHUNKS
    chips, me, core, chip, sibling = sharded_place()

    def columns(owner):
        return pl.ds(pl.multiple_of(owner * part, part), part)

    def at(r):
        return pl.ds(pl.multiple_of(r * step, step), step)

    def across(o, r):
        there = lax.rem(chip + o, chips) * 2 + core
        return pltpu.make_async_remote_copy(
            src_ref=tok_ref.at[at(r), :],
            dst_ref=full.at[at(r), columns(me)],
            send_sem=y_send.at[o - 1, r],
            recv_sem=y_recv.at[o - 1, r],
            device_id={"tp": there},
            device_id_type=MESH,
        )

    def beside(r):
        return pltpu.make_async_remote_copy(
            src_ref=tok_ref.at[at(r), :],
            dst_ref=full.at[at(r), columns(me)],
            send_sem=own_send.at[r],
            recv_sem=own_recv.at[r],
            device_id={"tp": sibling},
            device_id_type=MESH,
        )

    def forward(o, r):
        owner = lax.rem(chip - o + chips, chips) * 2 + core
        block = full.at[at(r), columns(owner)]
        return pltpu.make_async_remote_copy(
            src_ref=block,
            dst_ref=block,
            send_sem=fwd_send.at[o - 1, r],
            recv_sem=fwd_recv.at[o - 1, r],
            device_id={"tp": sibling},
            device_id_type=MESH,
        )

    greet(chips, core, chip, sibling)
    for r in range(CHUNKS):
        for o in range(1, chips):
            across(o, r).start()
    loads = [
        pltpu.make_async_copy(far, w_ref, w_sem.at[i])
        for i, (far, w_ref) in enumerate(zip(far_refs, w_refs))
    ]
    for load in loads:
        load.start()
    for r in range(CHUNKS):
        beside(r).start()
    full[:, columns(me)] = tok_ref[...]

    def chunk(first, pieces, carry):
        for i in range(pieces):
            for o in range(1, chips):
                across(o, first + i).wait_recv()
                forward(o, first + i).start()
        for i in range(pieces):
            beside(first + i).wait_recv()
            for o in range(1, chips):
                forward(o, first + i).wait_recv()
        size = step * pieces
        here = pl.ds(pl.multiple_of(first * step, step), size)
        squares = jnp.zeros((size, 1), jnp.float32)
        for b in range(2 * chips):
            piece = full[here, b * part : (b + 1) * part].astype(jnp.float32)
            squares = squares + jnp.sum(piece * piece, axis=1, keepdims=True)
        inv_rms = lax.rsqrt(squares / (part * 2 * chips) + TINY_NORM)
        for w_ref, out_ref in zip(w_refs, out_refs):
            summed = jnp.dot(full[here, :], w_ref[...], preferred_element_type=jnp.float32)
            out_ref[here, :] = (summed * inv_rms).astype(jnp.bfloat16)
        raw = jnp.dot(full[here, :], wg_ref[...], preferred_element_type=jnp.float32) * inv_rms
        lane = lax.broadcasted_iota(jnp.int32, raw.shape, 1)
        softplus = jnp.maximum(raw, 0.0) + jnp.log1p(jnp.exp(-jnp.abs(raw)))
        gates_ref[here, :] = jnp.where(lane < heads, jax.nn.sigmoid(raw), -rate_ref[...] * softplus)
        return carry

    for load in loads:
        load.wait()
    paired = CHUNKS // 2 - 1
    lax.fori_loop(0, paired, lambda r, carry: chunk(2 * r, 2, carry), 0)
    lax.fori_loop(2 * paired, CHUNKS, lambda r, carry: chunk(r, 1, carry), 0)
    for r in range(CHUNKS):
        for o in range(1, chips):
            across(o, r).wait_send()
            forward(o, r).wait_send()
        beside(r).wait_send()


def project(tokens, weights, w_gates, rates, heads):
    rows, part = tokens.shape
    tp = lax.axis_size("tp")
    others = max(tp // 2 - 1, 1)
    vm = pl.BlockSpec(memory_space=pltpu.VMEM)
    dma = pltpu.SemaphoreType.DMA
    return pl.pallas_call(
        functools.partial(project_kernel, heads),
        out_shape=tuple(
            jax.ShapeDtypeStruct((rows, w.shape[1]), jnp.bfloat16) for w in weights
        )
        + (jax.ShapeDtypeStruct((rows, w_gates.shape[1]), jnp.float32),),
        in_specs=[vm] + [pl.BlockSpec(memory_space=pl.ANY)] * len(weights) + [vm] * 2,
        out_specs=(vm,) * (1 + len(weights)),
        scratch_shapes=[
            pltpu.VMEM((rows, part * tp), jnp.bfloat16),
            dma((others, CHUNKS)),
            dma((others, CHUNKS)),
            dma((CHUNKS,)),
            dma((CHUNKS,)),
            dma((others, CHUNKS)),
            dma((others, CHUNKS)),
            dma((len(weights),)),
        ]
        + [pltpu.VMEM(w.shape, w.dtype) for w in weights],
        compiler_params=pltpu.CompilerParams(
            collective_id=0, has_side_effects=True, vmem_limit_bytes=48 * 1024 * 1024
        ),
        cost_estimate=pl.CostEstimate(
            flops=10_000_000_000, bytes_accessed=20_000_000, transcendentals=0
        ),
        name="gather_project",
    )(tokens, *weights, w_gates, rates)


def middle_kernel(
    heads, width, final_ref, gv_ref, gg_ref, cg_ref, taps_ref, ln_gain_ref, ln_shift_ref,
    outa_ref, outb_ref, dg_ref, gain_ref, mixed_ref, conv_ref,
    padded, filtered, halo_out, halo_in, sums_out, sums_in, window_s, sent_s, far_s,
    far_send, far_recv, halo_send, halo_recv, ln_send, ln_recv,
):
    rows = gv_ref.shape[0]
    halo = halo_in.shape[0]
    lanes = padded.shape[2]
    groups = padded.shape[0]
    kernel = taps_ref.shape[0]
    tiles = rows // BLOCK
    sp, place = lax.axis_size("sp"), lax.axis_index("sp")
    tp, me = lax.axis_size("tp"), lax.axis_index("tp")
    reaches = [1]
    while 2 * reaches[-1] < sp:
        reaches.append(2 * reaches[-1])
    last = len(reaches) - 1
    barrier = pltpu.get_barrier_semaphore()
    expected = tp - 1
    for step in reaches:
        ahead, behind = place + step < sp, place >= step

        @pl.when(ahead)
        def _(step=step):
            pl.semaphore_signal(
                barrier, inc=1, device_id={"sp": place + step}, device_id_type=MESH
            )

        @pl.when(behind)
        def _(step=step):
            pl.semaphore_signal(
                barrier, inc=1, device_id={"sp": place - step}, device_id_type=MESH
            )

        expected = expected + ahead.astype(jnp.int32) + behind.astype(jnp.int32)
    for step in range(1, tp):
        pl.semaphore_signal(
            barrier, inc=1, device_id={"tp": lax.rem(me + step, tp)}, device_id_type=MESH
        )
    pl.semaphore_wait(barrier, expected)

    def onward(src, dst, send, recv, step):
        return pltpu.make_async_remote_copy(
            src_ref=src,
            dst_ref=dst,
            send_sem=send,
            recv_sem=recv,
            device_id={"sp": jnp.minimum(place + step, sp - 1)},
            device_id_type=MESH,
        )

    def carry_copy(i, h):
        cut = slice(width, 2 * width) if i == last else slice(0, 2 * width)
        source = final_ref if i == 0 else sent_s.at[i - 1]
        return onward(
            source.at[h, :, cut], far_s.at[i, h, :, cut],
            far_send.at[i, h], far_recv.at[i, h], reaches[i],
        )

    def send_carry(i, h):
        @pl.when(place + reaches[i] < sp)
        def _():
            carry_copy(i, h).start()

    def take_carry(i, h):
        @pl.when(place >= reaches[i])
        def _():
            carry_copy(i, h).wait_recv()

        @pl.when(place < reaches[i])
        def _():
            far_s[i, h] = jnp.zeros((width, 2 * width), jnp.bfloat16)

    def combine(later, earlier):
        moved = mm(later[:, :width], earlier)
        return jnp.concatenate(
            [moved[:, :width], moved[:, width:] + later[:, width:].astype(jnp.float32)], axis=1
        )

    def exchange(i):
        for h in range(heads):
            take_carry(i, h)
            own = final_ref[h] if i == 0 else sent_s[i - 1, h]
            sent_s[i, h] = combine(own, far_s[i, h]).astype(jnp.bfloat16)
            send_carry(i + 1, h)
        for h in range(heads):
            if i == 0:
                window_s[h] = far_s[i, h].astype(jnp.float32)
            else:
                window_s[h] = combine(window_s[h], far_s[i, h])

    for h in range(heads):
        send_carry(0, h)

    def at(t):
        return pl.ds(pl.multiple_of(t * BLOCK, BLOCK), BLOCK)

    def unit(t, carry):
        value = gv_ref[at(t), :].astype(jnp.float32)
        units = (value * jax.nn.sigmoid(gg_ref[at(t), :].astype(jnp.float32))).astype(jnp.bfloat16)
        wide = units.astype(jnp.float32)
        for g in range(groups):
            padded[g, pl.ds(pl.multiple_of(t * BLOCK + halo, halo), BLOCK), :] = wide[
                :, g * lanes : (g + 1) * lanes
            ]
        return units

    units = unit(tiles - 1, 0)
    halo_out[...] = units[BLOCK - halo :, :]
    halo_copy = onward(halo_out, halo_in, halo_send.at[0], halo_recv.at[0], 1)

    @pl.when(place + 1 < sp)
    def _():
        halo_copy.start()

    def unit_loop(t, carry):
        unit(t, 0)
        return carry

    lax.fori_loop(0, tiles - 1, unit_loop, 0)

    def conv(t, carry):
        first = jnp.zeros((BLOCK, 1), jnp.float32)
        second = jnp.zeros((BLOCK, 1), jnp.float32)
        for g in range(groups):
            total = jnp.zeros((BLOCK, lanes), jnp.float32)
            for j in range(kernel):
                start = t * BLOCK + (halo - kernel + 1 + j)
                tap = taps_ref[j : j + 1, g * lanes : (g + 1) * lanes]
                total = total + padded[g, pl.ds(start, BLOCK), :] * tap
            filtered[g, at(t), :] = total
            first = first + jnp.sum(total, axis=1, keepdims=True)
            second = second + jnp.sum(total * total, axis=1, keepdims=True)
        lane = lax.broadcasted_iota(jnp.int32, (BLOCK, BLOCK), 1)
        sums_out[t] = jnp.where(lane == 0, first, jnp.where(lane == 1, second, 0.0)).T[:8, :]
        return carry

    half = tiles // 2
    lax.fori_loop(1, half, conv, 0)
    if last > 0:
        exchange(0)
    lax.fori_loop(half, tiles, conv, 0)

    @pl.when(place >= 1)
    def _():
        halo_copy.wait_recv()

    @pl.when(place < 1)
    def _():
        halo_in[...] = jnp.zeros(halo_in.shape, jnp.bfloat16)

    before = halo_in[...].astype(jnp.float32)
    for g in range(groups):
        padded[g, :halo, :] = before[:, g * lanes : (g + 1) * lanes]
    conv(0, 0)

    def ln_copy(step):
        return pltpu.make_async_remote_copy(
            src_ref=sums_out,
            dst_ref=sums_in.at[step - 1],
            send_sem=ln_send.at[step - 1],
            recv_sem=ln_recv.at[step - 1],
            device_id={"tp": lax.rem(me + step, tp)},
            device_id_type=MESH,
        )

    for step in range(1, tp):
        ln_copy(step).start()
    for i in range(1, last):
        exchange(i)
    for step in range(1, tp):
        ln_copy(step).wait()
    channels = groups * lanes * tp

    def norm(t, carry):
        sums = sums_out[t]
        for step in range(1, tp):
            sums = sums + sums_in[step - 1, t]
        sums = jnp.concatenate([sums, jnp.zeros((BLOCK - 8, BLOCK), jnp.float32)], axis=0).T
        center = sums[:, 0:1] / channels
        variance = jnp.maximum(sums[:, 1:2] / channels - center * center, 0.0)
        scale = lax.rsqrt(variance + TINY_VAR)
        for g in range(groups):
            cut = slice(g * lanes, (g + 1) * lanes)
            normed = (filtered[g, at(t), :] - center) * scale
            normed = normed * ln_gain_ref[:, cut] + ln_shift_ref[:, cut]
            gate = cg_ref[at(t), cut].astype(jnp.float32)
            conv_ref[at(t), cut] = (jax.nn.silu(normed) * jax.nn.silu(gate)).astype(jnp.bfloat16)
        return carry

    lax.fori_loop(0, tiles, norm, 0)
    carried = []
    for h in range(heads):
        take_carry(last, h)
        earlier = far_s[last, h, :, width:]
        if last > 0:
            window = window_s[h]
            earlier = mm(window[:, :width], earlier) + window[:, width:]
        carried.append(earlier.astype(jnp.bfloat16))

    def one_tile(t, carry):
        for h in range(heads):
            cut = slice(h * width, (h + 1) * width)
            result = outb_ref[h, at(t), :] + mm(outa_ref[h, at(t), :], carried[h])
            result = result * lax.rsqrt(
                jnp.mean(result * result, axis=-1, keepdims=True) + TINY_NORM
            )
            gate = dg_ref[at(t), cut].astype(jnp.float32)
            mixed_ref[at(t), cut] = (result * gain_ref[...] * jax.nn.silu(gate)).astype(
                jnp.bfloat16
            )
        return carry

    lax.fori_loop(0, tiles, one_tile, 0)
    for i in range(last + 1):
        @pl.when(place + reaches[i] < sp)
        def _(i=i):
            for h in range(heads):
                carry_copy(i, h).wait_send()

    @pl.when(place + 1 < sp)
    def _():
        halo_copy.wait_send()


def middle(final, glu_value, glu_gate, conv_gate, taps, ln_gain, ln_shift, outa, outb, gate, gain):
    heads, width = final.shape[0], final.shape[1]
    rows, channels = glu_value.shape
    kernel = taps.shape[0]
    halo = (kernel - 1 + 31) // 32 * 32
    lanes = min(channels, 128)
    groups = channels // lanes
    sp, tp = lax.axis_size("sp"), lax.axis_size("tp")
    steps = 1
    while 2**steps < sp:
        steps += 1
    vm = pl.BlockSpec(memory_space=pltpu.VMEM)
    dma = pltpu.SemaphoreType.DMA
    tiles = rows // BLOCK
    pair = (heads, width, 2 * width)
    return pl.pallas_call(
        functools.partial(middle_kernel, heads, width),
        out_shape=(
            jax.ShapeDtypeStruct((rows, heads * width), jnp.bfloat16),
            jax.ShapeDtypeStruct((rows, channels), jnp.bfloat16),
        ),
        in_specs=[vm] * 11,
        out_specs=(vm, vm),
        scratch_shapes=[
            pltpu.VMEM((groups, halo + rows, lanes), jnp.float32),
            pltpu.VMEM((groups, rows, lanes), jnp.float32),
            pltpu.VMEM((halo, channels), jnp.bfloat16),
            pltpu.VMEM((halo, channels), jnp.bfloat16),
            pltpu.VMEM((tiles, 8, BLOCK), jnp.float32),
            pltpu.VMEM((tp - 1, tiles, 8, BLOCK), jnp.float32),
            pltpu.VMEM(pair, jnp.float32),
            pltpu.VMEM((steps,) + pair, jnp.bfloat16),
            pltpu.VMEM((steps,) + pair, jnp.bfloat16),
            dma((steps, heads)),
            dma((steps, heads)),
            dma((1,)),
            dma((1,)),
            dma((tp - 1,)),
            dma((tp - 1,)),
        ],
        compiler_params=pltpu.CompilerParams(
            collective_id=2, has_side_effects=True, vmem_limit_bytes=40 * 1024 * 1024
        ),
        cost_estimate=pl.CostEstimate(
            flops=10_000_000_000, bytes_accessed=20_000_000, transcendentals=0
        ),
        name="exchange_middle",
    )(final, glu_value, glu_gate, conv_gate, taps, ln_gain, ln_shift, outa, outb, gate, gain)


def output_kernel(
    dm_ref, cm_ref, wd_ref, wc_ref, out_ref,
    beside_out, beside_in, across_out, across_in, b_send, b_recv, y_send, y_recv,
):
    chips, me, core, chip, sibling = sharded_place()
    rows = out_ref.shape[0]
    width = out_ref.shape[1] // CUTS

    def cols(n):
        return pl.ds(pl.multiple_of(n * width, width), width)

    def partial(target, n):
        at = pl.ds(pl.multiple_of(target * rows, rows), rows)
        summed = jnp.dot(dm_ref[at, :], wd_ref[:, cols(n)], preferred_element_type=jnp.float32)
        return summed + jnp.dot(
            cm_ref[at, :], wc_ref[:, cols(n)], preferred_element_type=jnp.float32
        )

    def beside(o, n):
        return pltpu.make_async_remote_copy(
            src_ref=beside_out.at[o, n],
            dst_ref=beside_in.at[o, n],
            send_sem=b_send.at[o, n],
            recv_sem=b_recv.at[o, n],
            device_id={"tp": sibling},
            device_id_type=MESH,
        )

    def across(o, n):
        there = lax.rem(chip + o, chips) * 2 + core
        return pltpu.make_async_remote_copy(
            src_ref=across_out.at[o - 1, n],
            dst_ref=across_in.at[o - 1, n],
            send_sem=y_send.at[o - 1, n],
            recv_sem=y_recv.at[o - 1, n],
            device_id={"tp": there},
            device_id_type=MESH,
        )

    greet(chips, core, chip, sibling)
    order = list(range(1, chips)) + [0]
    for o in order:
        their_chip = lax.rem(chip + o, chips) * 2

        def give(n, carry, o=o, their_chip=their_chip):
            beside_out[o, n] = partial(their_chip + 1 - core, n).astype(jnp.bfloat16)
            beside(o, n).start()
            return carry

        def keep(n, carry, o=o, their_chip=their_chip):
            mine = partial(their_chip + core, n)
            beside(o, n).wait_recv()
            mine = mine + beside_in[o, n].astype(jnp.float32)
            across_out[o - 1, n] = mine.astype(jnp.bfloat16)
            across(o, n).start()
            return carry

        if o != 0:

            def both(n, carry, give=give, keep=keep):
                @pl.when(n + 1 < CUTS)
                def _():
                    give(n + 1, 0)

                return keep(n, carry)

            give(0, 0)
            lax.fori_loop(0, CUTS, both, 0)
        else:
            lax.fori_loop(0, CUTS, give, 0)

    def close(n, carry):
        mine = partial(me, n)
        beside(0, n).wait_recv()
        mine = mine + beside_in[0, n].astype(jnp.float32)
        for o in range(1, chips):
            across(o, n).wait_recv()
            mine = mine + across_in[o - 1, n].astype(jnp.float32)
        out_ref[:, cols(n)] = mine.astype(jnp.bfloat16)
        return carry

    lax.fori_loop(0, CUTS, close, 0)

    def drain(n, carry):
        for o in range(chips):
            beside(o, n).wait_send()
        for o in range(1, chips):
            across(o, n).wait_send()
        return carry

    lax.fori_loop(0, CUTS, drain, 0)


def output_projection(delta_mixed, conv_mixed, out_delta, out_conv):
    tp = lax.axis_size("tp")
    chips = tp // 2
    others = max(chips - 1, 1)
    rows = delta_mixed.shape[0] // tp
    width = out_delta.shape[1]
    cut = width // CUTS
    vm = pl.BlockSpec(memory_space=pltpu.VMEM)
    dma = pltpu.SemaphoreType.DMA
    return pl.pallas_call(
        output_kernel,
        out_shape=jax.ShapeDtypeStruct((rows, width), jnp.bfloat16),
        in_specs=[vm] * 4,
        out_specs=vm,
        scratch_shapes=[
            pltpu.VMEM((chips, CUTS, rows, cut), jnp.bfloat16),
            pltpu.VMEM((chips, CUTS, rows, cut), jnp.bfloat16),
            pltpu.VMEM((others, CUTS, rows, cut), jnp.bfloat16),
            pltpu.VMEM((others, CUTS, rows, cut), jnp.bfloat16),
            dma((chips, CUTS)),
            dma((chips, CUTS)),
            dma((others, CUTS)),
            dma((others, CUTS)),
        ],
        compiler_params=pltpu.CompilerParams(
            collective_id=1, has_side_effects=True, vmem_limit_bytes=48 * 1024 * 1024
        ),
        cost_estimate=pl.CostEstimate(
            flops=10_000_000_000, bytes_accessed=20_000_000, transcendentals=0
        ),
        name="output_scatter",
    )(delta_mixed, conv_mixed, out_delta, out_conv)


def local(
    tokens,
    w_query,
    w_key,
    w_value,
    w_delta_gate,
    w_glu_value,
    w_glu_gate,
    w_conv_gate,
    w_beta,
    w_decay,
    decay_log,
    head_gain,
    conv_taps,
    ln_gain,
    ln_shift,
    out_delta,
    out_conv,
):
    head_size = head_gain.shape[0]
    heads_here = w_query.shape[1] // head_size
    first_head = lax.axis_index("tp") * heads_here
    rates = jnp.exp(lax.dynamic_slice_in_dim(decay_log, first_head, heads_here, 0))
    fill = head_size - 2 * heads_here
    rates = jnp.concatenate(
        [jnp.zeros((heads_here,), jnp.float32), rates, jnp.zeros((fill,), jnp.float32)]
    )[None, :]
    w_gates = jnp.concatenate(
        [
            lax.dynamic_slice_in_dim(w_beta, first_head, heads_here, 1),
            lax.dynamic_slice_in_dim(w_decay, first_head, heads_here, 1),
            jnp.zeros((w_beta.shape[0], fill), jnp.bfloat16),
        ],
        axis=1,
    )
    weights = (w_query, w_key, w_value, w_delta_gate, w_glu_value, w_glu_gate, w_conv_gate)
    (
        query_raw,
        key_raw,
        value_raw,
        delta_gate_raw,
        glu_value_raw,
        glu_gate_raw,
        conv_gate_raw,
        gates,
    ) = project(tokens, weights, w_gates, rates, heads_here)
    outa, outb, final = delta_rule(
        query_raw, key_raw, value_raw, gates, heads_here, head_size
    )
    delta_mixed, conv_mixed = middle(
        final,
        glu_value_raw,
        glu_gate_raw,
        conv_gate_raw,
        conv_taps.astype(jnp.float32),
        ln_gain[None, :],
        ln_shift[None, :],
        outa,
        outb,
        delta_gate_raw,
        head_gain[None, :],
    )
    return output_projection(delta_mixed, conv_mixed, out_delta, out_conv)


def solution(mesh):
    return jax.shard_map(
        local,
        mesh=mesh,
        in_specs=(
            P("sp", "tp"),
            P(None, "tp"),
            P(None, "tp"),
            P(None, "tp"),
            P(None, "tp"),
            P(None, "tp"),
            P(None, "tp"),
            P(None, "tp"),
            P(),
            P(),
            P(),
            P(),
            P(None, "tp"),
            P("tp"),
            P("tp"),
            P("tp", None),
            P("tp", None),
        ),
        out_specs=P(("sp", "tp"), None),
        check_vma=False,
    )
```

```python
import functools

import jax
import jax.numpy as jnp
from jax import lax
from jax.experimental import pallas as pl
from jax.experimental.pallas import tpu as pltpu
from jax.sharding import PartitionSpec as P

BLOCK = 128
PROJECTIONS = 7
QUERY, KEY, VALUE, DELTA_GATE, GLU_VALUE, GLU_GATE, CONV_GATE = range(PROJECTIONS)
OUT_CUT = 512
TINY_NORM = 1e-06
TINY_VAR = 1e-05
HIGHEST = lax.Precision.HIGHEST
MESH = pl.DeviceIdType.MESH


def nt(a, b):
    return lax.dot_general(a, b, (((1,), (1,)), ((), ())), preferred_element_type=jnp.float32)


def mm(a, b):
    return jnp.dot(
        a.astype(jnp.bfloat16), b.astype(jnp.bfloat16), preferred_element_type=jnp.float32
    )


def slice_shape(rows, columns, pieces):
    high = max(16, rows // pieces)
    across = pieces // (rows // high)
    return high, columns // across, across


def layer_kernel(
    heads, width,
    tok_hbm, wq_hbm, wk_hbm, wv_hbm, wdg_hbm, wgv_hbm, wgg_hbm, wcg_hbm,
    beta_hbm, decay_hbm, rate_hbm, gain_hbm, taps_hbm, ln_gain_hbm, ln_shift_hbm,
    out_delta_hbm, out_conv_hbm,
    out_ref,
    full, w_s, beta_s, decay_s, rate_s, gain_ref, taps_s, ln_gain_ref, ln_shift_ref,
    wg_s, rate_row, taps_ref, proj, gates_s, wfull,
    lhs_s, corr_s, score_s, wt_s, tail_s, state_ref, outa_ref, outb_ref, final_ref,
    padded, filtered, halo_out, halo_in, sums_out, sums_in, window_s, sent_s, far_s,
    mixed_out, mixed_in, acc_s,
    tok_sem, w_sem, small_sem, ow_sem,
    y_send, y_recv, own_send, own_recv, fwd_send, fwd_recv,
    wo_send, wo_recv, wy_send, wy_recv, wl_send, wl_recv, wx_send, wx_recv, wb_send, wb_recv,
    far_send, far_recv, halo_send, halo_recv, ln_send, ln_recv, mix_send, mix_recv,
):
    rows = full.shape[0]
    tp, me = lax.axis_size("tp"), lax.axis_index("tp")
    sp, place = lax.axis_size("sp"), lax.axis_index("sp")
    part = full.shape[1] // tp
    chips = tp // 2
    core = lax.rem(me, 2)
    chip = me // 2
    sibling = me + 1 - 2 * core
    tiles = rows // BLOCK
    halo = halo_in.shape[0]
    lanes = padded.shape[2]
    groups = padded.shape[0]
    kernel = taps_s.shape[0]
    line = sp // 2
    spot = place // 2
    side = lax.rem(place, 2)

    def at(t, count=1):
        return pl.ds(pl.multiple_of(t * BLOCK, BLOCK), count * BLOCK)

    def columns(owner):
        return pl.ds(pl.multiple_of(owner * part, part), part)

    token_loads = [
        pltpu.make_async_copy(
            tok_hbm.at[at(r), :], full.at[at(r), columns(me)], tok_sem.at[r]
        )
        for r in range(tiles)
    ]
    out_loads = [
        pltpu.make_async_copy(src, wfull.at[i, me], ow_sem.at[i])
        for i, src in enumerate((out_delta_hbm, out_conv_hbm))
    ]
    w_loads = [
        pltpu.make_async_copy(src, w_s.at[i], w_sem.at[i])
        for i, src in enumerate((wq_hbm, wk_hbm, wv_hbm, wdg_hbm, wgv_hbm, wgg_hbm, wcg_hbm))
    ]
    small_loads = [
        pltpu.make_async_copy(src, dst, small_sem.at[i])
        for i, (src, dst) in enumerate((
            (beta_hbm, beta_s), (decay_hbm, decay_s), (rate_hbm, rate_s), (gain_hbm, gain_ref),
            (taps_hbm, taps_s), (ln_gain_hbm, ln_gain_ref), (ln_shift_hbm, ln_shift_ref),
        ))
    ]
    token_loads[0].start()
    for load in out_loads + token_loads[1:] + small_loads + w_loads:
        load.start()

    reaches = [1]
    while 2 * reaches[-1] < sp:
        reaches.append(2 * reaches[-1])
    last = len(reaches) - 1
    distances = sorted(set(reaches) | set(range(2, sp, 2)))
    barrier = pltpu.get_barrier_semaphore()
    expected = tp - 1
    for step in range(1, tp):
        pl.semaphore_signal(
            barrier, inc=1, device_id={"tp": lax.rem(me + step, tp)}, device_id_type=MESH
        )
    for step in distances:
        ahead, behind = place + step < sp, place >= step

        @pl.when(ahead)
        def _(step=step):
            pl.semaphore_signal(
                barrier, inc=1, device_id={"sp": place + step}, device_id_type=MESH
            )

        @pl.when(behind)
        def _(step=step):
            pl.semaphore_signal(
                barrier, inc=1, device_id={"sp": place - step}, device_id_type=MESH
            )

        expected = expected + ahead.astype(jnp.int32) + behind.astype(jnp.int32)
    pl.semaphore_wait(barrier, expected)

    def to_tp(src, dst, send, recv, there):
        return pltpu.make_async_remote_copy(
            src_ref=src, dst_ref=dst, send_sem=send, recv_sem=recv,
            device_id={"tp": there}, device_id_type=MESH,
        )

    def to_sp(src, dst, send, recv, there):
        return pltpu.make_async_remote_copy(
            src_ref=src, dst_ref=dst, send_sem=send, recv_sem=recv,
            device_id={"sp": there}, device_id_type=MESH,
        )

    def far_peer(o):
        return lax.rem(chip + o, chips) * 2 + core

    def far_owner(o):
        return lax.rem(chip - o + chips, chips) * 2 + core

    def across(o, r):
        block = full.at[at(r), columns(me)]
        return to_tp(block, block, y_send.at[o - 1, r], y_recv.at[o - 1, r], far_peer(o))

    def beside(r):
        block = full.at[at(r), columns(me)]
        return to_tp(block, block, own_send.at[r], own_recv.at[r], sibling)

    def forward(o, r):
        block = full.at[at(r), columns(far_owner(o))]
        return to_tp(block, block, fwd_send.at[o - 1, r], fwd_recv.at[o - 1, r], sibling)

    high, broad, split = slice_shape(wfull.shape[2], wfull.shape[3], sp)

    def weight_slice(owner, index):
        top = pl.ds(pl.multiple_of(index // split * high, high), high)
        left = pl.ds(pl.multiple_of(lax.rem(index, split) * broad, broad), broad)
        return wfull.at[:, owner, top, left]

    def weights_beside():
        return to_tp(wfull.at[:, me], wfull.at[:, me], wo_send.at[0], wo_recv.at[0], sibling)

    def weights_across(o):
        piece = weight_slice(me, place)
        return to_tp(piece, piece, wy_send.at[o - 1], wy_recv.at[o - 1], far_peer(o))

    def weights_along(o, there, origin):
        piece = weight_slice(far_owner(o), 2 * origin + side)
        return to_sp(
            piece, piece, wl_send.at[o - 1, there], wl_recv.at[o - 1, origin], 2 * there + side
        )

    def weights_pair(o, j, parity):
        piece = weight_slice(far_owner(o), 2 * j + parity)
        return to_sp(
            piece, piece, wx_send.at[o - 1, j], wx_recv.at[o - 1, j], place + 1 - 2 * side
        )

    def weights_forward(o):
        block = wfull.at[:, far_owner(o)]
        return to_tp(block, block, wb_send.at[o - 1], wb_recv.at[o - 1], sibling)

    def both_ways(step, action):
        for there, valid in ((spot + step, spot + step < line), (spot - step, spot >= step)):
            @pl.when(valid)
            def _(there=there):
                action(jnp.clip(there, 0, line - 1))

    def spread_weights():
        for o in range(1, chips):
            weights_across(o).wait_recv()
        for step in range(1, line):
            def send(there):
                for o in range(1, chips):
                    weights_along(o, there, spot).start()

            both_ways(step, send)
        for o in range(1, chips):
            weights_pair(o, spot, side).start()

    def relay_weights(step):
        def relay(origin):
            for o in range(1, chips):
                weights_along(o, origin, origin).wait_recv()
                weights_pair(o, origin, side).start()

        both_ways(step, relay)

    def collect_weights():
        for o in range(1, chips):
            for j in range(line):
                weights_pair(o, j, 1 - side).wait_recv()
            weights_forward(o).start()

    for load in out_loads:
        load.wait()
    for o in range(1, chips):
        weights_across(o).start()
    for r in range(tiles):
        token_loads[r].wait()
        for o in range(1, chips):
            across(o, r).start()
        beside(r).start()
    weights_beside().start()
    for load in small_loads:
        load.wait()

    first_head = me * heads
    total_heads = beta_s.shape[0]
    lane_row = lax.broadcasted_iota(jnp.int32, (1, BLOCK), 1)
    rate = jnp.zeros((1, BLOCK), jnp.float32)
    for h in range(total_heads):
        value = jnp.exp(jnp.broadcast_to(rate_s[:, h : h + 1], (1, BLOCK)))
        rate = jnp.where(lane_row == h - first_head + heads, value, rate)
    rate = jnp.where((lane_row >= heads) & (lane_row < 2 * heads), rate, 0.0)
    rate_row[...] = rate
    pick_row = lax.broadcasted_iota(jnp.int32, (BLOCK, total_heads), 0)
    pick_col = lax.broadcasted_iota(jnp.int32, (BLOCK, total_heads), 1)
    pick_beta = (pick_row < heads) & (pick_col == pick_row + first_head)
    pick_decay = (
        (pick_row >= heads) & (pick_row < 2 * heads) & (pick_col == pick_row - heads + first_head)
    )
    wg_s[...] = (
        mm(jnp.where(pick_beta, 1.0, 0.0), beta_s[...])
        + mm(jnp.where(pick_decay, 1.0, 0.0), decay_s[...])
    ).astype(jnp.bfloat16)
    taps_ref[...] = taps_s[...].astype(jnp.float32)

    def receive(first, count):
        for i in range(count):
            for o in range(1, chips):
                across(o, first + i).wait_recv()
                forward(o, first + i).start()
        for i in range(count):
            beside(first + i).wait_recv()
            for o in range(1, chips):
                forward(o, first + i).wait_recv()

    def project(first, count):
        size = count * BLOCK
        here = at(first, count)
        squares = jnp.zeros((size, 1), jnp.float32)
        for b in range(tp):
            piece = full[here, b * part : (b + 1) * part].astype(jnp.float32)
            squares = squares + jnp.sum(piece * piece, axis=1, keepdims=True)
        inv_rms = lax.rsqrt(squares / (part * tp) + TINY_NORM)
        raw = nt(full[here, :], wg_s[...]) * inv_rms
        lane = lax.broadcasted_iota(jnp.int32, raw.shape, 1)
        softplus = jnp.maximum(raw, 0.0) + jnp.log1p(jnp.exp(-jnp.abs(raw)))
        gates_s[here, :] = jnp.where(
            lane < heads, jax.nn.sigmoid(raw), -rate_row[...] * softplus
        )
        for i in range(PROJECTIONS):
            summed = jnp.dot(full[here, :], w_s[i], preferred_element_type=jnp.float32)
            proj[i, here, :] = (summed * inv_rms).astype(jnp.bfloat16)

    row_id = lax.broadcasted_iota(jnp.int32, (BLOCK, BLOCK), 0)
    col_id = lax.broadcasted_iota(jnp.int32, (BLOCK, BLOCK), 1)
    causal = row_id >= col_id
    strict = row_id > col_id
    differ = row_id ^ col_id
    eye = jnp.where(row_id == col_id, 1.0, 0.0)
    tril = jnp.where(causal, 1.0, 0.0)

    def prepare(c):
        here = at(c)
        gates = gates_s[here, :]
        sums = jnp.dot(tril, gates, precision=HIGHEST, preferred_element_type=jnp.float32)
        chains = []
        for h in range(heads):
            cut = slice(h * width, (h + 1) * width)
            k, q = proj[KEY, here, cut], proj[QUERY, here, cut]
            v = proj[VALUE, here, cut].astype(jnp.float32)
            kf, qf = k.astype(jnp.float32), q.astype(jnp.float32)
            ik = lax.rsqrt(jnp.sum(kf * kf, axis=-1, keepdims=True) + TINY_NORM)
            iq = lax.rsqrt(jnp.sum(qf * qf, axis=-1, keepdims=True) + TINY_NORM)
            iq = iq * width ** (-0.5)
            beta = gates[:, h : h + 1]
            log_sum = sums[:, heads + h : heads + h + 1]
            log_full = jnp.broadcast_to(log_sum, (BLOCK, BLOCK))
            spread = log_full - log_full.T
            damp = jnp.where(causal, jnp.exp(jnp.where(causal, spread, 0.0)), 0.0)
            damp = damp * jnp.broadcast_to(ik, (BLOCK, BLOCK)).T
            lower = jnp.where(strict, nt(k, k) * damp * (beta * ik), 0.0)
            score_s[h, here, :] = (nt(q, k) * damp * iq).astype(jnp.bfloat16)
            grow = jnp.exp(log_sum)
            right = jnp.concatenate([v * beta, kf * (beta * ik * grow)], axis=1)
            tail = log_full[BLOCK - 1 : BLOCK, :]
            weighted = kf * (ik * jnp.exp(tail[:, :1] - log_sum))
            wt_s[h, c] = weighted.T.astype(jnp.bfloat16)
            tail_s[h, c] = jnp.broadcast_to(jnp.exp(tail), (8, BLOCK))
            lhs_s[h, c, BLOCK:, :] = (qf * (iq * grow)).astype(jnp.bfloat16)
            chains.append([h, lower, right, eye - jnp.where(differ == 1, lower, 0.0)])
        return here, c, chains

    def blocks(first, count):
        prepared = [prepare(first + i) for i in range(count)]
        size = 2
        while size < BLOCK:
            level = (differ >= size) & (differ < 2 * size)
            parts = [
                [mm(jnp.where(level, ch[1], 0.0), ch[3]) for ch in item[2]] for item in prepared
            ]
            for item, moves in zip(prepared, parts):
                for ch, moved in zip(item[2], moves):
                    ch[3] = ch[3] - mm(ch[3], moved)
            size *= 2
        for here, c, chains in prepared:
            for h, lower, right, inverse in chains:
                solved = mm(inverse, right)
                corr_s[h, here, :] = solved[:, :width]
                lhs_s[h, c, :BLOCK, :] = solved[:, width:].astype(jnp.bfloat16)

    def advance(c):
        here = at(c)
        boths = [mm(lhs_s[h, c], state_ref[h]) for h in range(heads)]
        fresh = []
        for h in range(heads):
            first = boths[h][:BLOCK]
            fresh.append(
                jnp.concatenate(
                    [-first[:, :width], corr_s[h, here, :] - first[:, width:]], axis=1
                ).astype(jnp.bfloat16)
            )
        for h in range(heads):
            decay = tail_s[h, c][:1, :]
            decay = jnp.concatenate([decay, decay], axis=1)
            state_ref[h] = state_ref[h] * decay + mm(wt_s[h, c], fresh[h])
        for h in range(heads):
            out = boths[h][BLOCK:] + mm(score_s[h, here, :], fresh[h])
            outa_ref[h, here, :] = out[:, :width].astype(jnp.bfloat16)
            outb_ref[h, here, :] = out[:, width:]

    def unit(t):
        value = proj[GLU_VALUE, at(t), :].astype(jnp.float32)
        gate = proj[GLU_GATE, at(t), :].astype(jnp.float32)
        units = (value * jax.nn.sigmoid(gate)).astype(jnp.bfloat16)
        wide = units.astype(jnp.float32)
        for g in range(groups):
            padded[g, pl.ds(pl.multiple_of(t * BLOCK + halo, halo), BLOCK), :] = wide[
                :, g * lanes : (g + 1) * lanes
            ]
        return units

    def conv(t, carry=0):
        first = jnp.zeros((BLOCK, 1), jnp.float32)
        second = jnp.zeros((BLOCK, 1), jnp.float32)
        for g in range(groups):
            total = jnp.zeros((BLOCK, lanes), jnp.float32)
            for j in range(kernel):
                start = t * BLOCK + (halo - kernel + 1 + j)
                tap = taps_ref[j : j + 1, g * lanes : (g + 1) * lanes]
                total = total + padded[g, pl.ds(start, BLOCK), :] * tap
            filtered[g, at(t), :] = total
            first = first + jnp.sum(total, axis=1, keepdims=True)
            second = second + jnp.sum(total * total, axis=1, keepdims=True)
        lane = lax.broadcasted_iota(jnp.int32, (BLOCK, BLOCK), 1)
        sums_out[t] = jnp.where(lane == 0, first, jnp.where(lane == 1, second, 0.0)).T[:8, :]
        return carry

    for h in range(heads):
        state_ref[h] = jnp.concatenate([eye, jnp.zeros((width, width), jnp.float32)], axis=1)
    for load in w_loads:
        load.wait()
    spread_weights()
    receive(0, 2)
    project(0, 2)

    def pair(i, carry):
        receive(2 * i, 2)
        relay_weights(i)
        project(2 * i, 2)
        blocks(2 * i - 2, 2)
        for n in range(2):
            advance(2 * i - 2 + n)
            unit(2 * i - 2 + n)

        def filter_tile(t, inner):
            @pl.when(t > 0)
            def _():
                conv(t)

            return inner

        lax.fori_loop(2 * i - 2, 2 * i, filter_tile, 0)
        return carry

    paired = tiles // 2 - 1
    lax.fori_loop(1, paired, pair, 0)
    for step in range(paired, line):
        relay_weights(step)
    tail = 2 * paired
    receive(tail, 1)
    project(tail, 1)
    blocks(tail - 2, 2)
    for n in range(2):
        advance(tail - 2 + n)
    receive(tail + 1, 1)
    project(tail + 1, 1)
    units = unit(tail + 1)
    halo_out[...] = units[BLOCK - halo :, :]
    halo_copy = to_sp(
        halo_out, halo_in, halo_send.at[0], halo_recv.at[0], jnp.minimum(place + 1, sp - 1)
    )

    @pl.when(place + 1 < sp)
    def _():
        halo_copy.start()

    blocks(tail, 2)
    for n in range(2):
        advance(tail + n)
    final_ref[...] = state_ref[...].astype(jnp.bfloat16)

    def carry_copy(i, h):
        cut = slice(width, 2 * width) if i == last else slice(0, 2 * width)
        source = final_ref if i == 0 else sent_s.at[i - 1]
        return to_sp(
            source.at[h, :, cut], far_s.at[i, h, :, cut], far_send.at[i, h], far_recv.at[i, h],
            jnp.minimum(place + reaches[i], sp - 1),
        )

    def send_carry(i, h):
        @pl.when(place + reaches[i] < sp)
        def _():
            carry_copy(i, h).start()

    def take_carry(i, h):
        @pl.when(place >= reaches[i])
        def _():
            carry_copy(i, h).wait_recv()

        @pl.when(place < reaches[i])
        def _():
            far_s[i, h] = jnp.zeros((width, 2 * width), jnp.bfloat16)

    def combine(later, earlier):
        moved = mm(later[:, :width], earlier)
        return jnp.concatenate(
            [moved[:, :width], moved[:, width:] + later[:, width:].astype(jnp.float32)], axis=1
        )

    def exchange(i):
        for h in range(heads):
            take_carry(i, h)
            own = final_ref[h] if i == 0 else sent_s[i - 1, h]
            sent_s[i, h] = combine(own, far_s[i, h]).astype(jnp.bfloat16)
            send_carry(i + 1, h)
        for h in range(heads):
            if i == 0:
                window_s[h] = far_s[i, h].astype(jnp.float32)
            else:
                window_s[h] = combine(window_s[h], far_s[i, h])

    for h in range(heads):
        send_carry(0, h)

    for n in range(3):
        unit(tail - 2 + n)
    lax.fori_loop(tail - 2, tail + 2, conv, 0)

    @pl.when(place >= 1)
    def _():
        halo_copy.wait_recv()

    @pl.when(place < 1)
    def _():
        halo_in[...] = jnp.zeros(halo_in.shape, jnp.bfloat16)

    before = halo_in[...].astype(jnp.float32)
    for g in range(groups):
        padded[g, :halo, :] = before[:, g * lanes : (g + 1) * lanes]
    conv(0)

    def ln_copy(step):
        return to_tp(
            sums_out, sums_in.at[step - 1], ln_send.at[step - 1], ln_recv.at[step - 1],
            lax.rem(me + step, tp),
        )

    for step in range(1, tp):
        ln_copy(step).start()
    if last > 0:
        exchange(0)
    for step in range(1, tp):
        ln_copy(step).wait_recv()
    channels = groups * lanes * tp
    per = tiles // tp

    def mixed_copy(kind, there):
        return to_tp(
            mixed_out.at[kind, there], mixed_in.at[kind, me],
            mix_send.at[kind, there], mix_recv.at[kind, me], there,
        )

    def mixed_wait(kind, source):
        to_tp(
            mixed_out.at[kind, source], mixed_in.at[kind, source],
            mix_send.at[kind, source], mix_recv.at[kind, source], source,
        ).wait_recv()

    far_targets = [
        lax.rem(chip + o, chips) * 2 + lax.rem(core + c, 2) for o in range(1, chips) for c in (0, 1)
    ]

    def norm(target):
        def tile(i, carry):
            t = target * per + i
            here = pl.ds(pl.multiple_of(i * BLOCK, BLOCK), BLOCK)
            sums = sums_out[t]
            for step in range(1, tp):
                sums = sums + sums_in[step - 1, t]
            sums = jnp.concatenate([sums, jnp.zeros((BLOCK - 8, BLOCK), jnp.float32)], axis=0).T
            center = sums[:, 0:1] / channels
            variance = jnp.maximum(sums[:, 1:2] / channels - center * center, 0.0)
            scale = lax.rsqrt(variance + TINY_VAR)
            for g in range(groups):
                cut = slice(g * lanes, (g + 1) * lanes)
                normed = (filtered[g, at(t), :] - center) * scale
                normed = normed * ln_gain_ref[:, cut] + ln_shift_ref[:, cut]
                gate = proj[CONV_GATE, at(t), cut].astype(jnp.float32)
                mixed_out[1, target, here, cut] = (
                    jax.nn.silu(normed) * jax.nn.silu(gate)
                ).astype(jnp.bfloat16)
            return carry

        lax.fori_loop(0, per, tile, 0)

    for target in far_targets + [sibling]:
        norm(target)
        mixed_copy(1, target).start()
    norm(me)
    for i in range(1, last):
        exchange(i)
    collect_weights()

    def out_columns(n):
        return pl.ds(pl.multiple_of(n * OUT_CUT, OUT_CUT), OUT_CUT)

    cuts = out_ref.shape[1] // OUT_CUT
    sources = [sibling] + far_targets
    for source in sources:
        mixed_wait(1, source)
    weights_beside().wait_recv()
    for o in range(1, chips):
        weights_forward(o).wait_recv()

    def conv_part(n, carry):
        total = jnp.dot(
            mixed_out[1, me], wfull[1, me, :, out_columns(n)], preferred_element_type=jnp.float32
        )
        for source in sources:
            total = total + jnp.dot(
                mixed_in[1, source], wfull[1, source, :, out_columns(n)],
                preferred_element_type=jnp.float32,
            )
        acc_s[:, out_columns(n)] = total
        return carry

    lax.fori_loop(0, cuts, conv_part, 0)

    carried = []
    for h in range(heads):
        take_carry(last, h)
        earlier = far_s[last, h, :, width:]
        if last > 0:
            window = window_s[h]
            earlier = mm(window[:, :width], earlier) + window[:, width:]
        carried.append(earlier.astype(jnp.bfloat16))

    def attend(target):
        def tile(i, carry):
            t = target * per + i
            here = pl.ds(pl.multiple_of(i * BLOCK, BLOCK), BLOCK)
            for h in range(heads):
                cut = slice(h * width, (h + 1) * width)
                result = outb_ref[h, at(t), :] + mm(outa_ref[h, at(t), :], carried[h])
                result = result * lax.rsqrt(
                    jnp.mean(result * result, axis=-1, keepdims=True) + TINY_NORM
                )
                gate = proj[DELTA_GATE, at(t), cut].astype(jnp.float32)
                mixed_out[0, target, here, cut] = (
                    result * gain_ref[...] * jax.nn.silu(gate)
                ).astype(jnp.bfloat16)
            return carry

        lax.fori_loop(0, per, tile, 0)

    for target in far_targets + [sibling]:
        attend(target)
        mixed_copy(0, target).start()
    attend(me)
    mixed_wait(0, sibling)

    def near_part(n, carry):
        total = jnp.dot(
            mixed_out[0, me], wfull[0, me, :, out_columns(n)], preferred_element_type=jnp.float32
        )
        total = total + jnp.dot(
            mixed_in[0, sibling], wfull[0, sibling, :, out_columns(n)],
            preferred_element_type=jnp.float32,
        )
        acc_s[:, out_columns(n)] = acc_s[:, out_columns(n)] + total
        return carry

    lax.fori_loop(0, cuts, near_part, 0)
    for index, source in enumerate(far_targets):
        mixed_wait(0, source)

        def far_part(n, carry, source=source, closing=index + 1 == len(far_targets)):
            total = acc_s[:, out_columns(n)] + jnp.dot(
                mixed_in[0, source], wfull[0, source, :, out_columns(n)],
                preferred_element_type=jnp.float32,
            )
            if closing:
                out_ref[:, out_columns(n)] = total.astype(jnp.bfloat16)
            else:
                acc_s[:, out_columns(n)] = total
            return carry

        lax.fori_loop(0, cuts, far_part, 0)

    for r in range(tiles):
        for o in range(1, chips):
            across(o, r).wait_send()
            forward(o, r).wait_send()
        beside(r).wait_send()
    weights_beside().wait_send()
    for o in range(1, chips):
        weights_across(o).wait_send()
        weights_forward(o).wait_send()
        for j in range(line):
            weights_pair(o, j, side).wait_send()
    for step in range(1, line):
        def sent(there):
            for o in range(1, chips):
                weights_along(o, there, spot).wait_send()

        both_ways(step, sent)
    for i in range(last + 1):
        @pl.when(place + reaches[i] < sp)
        def _(i=i):
            for h in range(heads):
                carry_copy(i, h).wait_send()

    @pl.when(place + 1 < sp)
    def _():
        halo_copy.wait_send()

    for step in range(1, tp):
        ln_copy(step).wait_send()
    for kind in range(2):
        for target in sources:
            mixed_copy(kind, target).wait_send()


def layer(tokens, weights, w_beta, w_decay, decay_log, gain, taps, ln_gain, ln_shift, out_delta, out_conv):
    rows, part = tokens.shape
    width = gain.shape[1]
    features, held = weights[0].shape
    heads = held // width
    channels = taps.shape[1]
    depth, columns = out_delta.shape
    kernel = taps.shape[0]
    halo = (kernel - 1 + 31) // 32 * 32
    lanes = min(channels, 128)
    groups = channels // lanes
    sp, tp = lax.axis_size("sp"), lax.axis_size("tp")
    others = max(tp // 2 - 1, 1)
    line = sp // 2
    steps = 1
    while 2**steps < sp:
        steps += 1
    tiles = rows // BLOCK
    slot = rows // tp
    dma = pltpu.SemaphoreType.DMA
    pair = (heads, width, 2 * width)
    bf16, f32 = jnp.bfloat16, jnp.float32
    vmem = pltpu.VMEM
    return pl.pallas_call(
        functools.partial(layer_kernel, heads, width),
        out_shape=jax.ShapeDtypeStruct((slot, columns), bf16),
        in_specs=[pl.BlockSpec(memory_space=pl.ANY)] * 17,
        out_specs=pl.BlockSpec(memory_space=pltpu.VMEM),
        scratch_shapes=[
            vmem((rows, features), bf16),
            vmem((PROJECTIONS, features, held), bf16),
            vmem(w_beta.shape, bf16),
            vmem(w_decay.shape, bf16),
            vmem(decay_log.shape, f32),
            vmem(gain.shape, f32),
            vmem(taps.shape, bf16),
            vmem(ln_gain.shape, f32),
            vmem(ln_shift.shape, f32),
            vmem((BLOCK, features), bf16),
            vmem((1, BLOCK), f32),
            vmem(taps.shape, f32),
            vmem((PROJECTIONS, rows, held), bf16),
            vmem((rows, BLOCK), f32),
            vmem((2, tp, depth, columns), bf16),
            vmem((heads, tiles, 2 * BLOCK, width), bf16),
            vmem((heads, rows, width), f32),
            vmem((heads, rows, BLOCK), bf16),
            vmem((heads, tiles, width, BLOCK), bf16),
            vmem((heads, tiles, 8, BLOCK), f32),
            vmem(pair, f32),
            vmem((heads, rows, width), bf16),
            vmem((heads, rows, width), f32),
            vmem(pair, bf16),
            vmem((groups, halo + rows, lanes), f32),
            vmem((groups, rows, lanes), f32),
            vmem((halo, channels), bf16),
            vmem((halo, channels), bf16),
            vmem((tiles, 8, BLOCK), f32),
            vmem((tp - 1, tiles, 8, BLOCK), f32),
            vmem(pair, f32),
            vmem((steps,) + pair, bf16),
            vmem((steps,) + pair, bf16),
            vmem((2, tp, slot, channels), bf16),
            vmem((2, tp, slot, channels), bf16),
            vmem((slot, columns), f32),
            dma((tiles,)),
            dma((PROJECTIONS,)),
            dma((7,)),
            dma((2,)),
            dma((others, tiles)),
            dma((others, tiles)),
            dma((tiles,)),
            dma((tiles,)),
            dma((others, tiles)),
            dma((others, tiles)),
            dma((1,)),
            dma((1,)),
            dma((others,)),
            dma((others,)),
            dma((others, line)),
            dma((others, line)),
            dma((others, line)),
            dma((others, line)),
            dma((others,)),
            dma((others,)),
            dma((steps, heads)),
            dma((steps, heads)),
            dma((1,)),
            dma((1,)),
            dma((tp - 1,)),
            dma((tp - 1,)),
            dma((2, tp)),
            dma((2, tp)),
        ],
        compiler_params=pltpu.CompilerParams(
            collective_id=0, has_side_effects=True, vmem_limit_bytes=60 * 1024 * 1024
        ),
        cost_estimate=pl.CostEstimate(
            flops=20_000_000_000, bytes_accessed=20_000_000, transcendentals=0
        ),
        name="layer",
    )(
        tokens, *weights, w_beta, w_decay, decay_log, gain, taps, ln_gain, ln_shift,
        out_delta, out_conv,
    )


def local(
    tokens,
    w_query,
    w_key,
    w_value,
    w_delta_gate,
    w_glu_value,
    w_glu_gate,
    w_conv_gate,
    w_beta,
    w_decay,
    decay_log,
    head_gain,
    conv_taps,
    ln_gain,
    ln_shift,
    out_delta,
    out_conv,
):
    weights = (w_query, w_key, w_value, w_delta_gate, w_glu_value, w_glu_gate, w_conv_gate)
    return layer(
        tokens,
        weights,
        w_beta.T,
        w_decay.T,
        decay_log[None, :],
        head_gain[None, :],
        conv_taps,
        ln_gain[None, :],
        ln_shift[None, :],
        out_delta,
        out_conv,
    )


def solution(mesh):
    return jax.shard_map(
        local,
        mesh=mesh,
        in_specs=(
            P("sp", "tp"),
            P(None, "tp"),
            P(None, "tp"),
            P(None, "tp"),
            P(None, "tp"),
            P(None, "tp"),
            P(None, "tp"),
            P(None, "tp"),
            P(),
            P(),
            P(),
            P(),
            P(None, "tp"),
            P("tp"),
            P("tp"),
            P("tp", None),
            P("tp", None),
        ),
        out_specs=P(("sp", "tp"), None),
        check_vma=False,
    )
```

```python
import functools

import jax
import jax.numpy as jnp
from jax import lax
from jax.experimental import pallas as pl
from jax.experimental.pallas import tpu as pltpu
from jax.sharding import PartitionSpec as P

BLOCK = 128
PROJECTIONS = 7
QUERY, KEY, VALUE, DELTA_GATE, GLU_VALUE, GLU_GATE, CONV_GATE = range(PROJECTIONS)
OUT_CUT = 512
TINY_NORM = 1e-06
TINY_VAR = 1e-05
HIGHEST = lax.Precision.HIGHEST
MESH = pl.DeviceIdType.MESH


def nt(a, b):
    return lax.dot_general(a, b, (((1,), (1,)), ((), ())), preferred_element_type=jnp.float32)


def mm(a, b):
    return jnp.dot(
        a.astype(jnp.bfloat16), b.astype(jnp.bfloat16), preferred_element_type=jnp.float32
    )


def slice_shape(rows, columns, pieces):
    high = max(16, rows // pieces)
    across = pieces // (rows // high)
    return high, columns // across, across


def layer_kernel(
    heads, width,
    tok_hbm, wq_hbm, wk_hbm, wv_hbm, wdg_hbm, wgv_hbm, wgg_hbm, wcg_hbm,
    beta_hbm, decay_hbm, rate_hbm, gain_hbm, taps_hbm, ln_gain_hbm, ln_shift_hbm,
    out_delta_hbm, out_conv_hbm,
    out_ref,
    full, w_s, beta_s, decay_s, rate_s, gain_ref, taps_s, ln_gain_ref, ln_shift_ref,
    wg_s, rate_row, taps_ref, proj, gates_s, wfull,
    lhs_s, corr_s, score_s, wt_s, tail_s, state_ref, outa_ref, outb_ref, final_ref,
    padded, filtered, halo_out, halo_in, sums_out, sums_in, window_s, sent_s, far_s,
    mixed_out, mixed_in, acc_s,
    tok_sem, w_sem, small_sem, ow_sem,
    y_send, y_recv, own_send, own_recv, fwd_send, fwd_recv,
    wo_send, wo_recv, wy_send, wy_recv, wl_send, wl_recv, wx_send, wx_recv, wb_send, wb_recv,
    far_send, far_recv, halo_send, halo_recv, ln_send, ln_recv, mix_send, mix_recv,
):
    rows = full.shape[0]
    tp, me = lax.axis_size("tp"), lax.axis_index("tp")
    sp, place = lax.axis_size("sp"), lax.axis_index("sp")
    part = full.shape[1] // tp
    chips = tp // 2
    core = lax.rem(me, 2)
    chip = me // 2
    sibling = me + 1 - 2 * core
    tiles = rows // BLOCK
    halo = halo_in.shape[0]
    lanes = padded.shape[2]
    groups = padded.shape[0]
    kernel = taps_s.shape[0]
    line = sp // 2
    spot = place // 2
    side = lax.rem(place, 2)

    def at(t, count=1):
        return pl.ds(pl.multiple_of(t * BLOCK, BLOCK), count * BLOCK)

    def columns(owner):
        return pl.ds(pl.multiple_of(owner * part, part), part)

    token_loads = [
        pltpu.make_async_copy(
            tok_hbm.at[at(r), :], full.at[at(r), columns(me)], tok_sem.at[r]
        )
        for r in range(tiles)
    ]
    out_loads = [
        pltpu.make_async_copy(src, wfull.at[i, me], ow_sem.at[i])
        for i, src in enumerate((out_delta_hbm, out_conv_hbm))
    ]
    w_loads = [
        pltpu.make_async_copy(src, w_s.at[i], w_sem.at[i])
        for i, src in enumerate((wq_hbm, wk_hbm, wv_hbm, wdg_hbm, wgv_hbm, wgg_hbm, wcg_hbm))
    ]
    small_loads = [
        pltpu.make_async_copy(src, dst, small_sem.at[i])
        for i, (src, dst) in enumerate((
            (beta_hbm, beta_s), (decay_hbm, decay_s), (rate_hbm, rate_s), (gain_hbm, gain_ref),
            (taps_hbm, taps_s), (ln_gain_hbm, ln_gain_ref), (ln_shift_hbm, ln_shift_ref),
        ))
    ]
    token_loads[0].start()
    for load in out_loads + token_loads[1:] + small_loads + w_loads:
        load.start()

    reaches = [1]
    while 2 * reaches[-1] < sp:
        reaches.append(2 * reaches[-1])
    last = len(reaches) - 1
    barrier = pltpu.get_barrier_semaphore()
    expected = tp - 1
    for step in range(1, tp):
        pl.semaphore_signal(
            barrier, inc=1, device_id={"tp": lax.rem(me + step, tp)}, device_id_type=MESH
        )
    for step in reaches:
        ahead, behind = place + step < sp, place >= step

        @pl.when(ahead)
        def _(step=step):
            pl.semaphore_signal(
                barrier, inc=1, device_id={"sp": place + step}, device_id_type=MESH
            )

        @pl.when(behind)
        def _(step=step):
            pl.semaphore_signal(
                barrier, inc=1, device_id={"sp": place - step}, device_id_type=MESH
            )

        expected = expected + ahead.astype(jnp.int32) + behind.astype(jnp.int32)
    pl.semaphore_wait(barrier, expected)

    def to_tp(src, dst, send, recv, there):
        return pltpu.make_async_remote_copy(
            src_ref=src, dst_ref=dst, send_sem=send, recv_sem=recv,
            device_id={"tp": there}, device_id_type=MESH,
        )

    def to_sp(src, dst, send, recv, there):
        return pltpu.make_async_remote_copy(
            src_ref=src, dst_ref=dst, send_sem=send, recv_sem=recv,
            device_id={"sp": there}, device_id_type=MESH,
        )

    def far_peer(o):
        return lax.rem(chip + o, chips) * 2 + core

    def far_owner(o):
        return lax.rem(chip - o + chips, chips) * 2 + core

    def across(o, r):
        block = full.at[at(r), columns(me)]
        return to_tp(block, block, y_send.at[o - 1, r], y_recv.at[o - 1, r], far_peer(o))

    def beside(r):
        block = full.at[at(r), columns(me)]
        return to_tp(block, block, own_send.at[r], own_recv.at[r], sibling)

    def forward(o, r):
        block = full.at[at(r), columns(far_owner(o))]
        return to_tp(block, block, fwd_send.at[o - 1, r], fwd_recv.at[o - 1, r], sibling)

    high, broad, split = slice_shape(wfull.shape[2], wfull.shape[3], sp)

    def weight_slice(owner, index):
        top = pl.ds(pl.multiple_of(index // split * high, high), high)
        left = pl.ds(pl.multiple_of(lax.rem(index, split) * broad, broad), broad)
        return wfull.at[:, owner, top, left]

    def weights_beside():
        return to_tp(wfull.at[:, me], wfull.at[:, me], wo_send.at[0], wo_recv.at[0], sibling)

    def weights_across(o):
        piece = weight_slice(me, place)
        return to_tp(piece, piece, wy_send.at[o - 1], wy_recv.at[o - 1], far_peer(o))

    def weights_along(o, origin, up):
        piece = weight_slice(far_owner(o), 2 * origin + side)
        there = jnp.clip(spot + (1 if up else -1), 0, line - 1)
        return to_sp(
            piece, piece, wl_send.at[o - 1, int(up), origin], wl_recv.at[o - 1, origin],
            2 * there + side,
        )

    def weights_pair(o, j, parity):
        piece = weight_slice(far_owner(o), 2 * j + parity)
        return to_sp(
            piece, piece, wx_send.at[o - 1, j], wx_recv.at[o - 1, j], place + 1 - 2 * side
        )

    def weights_forward(o):
        block = wfull.at[:, far_owner(o)]
        return to_tp(block, block, wb_send.at[o - 1], wb_recv.at[o - 1], sibling)

    def pass_on(origin, up, arrived):
        for o in range(1, chips):
            if arrived:
                weights_along(o, origin, up).wait_recv()

            @pl.when(spot + 1 < line if up else spot >= 1)
            def _(o=o):
                weights_along(o, origin, up).start()

            if arrived:
                weights_pair(o, origin, side).start()

    def spread_weights():
        for o in range(1, chips):
            weights_across(o).wait_recv()
        pass_on(spot, True, False)
        pass_on(spot, False, False)
        for o in range(1, chips):
            weights_pair(o, spot, side).start()

    def relay_weights(step):
        @pl.when(spot >= step)
        def _():
            pass_on(jnp.maximum(spot - step, 0), True, True)

        @pl.when(spot + step < line)
        def _():
            pass_on(jnp.minimum(spot + step, line - 1), False, True)

    def collect_weights():
        for o in range(1, chips):
            for j in range(line):
                weights_pair(o, j, 1 - side).wait_recv()
            weights_forward(o).start()

    for load in out_loads:
        load.wait()
    for o in range(1, chips):
        weights_across(o).start()
    for r in range(tiles):
        token_loads[r].wait()
        for o in range(1, chips):
            across(o, r).start()
        beside(r).start()
    weights_beside().start()
    for load in small_loads:
        load.wait()

    first_head = me * heads
    total_heads = beta_s.shape[0]
    lane_row = lax.broadcasted_iota(jnp.int32, (1, BLOCK), 1)
    rate = jnp.zeros((1, BLOCK), jnp.float32)
    for h in range(total_heads):
        value = jnp.exp(jnp.broadcast_to(rate_s[:, h : h + 1], (1, BLOCK)))
        rate = jnp.where(lane_row == h - first_head + heads, value, rate)
    rate = jnp.where((lane_row >= heads) & (lane_row < 2 * heads), rate, 0.0)
    rate_row[...] = rate
    pick_row = lax.broadcasted_iota(jnp.int32, (BLOCK, total_heads), 0)
    pick_col = lax.broadcasted_iota(jnp.int32, (BLOCK, total_heads), 1)
    pick_beta = (pick_row < heads) & (pick_col == pick_row + first_head)
    pick_decay = (
        (pick_row >= heads) & (pick_row < 2 * heads) & (pick_col == pick_row - heads + first_head)
    )
    wg_s[...] = (
        mm(jnp.where(pick_beta, 1.0, 0.0), beta_s[...])
        + mm(jnp.where(pick_decay, 1.0, 0.0), decay_s[...])
    ).astype(jnp.bfloat16)
    taps_ref[...] = taps_s[...].astype(jnp.float32)

    def receive(first, count):
        for i in range(count):
            for o in range(1, chips):
                across(o, first + i).wait_recv()
                forward(o, first + i).start()
        for i in range(count):
            beside(first + i).wait_recv()
            for o in range(1, chips):
                forward(o, first + i).wait_recv()

    def project_steps(first, count):
        size = count * BLOCK
        here = at(first, count)
        squares = jnp.zeros((size, 1), jnp.float32)
        for b in range(tp):
            piece = full[here, b * part : (b + 1) * part].astype(jnp.float32)
            squares = squares + jnp.sum(piece * piece, axis=1, keepdims=True)
        inv_rms = lax.rsqrt(squares / (part * tp) + TINY_NORM)
        raw = nt(full[here, :], wg_s[...]) * inv_rms
        lane = lax.broadcasted_iota(jnp.int32, raw.shape, 1)
        softplus = jnp.maximum(raw, 0.0) + jnp.log1p(jnp.exp(-jnp.abs(raw)))
        gates_s[here, :] = jnp.where(
            lane < heads, jax.nn.sigmoid(raw), -rate_row[...] * softplus
        )
        yield
        for i in range(PROJECTIONS):
            summed = jnp.dot(full[here, :], w_s[i], preferred_element_type=jnp.float32)
            proj[i, here, :] = (summed * inv_rms).astype(jnp.bfloat16)
            yield

    row_id = lax.broadcasted_iota(jnp.int32, (BLOCK, BLOCK), 0)
    col_id = lax.broadcasted_iota(jnp.int32, (BLOCK, BLOCK), 1)
    causal = row_id >= col_id
    strict = row_id > col_id
    differ = row_id ^ col_id
    eye = jnp.where(row_id == col_id, 1.0, 0.0)
    tril = jnp.where(causal, 1.0, 0.0)

    def prepare(c):
        here = at(c)
        gates = gates_s[here, :]
        sums = jnp.dot(tril, gates, precision=HIGHEST, preferred_element_type=jnp.float32)
        chains = []
        for h in range(heads):
            cut = slice(h * width, (h + 1) * width)
            k, q = proj[KEY, here, cut], proj[QUERY, here, cut]
            v = proj[VALUE, here, cut].astype(jnp.float32)
            kf, qf = k.astype(jnp.float32), q.astype(jnp.float32)
            ik = lax.rsqrt(jnp.sum(kf * kf, axis=-1, keepdims=True) + TINY_NORM)
            iq = lax.rsqrt(jnp.sum(qf * qf, axis=-1, keepdims=True) + TINY_NORM)
            iq = iq * width ** (-0.5)
            beta = gates[:, h : h + 1]
            log_sum = sums[:, heads + h : heads + h + 1]
            log_full = jnp.broadcast_to(log_sum, (BLOCK, BLOCK))
            spread = log_full - log_full.T
            damp = jnp.where(causal, jnp.exp(jnp.where(causal, spread, 0.0)), 0.0)
            damp = damp * jnp.broadcast_to(ik, (BLOCK, BLOCK)).T
            lower = jnp.where(strict, nt(k, k) * damp * (beta * ik), 0.0)
            score_s[h, here, :] = (nt(q, k) * damp * iq).astype(jnp.bfloat16)
            grow = jnp.exp(log_sum)
            right = jnp.concatenate([v * beta, kf * (beta * ik * grow)], axis=1)
            tail = log_full[BLOCK - 1 : BLOCK, :]
            weighted = kf * (ik * jnp.exp(tail[:, :1] - log_sum))
            wt_s[h, c] = weighted.T.astype(jnp.bfloat16)
            tail_s[h, c] = jnp.broadcast_to(jnp.exp(tail), (8, BLOCK))
            lhs_s[h, c, BLOCK:, :] = (qf * (iq * grow)).astype(jnp.bfloat16)
            chains.append([h, lower, right, eye - jnp.where(differ == 1, lower, 0.0)])
        return here, c, chains

    def blocks_steps(first, count):
        prepared = [prepare(first + i) for i in range(count)]
        yield
        size = 2
        while size < BLOCK:
            level = (differ >= size) & (differ < 2 * size)
            parts = [
                [mm(jnp.where(level, ch[1], 0.0), ch[3]) for ch in item[2]] for item in prepared
            ]
            yield
            for item, moves in zip(prepared, parts):
                for ch, moved in zip(item[2], moves):
                    ch[3] = ch[3] - mm(ch[3], moved)
            size *= 2
            yield
        for here, c, chains in prepared:
            for h, lower, right, inverse in chains:
                solved = mm(inverse, right)
                corr_s[h, here, :] = solved[:, :width]
                lhs_s[h, c, :BLOCK, :] = solved[:, width:].astype(jnp.bfloat16)

    def advance_steps(c):
        here = at(c)
        boths = [mm(lhs_s[h, c], state_ref[h]) for h in range(heads)]
        fresh = []
        for h in range(heads):
            first = boths[h][:BLOCK]
            fresh.append(
                jnp.concatenate(
                    [-first[:, :width], corr_s[h, here, :] - first[:, width:]], axis=1
                ).astype(jnp.bfloat16)
            )
        yield
        for h in range(heads):
            decay = tail_s[h, c][:1, :]
            decay = jnp.concatenate([decay, decay], axis=1)
            state_ref[h] = state_ref[h] * decay + mm(wt_s[h, c], fresh[h])
        for h in range(heads):
            out = boths[h][BLOCK:] + mm(score_s[h, here, :], fresh[h])
            outa_ref[h, here, :] = out[:, :width].astype(jnp.bfloat16)
            outb_ref[h, here, :] = out[:, width:]
        yield

    def in_turn(*steps):
        steps = list(steps)
        while steps:
            for step in list(steps):
                if next(step, step) is step:
                    steps.remove(step)

    def one_by_one(*steps):
        for step in steps:
            yield from step

    def unit(t):
        value = proj[GLU_VALUE, at(t), :].astype(jnp.float32)
        gate = proj[GLU_GATE, at(t), :].astype(jnp.float32)
        units = (value * jax.nn.sigmoid(gate)).astype(jnp.bfloat16)
        wide = units.astype(jnp.float32)
        for g in range(groups):
            padded[g, pl.ds(pl.multiple_of(t * BLOCK + halo, halo), BLOCK), :] = wide[
                :, g * lanes : (g + 1) * lanes
            ]
        return units

    def conv(t, carry=0):
        first = jnp.zeros((BLOCK, 1), jnp.float32)
        second = jnp.zeros((BLOCK, 1), jnp.float32)
        for g in range(groups):
            total = jnp.zeros((BLOCK, lanes), jnp.float32)
            for j in range(kernel):
                start = t * BLOCK + (halo - kernel + 1 + j)
                tap = taps_ref[j : j + 1, g * lanes : (g + 1) * lanes]
                total = total + padded[g, pl.ds(start, BLOCK), :] * tap
            filtered[g, at(t), :] = total
            first = first + jnp.sum(total, axis=1, keepdims=True)
            second = second + jnp.sum(total * total, axis=1, keepdims=True)
        lane = lax.broadcasted_iota(jnp.int32, (BLOCK, BLOCK), 1)
        sums_out[t] = jnp.where(lane == 0, first, jnp.where(lane == 1, second, 0.0)).T[:8, :]
        return carry

    for h in range(heads):
        state_ref[h] = jnp.concatenate([eye, jnp.zeros((width, width), jnp.float32)], axis=1)
    for load in w_loads:
        load.wait()
    spread_weights()

    def filter_tiles(first, count):
        for n in range(count):
            unit(first + n)

        def filter_tile(t, carry):
            @pl.when(t > 0)
            def _():
                conv(t)

            return carry

        lax.fori_loop(first, first + count, filter_tile, 0)

    def pair(i, carry):
        receive(2 * i, 2)
        in_turn(project_steps(2 * i, 2))
        relay_weights(i + 1)
        in_turn(blocks_steps(2 * i, 2))
        in_turn(one_by_one(advance_steps(2 * i), advance_steps(2 * i + 1)))
        filter_tiles(2 * i, 2)
        return carry

    tail = tiles - 4
    lax.fori_loop(0, tail // 2, pair, 0)
    receive(tail, 2)
    in_turn(project_steps(tail, 2))
    filter_tiles(tail, 2)
    for step in range(tail // 2 + 1, line):
        relay_weights(step)
    receive(tail + 2, 2)
    in_turn(blocks_steps(tail, 2), project_steps(tail + 2, 2))
    for n in range(2):
        units = unit(tail + 2 + n)
    halo_out[...] = units[BLOCK - halo :, :]
    halo_copy = to_sp(
        halo_out, halo_in, halo_send.at[0], halo_recv.at[0], jnp.minimum(place + 1, sp - 1)
    )

    @pl.when(place + 1 < sp)
    def _():
        halo_copy.start()

    in_turn(
        blocks_steps(tail + 2, 2), one_by_one(advance_steps(tail), advance_steps(tail + 1))
    )
    in_turn(one_by_one(advance_steps(tail + 2), advance_steps(tail + 3)))
    final_ref[...] = state_ref[...].astype(jnp.bfloat16)

    def carry_copy(i, h):
        cut = slice(width, 2 * width) if i == last else slice(0, 2 * width)
        source = final_ref if i == 0 else sent_s.at[i - 1]
        return to_sp(
            source.at[h, :, cut], far_s.at[i, h, :, cut], far_send.at[i, h], far_recv.at[i, h],
            jnp.minimum(place + reaches[i], sp - 1),
        )

    def send_carry(i, h):
        @pl.when(place + reaches[i] < sp)
        def _():
            carry_copy(i, h).start()

    def take_carry(i, h):
        @pl.when(place >= reaches[i])
        def _():
            carry_copy(i, h).wait_recv()

        @pl.when(place < reaches[i])
        def _():
            far_s[i, h] = jnp.zeros((width, 2 * width), jnp.bfloat16)

    def combine(later, earlier):
        moved = mm(later[:, :width], earlier)
        return jnp.concatenate(
            [moved[:, :width], moved[:, width:] + later[:, width:].astype(jnp.float32)], axis=1
        )

    def exchange(i):
        for h in range(heads):
            take_carry(i, h)
            own = final_ref[h] if i == 0 else sent_s[i - 1, h]
            sent_s[i, h] = combine(own, far_s[i, h]).astype(jnp.bfloat16)
            send_carry(i + 1, h)
        for h in range(heads):
            if i == 0:
                window_s[h] = far_s[i, h].astype(jnp.float32)
            else:
                window_s[h] = combine(window_s[h], far_s[i, h])

    for h in range(heads):
        send_carry(0, h)

    lax.fori_loop(tail + 2, tail + 4, conv, 0)

    @pl.when(place >= 1)
    def _():
        halo_copy.wait_recv()

    @pl.when(place < 1)
    def _():
        halo_in[...] = jnp.zeros(halo_in.shape, jnp.bfloat16)

    before = halo_in[...].astype(jnp.float32)
    for g in range(groups):
        padded[g, :halo, :] = before[:, g * lanes : (g + 1) * lanes]
    conv(0)

    def ln_copy(step):
        return to_tp(
            sums_out, sums_in.at[step - 1], ln_send.at[step - 1], ln_recv.at[step - 1],
            lax.rem(me + step, tp),
        )

    for step in range(1, tp):
        ln_copy(step).start()
    if last > 0:
        exchange(0)
    for step in range(1, tp):
        ln_copy(step).wait_recv()
    channels = groups * lanes * tp
    per = tiles // tp

    def mixed_copy(kind, there):
        return to_tp(
            mixed_out.at[kind, there], mixed_in.at[kind, me],
            mix_send.at[kind, there], mix_recv.at[kind, me], there,
        )

    def mixed_wait(kind, source):
        to_tp(
            mixed_out.at[kind, source], mixed_in.at[kind, source],
            mix_send.at[kind, source], mix_recv.at[kind, source], source,
        ).wait_recv()

    far_targets = [
        lax.rem(chip + o, chips) * 2 + lax.rem(core + c, 2) for o in range(1, chips) for c in (0, 1)
    ]

    def norm(target):
        def tile(i, carry):
            t = target * per + i
            here = pl.ds(pl.multiple_of(i * BLOCK, BLOCK), BLOCK)
            sums = sums_out[t]
            for step in range(1, tp):
                sums = sums + sums_in[step - 1, t]
            sums = jnp.concatenate([sums, jnp.zeros((BLOCK - 8, BLOCK), jnp.float32)], axis=0).T
            center = sums[:, 0:1] / channels
            variance = jnp.maximum(sums[:, 1:2] / channels - center * center, 0.0)
            scale = lax.rsqrt(variance + TINY_VAR)
            for g in range(groups):
                cut = slice(g * lanes, (g + 1) * lanes)
                normed = (filtered[g, at(t), :] - center) * scale
                normed = normed * ln_gain_ref[:, cut] + ln_shift_ref[:, cut]
                gate = proj[CONV_GATE, at(t), cut].astype(jnp.float32)
                mixed_out[1, target, here, cut] = (
                    jax.nn.silu(normed) * jax.nn.silu(gate)
                ).astype(jnp.bfloat16)
            return carry

        lax.fori_loop(0, per, tile, 0)

    for target in far_targets + [sibling]:
        norm(target)
        mixed_copy(1, target).start()
    norm(me)
    for i in range(1, last):
        exchange(i)
    collect_weights()

    def out_columns(n):
        return pl.ds(pl.multiple_of(n * OUT_CUT, OUT_CUT), OUT_CUT)

    cuts = out_ref.shape[1] // OUT_CUT
    sources = [sibling] + far_targets
    def conv_part(n, carry):
        total = jnp.dot(
            mixed_out[1, me], wfull[1, me, :, out_columns(n)], preferred_element_type=jnp.float32
        )
        for source in sources:
            total = total + jnp.dot(
                mixed_in[1, source], wfull[1, source, :, out_columns(n)],
                preferred_element_type=jnp.float32,
            )
        acc_s[:, out_columns(n)] = total
        return carry


    carried = []
    for h in range(heads):
        take_carry(last, h)
        earlier = far_s[last, h, :, width:]
        if last > 0:
            window = window_s[h]
            earlier = mm(window[:, :width], earlier) + window[:, width:]
        carried.append(earlier.astype(jnp.bfloat16))

    def attend(target):
        def tile(i, carry):
            t = target * per + i
            here = pl.ds(pl.multiple_of(i * BLOCK, BLOCK), BLOCK)
            for h in range(heads):
                cut = slice(h * width, (h + 1) * width)
                result = outb_ref[h, at(t), :] + mm(outa_ref[h, at(t), :], carried[h])
                result = result * lax.rsqrt(
                    jnp.mean(result * result, axis=-1, keepdims=True) + TINY_NORM
                )
                gate = proj[DELTA_GATE, at(t), cut].astype(jnp.float32)
                mixed_out[0, target, here, cut] = (
                    result * gain_ref[...] * jax.nn.silu(gate)
                ).astype(jnp.bfloat16)
            return carry

        lax.fori_loop(0, per, tile, 0)

    for target in far_targets + [sibling]:
        attend(target)
        mixed_copy(0, target).start()
    attend(me)
    for source in sources:
        mixed_wait(1, source)
    weights_beside().wait_recv()
    for o in range(1, chips):
        weights_forward(o).wait_recv()
    lax.fori_loop(0, cuts, conv_part, 0)
    mixed_wait(0, sibling)

    def near_part(n, carry):
        total = jnp.dot(
            mixed_out[0, me], wfull[0, me, :, out_columns(n)], preferred_element_type=jnp.float32
        )
        total = total + jnp.dot(
            mixed_in[0, sibling], wfull[0, sibling, :, out_columns(n)],
            preferred_element_type=jnp.float32,
        )
        acc_s[:, out_columns(n)] = acc_s[:, out_columns(n)] + total
        return carry

    lax.fori_loop(0, cuts, near_part, 0)
    for index, source in enumerate(far_targets):
        mixed_wait(0, source)

        def far_part(n, carry, source=source, closing=index + 1 == len(far_targets)):
            total = acc_s[:, out_columns(n)] + jnp.dot(
                mixed_in[0, source], wfull[0, source, :, out_columns(n)],
                preferred_element_type=jnp.float32,
            )
            if closing:
                out_ref[:, out_columns(n)] = total.astype(jnp.bfloat16)
            else:
                acc_s[:, out_columns(n)] = total
            return carry

        lax.fori_loop(0, cuts, far_part, 0)

    for r in range(tiles):
        for o in range(1, chips):
            across(o, r).wait_send()
            forward(o, r).wait_send()
        beside(r).wait_send()
    weights_beside().wait_send()
    for o in range(1, chips):
        weights_across(o).wait_send()
        weights_forward(o).wait_send()
        for j in range(line):
            weights_pair(o, j, side).wait_send()
    for origin in range(line):
        for up in (True, False):
            @pl.when((origin <= spot) & (spot + 1 < line) if up else (origin >= spot) & (spot >= 1))
            def _(origin=origin, up=up):
                for o in range(1, chips):
                    weights_along(o, origin, up).wait_send()

    for i in range(last + 1):
        @pl.when(place + reaches[i] < sp)
        def _(i=i):
            for h in range(heads):
                carry_copy(i, h).wait_send()

    @pl.when(place + 1 < sp)
    def _():
        halo_copy.wait_send()

    for step in range(1, tp):
        ln_copy(step).wait_send()
    for kind in range(2):
        for target in sources:
            mixed_copy(kind, target).wait_send()


def layer(tokens, weights, w_beta, w_decay, decay_log, gain, taps, ln_gain, ln_shift, out_delta, out_conv):
    rows, part = tokens.shape
    width = gain.shape[1]
    features, held = weights[0].shape
    heads = held // width
    channels = taps.shape[1]
    depth, columns = out_delta.shape
    kernel = taps.shape[0]
    halo = (kernel - 1 + 31) // 32 * 32
    lanes = min(channels, 128)
    groups = channels // lanes
    sp, tp = lax.axis_size("sp"), lax.axis_size("tp")
    others = max(tp // 2 - 1, 1)
    line = sp // 2
    steps = 1
    while 2**steps < sp:
        steps += 1
    tiles = rows // BLOCK
    slot = rows // tp
    dma = pltpu.SemaphoreType.DMA
    pair = (heads, width, 2 * width)
    bf16, f32 = jnp.bfloat16, jnp.float32
    vmem = pltpu.VMEM
    return pl.pallas_call(
        functools.partial(layer_kernel, heads, width),
        out_shape=jax.ShapeDtypeStruct((slot, columns), bf16),
        in_specs=[pl.BlockSpec(memory_space=pltpu.HBM)] * 17,
        out_specs=pl.BlockSpec(memory_space=pltpu.VMEM),
        scratch_shapes=[
            vmem((rows, features), bf16),
            vmem((PROJECTIONS, features, held), bf16),
            vmem(w_beta.shape, bf16),
            vmem(w_decay.shape, bf16),
            vmem(decay_log.shape, f32),
            vmem(gain.shape, f32),
            vmem(taps.shape, bf16),
            vmem(ln_gain.shape, f32),
            vmem(ln_shift.shape, f32),
            vmem((BLOCK, features), bf16),
            vmem((1, BLOCK), f32),
            vmem(taps.shape, f32),
            vmem((PROJECTIONS, rows, held), bf16),
            vmem((rows, BLOCK), f32),
            vmem((2, tp, depth, columns), bf16),
            vmem((heads, tiles, 2 * BLOCK, width), bf16),
            vmem((heads, rows, width), f32),
            vmem((heads, rows, BLOCK), bf16),
            vmem((heads, tiles, width, BLOCK), bf16),
            vmem((heads, tiles, 8, BLOCK), f32),
            vmem(pair, f32),
            vmem((heads, rows, width), bf16),
            vmem((heads, rows, width), f32),
            vmem(pair, bf16),
            vmem((groups, halo + rows, lanes), f32),
            vmem((groups, rows, lanes), f32),
            vmem((halo, channels), bf16),
            vmem((halo, channels), bf16),
            vmem((tiles, 8, BLOCK), f32),
            vmem((tp - 1, tiles, 8, BLOCK), f32),
            vmem(pair, f32),
            vmem((steps,) + pair, bf16),
            vmem((steps,) + pair, bf16),
            vmem((2, tp, slot, channels), bf16),
            vmem((2, tp, slot, channels), bf16),
            vmem((slot, columns), f32),
            dma((tiles,)),
            dma((PROJECTIONS,)),
            dma((7,)),
            dma((2,)),
            dma((others, tiles)),
            dma((others, tiles)),
            dma((tiles,)),
            dma((tiles,)),
            dma((others, tiles)),
            dma((others, tiles)),
            dma((1,)),
            dma((1,)),
            dma((others,)),
            dma((others,)),
            dma((others, 2, line)),
            dma((others, line)),
            dma((others, line)),
            dma((others, line)),
            dma((others,)),
            dma((others,)),
            dma((steps, heads)),
            dma((steps, heads)),
            dma((1,)),
            dma((1,)),
            dma((tp - 1,)),
            dma((tp - 1,)),
            dma((2, tp)),
            dma((2, tp)),
        ],
        compiler_params=pltpu.CompilerParams(
            collective_id=0, has_side_effects=True, vmem_limit_bytes=46 * 1024 * 1024
        ),
        cost_estimate=pl.CostEstimate(
            flops=20_000_000_000, bytes_accessed=20_000_000, transcendentals=0
        ),
        name="layer",
    )(
        *(
            pltpu.with_memory_space_constraint(x, pltpu.HBM)
            for x in (
                tokens, *weights, w_beta, w_decay, decay_log, gain, taps, ln_gain, ln_shift,
                out_delta, out_conv,
            )
        )
    )


def local(
    tokens,
    w_query,
    w_key,
    w_value,
    w_delta_gate,
    w_glu_value,
    w_glu_gate,
    w_conv_gate,
    w_beta,
    w_decay,
    decay_log,
    head_gain,
    conv_taps,
    ln_gain,
    ln_shift,
    out_delta,
    out_conv,
):
    weights = (w_query, w_key, w_value, w_delta_gate, w_glu_value, w_glu_gate, w_conv_gate)
    return layer(
        tokens,
        weights,
        w_beta.T,
        w_decay.T,
        decay_log[None, :],
        head_gain[None, :],
        conv_taps,
        ln_gain[None, :],
        ln_shift[None, :],
        out_delta,
        out_conv,
    )


def solution(mesh):
    return jax.shard_map(
        local,
        mesh=mesh,
        in_specs=(
            P("sp", "tp"),
            P(None, "tp"),
            P(None, "tp"),
            P(None, "tp"),
            P(None, "tp"),
            P(None, "tp"),
            P(None, "tp"),
            P(None, "tp"),
            P(),
            P(),
            P(),
            P(),
            P(None, "tp"),
            P("tp"),
            P("tp"),
            P("tp", None),
            P("tp", None),
        ),
        out_specs=P(("sp", "tp"), None),
        check_vma=False,
    )
```

```python
import functools

import jax
import jax.numpy as jnp
from jax import lax
from jax.experimental import pallas as pl
from jax.experimental.pallas import tpu as pltpu
from jax.sharding import PartitionSpec as P

BLOCK = 128
PROJECTIONS = 7
QUERY, KEY, VALUE, DELTA_GATE, GLU_VALUE, GLU_GATE, CONV_GATE = range(PROJECTIONS)
OUT_CUT = 512
TINY_NORM = 1e-06
TINY_VAR = 1e-05
HIGHEST = lax.Precision.HIGHEST
MESH = pl.DeviceIdType.MESH


def nt(a, b):
    return lax.dot_general(a, b, (((1,), (1,)), ((), ())), preferred_element_type=jnp.float32)


def mm(a, b):
    return jnp.dot(
        a.astype(jnp.bfloat16), b.astype(jnp.bfloat16), preferred_element_type=jnp.float32
    )


def slice_shape(rows, columns, pieces):
    high = max(16, rows // pieces)
    across = pieces // (rows // high)
    return high, columns // across, across


def layer_kernel(
    heads, width,
    tok_hbm, wq_hbm, wk_hbm, wv_hbm, wdg_hbm, wgv_hbm, wgg_hbm, wcg_hbm,
    beta_hbm, decay_hbm, rate_hbm, gain_hbm, taps_hbm, ln_gain_hbm, ln_shift_hbm,
    out_delta_hbm, out_conv_hbm,
    out_ref,
    full, w_s, beta_s, decay_s, rate_s, gain_ref, taps_s, ln_gain_ref, ln_shift_ref,
    wg_s, rate_row, taps_ref, proj, gates_s, wfull,
    lhs_s, corr_s, score_s, wt_s, tail_s, state_ref, outa_ref, outb_ref, final_ref,
    padded, filtered, halo_out, halo_in, sums_out, sums_in, window_s, sent_s, far_s,
    mixed_out, mixed_in, acc_s,
    tok_sem, w_sem, small_sem, ow_sem,
    y_send, y_recv, own_send, own_recv, fwd_send, fwd_recv,
    wo_send, wo_recv, wy_send, wy_recv, wl_send, wl_recv, wx_send, wx_recv, wb_send, wb_recv,
    far_send, far_recv, halo_send, halo_recv, ln_send, ln_recv, mix_send, mix_recv,
):
    rows = full.shape[0]
    tp, me = lax.axis_size("tp"), lax.axis_index("tp")
    sp, place = lax.axis_size("sp"), lax.axis_index("sp")
    part = full.shape[1] // tp
    chips = tp // 2
    core = lax.rem(me, 2)
    chip = me // 2
    sibling = me + 1 - 2 * core
    tiles = rows // BLOCK
    halo = halo_in.shape[0]
    lanes = padded.shape[2]
    groups = padded.shape[0]
    kernel = taps_s.shape[0]
    line = sp // 2
    spot = place // 2
    side = lax.rem(place, 2)

    def at(t, count=1):
        return pl.ds(pl.multiple_of(t * BLOCK, BLOCK), count * BLOCK)

    def columns(owner):
        return pl.ds(pl.multiple_of(owner * part, part), part)

    token_loads = [
        pltpu.make_async_copy(
            tok_hbm.at[at(r), :], full.at[at(r), columns(me)], tok_sem.at[r]
        )
        for r in range(tiles)
    ]
    out_loads = [
        pltpu.make_async_copy(src, wfull.at[i, me], ow_sem.at[i])
        for i, src in enumerate((out_delta_hbm, out_conv_hbm))
    ]
    w_loads = [
        pltpu.make_async_copy(src, w_s.at[i], w_sem.at[i])
        for i, src in enumerate((wq_hbm, wk_hbm, wv_hbm, wdg_hbm, wgv_hbm, wgg_hbm, wcg_hbm))
    ]
    small_loads = [
        pltpu.make_async_copy(src, dst, small_sem.at[i])
        for i, (src, dst) in enumerate((
            (beta_hbm, beta_s), (decay_hbm, decay_s), (rate_hbm, rate_s), (gain_hbm, gain_ref),
            (taps_hbm, taps_s), (ln_gain_hbm, ln_gain_ref), (ln_shift_hbm, ln_shift_ref),
        ))
    ]
    for load in out_loads + token_loads + small_loads:
        load.start()

    reaches = [1]
    while 2 * reaches[-1] < sp:
        reaches.append(2 * reaches[-1])
    last = len(reaches) - 1
    barrier = pltpu.get_barrier_semaphore()
    expected = tp - 1
    for step in range(1, tp):
        pl.semaphore_signal(
            barrier, inc=1, device_id={"tp": lax.rem(me + step, tp)}, device_id_type=MESH
        )
    for step in reaches:
        ahead, behind = place + step < sp, place >= step

        @pl.when(ahead)
        def _(step=step):
            pl.semaphore_signal(
                barrier, inc=1, device_id={"sp": place + step}, device_id_type=MESH
            )

        @pl.when(behind)
        def _(step=step):
            pl.semaphore_signal(
                barrier, inc=1, device_id={"sp": place - step}, device_id_type=MESH
            )

        expected = expected + ahead.astype(jnp.int32) + behind.astype(jnp.int32)
    pl.semaphore_wait(barrier, expected)

    def to_tp(src, dst, send, recv, there):
        return pltpu.make_async_remote_copy(
            src_ref=src, dst_ref=dst, send_sem=send, recv_sem=recv,
            device_id={"tp": there}, device_id_type=MESH,
        )

    def to_sp(src, dst, send, recv, there):
        return pltpu.make_async_remote_copy(
            src_ref=src, dst_ref=dst, send_sem=send, recv_sem=recv,
            device_id={"sp": there}, device_id_type=MESH,
        )

    def far_peer(o):
        return lax.rem(chip + o, chips) * 2 + core

    def far_owner(o):
        return lax.rem(chip - o + chips, chips) * 2 + core

    def across(o, r):
        block = full.at[at(r), columns(me)]
        return to_tp(block, block, y_send.at[o - 1, r], y_recv.at[o - 1, r], far_peer(o))

    def beside(r):
        block = full.at[at(r), columns(me)]
        return to_tp(block, block, own_send.at[r], own_recv.at[r], sibling)

    def forward(o, r):
        block = full.at[at(r), columns(far_owner(o))]
        return to_tp(block, block, fwd_send.at[o - 1, r], fwd_recv.at[o - 1, r], sibling)

    high, broad, split = slice_shape(wfull.shape[2], wfull.shape[3], sp)

    def weight_slice(owner, index):
        top = pl.ds(pl.multiple_of(index // split * high, high), high)
        left = pl.ds(pl.multiple_of(lax.rem(index, split) * broad, broad), broad)
        return wfull.at[:, owner, top, left]

    def weights_beside():
        return to_tp(wfull.at[:, me], wfull.at[:, me], wo_send.at[0], wo_recv.at[0], sibling)

    def weights_across(o):
        piece = weight_slice(me, place)
        return to_tp(piece, piece, wy_send.at[o - 1], wy_recv.at[o - 1], far_peer(o))

    def weights_along(o, origin, up):
        piece = weight_slice(far_owner(o), 2 * origin + side)
        there = jnp.clip(spot + (1 if up else -1), 0, line - 1)
        return to_sp(
            piece, piece, wl_send.at[o - 1, int(up), origin], wl_recv.at[o - 1, origin],
            2 * there + side,
        )

    def weights_pair(o, j, parity):
        piece = weight_slice(far_owner(o), 2 * j + parity)
        return to_sp(
            piece, piece, wx_send.at[o - 1, j], wx_recv.at[o - 1, j], place + 1 - 2 * side
        )

    def weights_forward(o):
        block = wfull.at[:, far_owner(o)]
        return to_tp(block, block, wb_send.at[o - 1], wb_recv.at[o - 1], sibling)

    def pass_on(origin, up, arrived):
        for o in range(1, chips):
            if arrived:
                weights_along(o, origin, up).wait_recv()

            @pl.when(spot + 1 < line if up else spot >= 1)
            def _(o=o):
                weights_along(o, origin, up).start()

            if arrived:
                weights_pair(o, origin, side).start()

    def spread_weights():
        for o in range(1, chips):
            weights_across(o).wait_recv()
        pass_on(spot, True, False)
        pass_on(spot, False, False)
        for o in range(1, chips):
            weights_pair(o, spot, side).start()

    def relay_weights(step):
        @pl.when(spot >= step)
        def _():
            pass_on(jnp.maximum(spot - step, 0), True, True)

        @pl.when(spot + step < line)
        def _():
            pass_on(jnp.minimum(spot + step, line - 1), False, True)

    def collect_weights():
        for o in range(1, chips):
            for j in range(line):
                weights_pair(o, j, 1 - side).wait_recv()
            weights_forward(o).start()

    for load in out_loads:
        load.wait()
    for o in range(1, chips):
        weights_across(o).start()
    for r in range(tiles):
        token_loads[r].wait()
        for o in range(1, chips):
            across(o, r).start()
        beside(r).start()
    for load in w_loads:
        load.start()
    for load in small_loads:
        load.wait()

    first_head = me * heads
    total_heads = beta_s.shape[0]
    lane_row = lax.broadcasted_iota(jnp.int32, (1, BLOCK), 1)
    rate = jnp.zeros((1, BLOCK), jnp.float32)
    for h in range(total_heads):
        value = jnp.exp(jnp.broadcast_to(rate_s[:, h : h + 1], (1, BLOCK)))
        rate = jnp.where(lane_row == h - first_head + heads, value, rate)
    rate = jnp.where((lane_row >= heads) & (lane_row < 2 * heads), rate, 0.0)
    rate_row[...] = rate
    pick_row = lax.broadcasted_iota(jnp.int32, (BLOCK, total_heads), 0)
    pick_col = lax.broadcasted_iota(jnp.int32, (BLOCK, total_heads), 1)
    pick_beta = (pick_row < heads) & (pick_col == pick_row + first_head)
    pick_decay = (
        (pick_row >= heads) & (pick_row < 2 * heads) & (pick_col == pick_row - heads + first_head)
    )
    wg_s[...] = (
        mm(jnp.where(pick_beta, 1.0, 0.0), beta_s[...])
        + mm(jnp.where(pick_decay, 1.0, 0.0), decay_s[...])
    ).astype(jnp.bfloat16)
    taps_ref[...] = taps_s[...].astype(jnp.float32)

    def pass_tokens(first, count):
        for i in range(count):
            for o in range(1, chips):
                across(o, first + i).wait_recv()
                forward(o, first + i).start()

    def take_tokens(first, count):
        for i in range(count):
            beside(first + i).wait_recv()
            for o in range(1, chips):
                forward(o, first + i).wait_recv()

    def project_steps(first, count):
        size = count * BLOCK
        here = at(first, count)
        squares = jnp.zeros((size, 1), jnp.float32)
        for b in range(tp):
            piece = full[here, b * part : (b + 1) * part].astype(jnp.float32)
            squares = squares + jnp.sum(piece * piece, axis=1, keepdims=True)
        inv_rms = lax.rsqrt(squares / (part * tp) + TINY_NORM)
        raw = nt(full[here, :], wg_s[...]) * inv_rms
        lane = lax.broadcasted_iota(jnp.int32, raw.shape, 1)
        softplus = jnp.maximum(raw, 0.0) + jnp.log1p(jnp.exp(-jnp.abs(raw)))
        gates_s[here, :] = jnp.where(
            lane < heads, jax.nn.sigmoid(raw), -rate_row[...] * softplus
        )
        yield
        for i in range(PROJECTIONS):
            summed = jnp.dot(full[here, :], w_s[i], preferred_element_type=jnp.float32)
            proj[i, here, :] = (summed * inv_rms).astype(jnp.bfloat16)
            yield

    row_id = lax.broadcasted_iota(jnp.int32, (BLOCK, BLOCK), 0)
    col_id = lax.broadcasted_iota(jnp.int32, (BLOCK, BLOCK), 1)
    causal = row_id >= col_id
    strict = row_id > col_id
    differ = row_id ^ col_id
    eye = jnp.where(row_id == col_id, 1.0, 0.0)
    tril = jnp.where(causal, 1.0, 0.0)

    def prepare(c):
        here = at(c)
        gates = gates_s[here, :]
        sums = jnp.dot(tril, gates, precision=HIGHEST, preferred_element_type=jnp.float32)
        chains = []
        for h in range(heads):
            cut = slice(h * width, (h + 1) * width)
            k, q = proj[KEY, here, cut], proj[QUERY, here, cut]
            v = proj[VALUE, here, cut].astype(jnp.float32)
            kf, qf = k.astype(jnp.float32), q.astype(jnp.float32)
            ik = lax.rsqrt(jnp.sum(kf * kf, axis=-1, keepdims=True) + TINY_NORM)
            iq = lax.rsqrt(jnp.sum(qf * qf, axis=-1, keepdims=True) + TINY_NORM)
            iq = iq * width ** (-0.5)
            beta = gates[:, h : h + 1]
            log_sum = sums[:, heads + h : heads + h + 1]
            log_full = jnp.broadcast_to(log_sum, (BLOCK, BLOCK))
            spread = log_full - log_full.T
            damp = jnp.where(causal, jnp.exp(jnp.where(causal, spread, 0.0)), 0.0)
            damp = damp * jnp.broadcast_to(ik, (BLOCK, BLOCK)).T
            lower = jnp.where(strict, nt(k, k) * damp * (beta * ik), 0.0)
            score_s[h, here, :] = (nt(q, k) * damp * iq).astype(jnp.bfloat16)
            grow = jnp.exp(log_sum)
            right = jnp.concatenate([v * beta, kf * (beta * ik * grow)], axis=1)
            tail = log_full[BLOCK - 1 : BLOCK, :]
            weighted = kf * (ik * jnp.exp(tail[:, :1] - log_sum))
            wt_s[h, c] = weighted.T.astype(jnp.bfloat16)
            tail_s[h, c] = jnp.broadcast_to(jnp.exp(tail), (8, BLOCK))
            lhs_s[h, c, BLOCK:, :] = (qf * (iq * grow)).astype(jnp.bfloat16)
            chains.append([h, lower, right, eye - jnp.where(differ == 1, lower, 0.0)])
        return here, c, chains

    def blocks_steps(first, count):
        prepared = [prepare(first + i) for i in range(count)]
        yield
        size = 2
        while size < BLOCK:
            level = (differ >= size) & (differ < 2 * size)
            parts = [
                [mm(jnp.where(level, ch[1], 0.0), ch[3]) for ch in item[2]] for item in prepared
            ]
            yield
            for item, moves in zip(prepared, parts):
                for ch, moved in zip(item[2], moves):
                    ch[3] = ch[3] - mm(ch[3], moved)
            size *= 2
            yield
        for here, c, chains in prepared:
            for h, lower, right, inverse in chains:
                solved = mm(inverse, right)
                corr_s[h, here, :] = solved[:, :width]
                lhs_s[h, c, :BLOCK, :] = solved[:, width:].astype(jnp.bfloat16)

    def advance_steps(c):
        here = at(c)
        boths = [mm(lhs_s[h, c], state_ref[h]) for h in range(heads)]
        fresh = []
        for h in range(heads):
            first = boths[h][:BLOCK]
            fresh.append(
                jnp.concatenate(
                    [-first[:, :width], corr_s[h, here, :] - first[:, width:]], axis=1
                ).astype(jnp.bfloat16)
            )
        yield
        for h in range(heads):
            decay = tail_s[h, c][:1, :]
            decay = jnp.concatenate([decay, decay], axis=1)
            state_ref[h] = state_ref[h] * decay + mm(wt_s[h, c], fresh[h])
        for h in range(heads):
            out = boths[h][BLOCK:] + mm(score_s[h, here, :], fresh[h])
            outa_ref[h, here, :] = out[:, :width].astype(jnp.bfloat16)
            outb_ref[h, here, :] = out[:, width:]
        yield

    def in_turn(*steps):
        steps = list(steps)
        while steps:
            for step in list(steps):
                if next(step, step) is step:
                    steps.remove(step)

    def one_by_one(*steps):
        for step in steps:
            yield from step

    def unit(t):
        value = proj[GLU_VALUE, at(t), :].astype(jnp.float32)
        gate = proj[GLU_GATE, at(t), :].astype(jnp.float32)
        units = (value * jax.nn.sigmoid(gate)).astype(jnp.bfloat16)
        wide = units.astype(jnp.float32)
        for g in range(groups):
            padded[g, pl.ds(pl.multiple_of(t * BLOCK + halo, halo), BLOCK), :] = wide[
                :, g * lanes : (g + 1) * lanes
            ]
        return units

    def conv_steps(t):
        first = jnp.zeros((BLOCK, 1), jnp.float32)
        second = jnp.zeros((BLOCK, 1), jnp.float32)
        for g in range(groups):
            total = jnp.zeros((BLOCK, lanes), jnp.float32)
            for j in range(kernel):
                start = t * BLOCK + (halo - kernel + 1 + j)
                tap = taps_ref[j : j + 1, g * lanes : (g + 1) * lanes]
                total = total + padded[g, pl.ds(start, BLOCK), :] * tap
            filtered[g, at(t), :] = total
            first = first + jnp.sum(total, axis=1, keepdims=True)
            second = second + jnp.sum(total * total, axis=1, keepdims=True)
            yield
        lane = lax.broadcasted_iota(jnp.int32, (BLOCK, BLOCK), 1)
        sums_out[t] = jnp.where(lane == 0, first, jnp.where(lane == 1, second, 0.0)).T[:8, :]
        yield

    def conv(t):
        for step in conv_steps(t):
            pass

    for h in range(heads):
        state_ref[h] = jnp.concatenate([eye, jnp.zeros((width, width), jnp.float32)], axis=1)
    for load in w_loads:
        load.wait()
    def filter_tiles(first, count):
        for n in range(count):
            unit(first + n)

        def filter_tile(t, carry):
            @pl.when(t > 0)
            def _():
                conv(t)

            return carry

        lax.fori_loop(first, first + count, filter_tile, 0)

    tail = tiles - 4
    ln_parts = (pl.ds(2, tail), pl.ds(0, 2), pl.ds(tail + 2, 2))

    def ln_copy(step, which):
        cut = ln_parts[which]
        return to_tp(
            sums_out.at[cut], sums_in.at[step - 1, cut],
            ln_send.at[step - 1, which], ln_recv.at[step - 1, which], lax.rem(me + step, tp),
        )

    spread_weights()
    pass_tokens(0, 2)
    take_tokens(0, 2)
    in_turn(project_steps(0, 2))
    relay_weights(1)
    filter_tiles(0, 2)
    in_turn(blocks_steps(0, 2))
    in_turn(one_by_one(advance_steps(0), advance_steps(1)))
    pass_tokens(2, 2)

    def pair(i, carry):
        take_tokens(2 * i, 2)
        in_turn(project_steps(2 * i, 2))
        filter_tiles(2 * i, 2)
        pass_tokens(2 * i + 2, 2)
        relay_weights(i + 1)
        return carry

    lax.fori_loop(1, tail // 2, pair, 0)
    take_tokens(tail, 2)
    in_turn(project_steps(tail, 2))
    filter_tiles(tail, 2)
    for step in range(1, tp):
        ln_copy(step, 0).start()
    in_turn(blocks_steps(2, tail))
    pass_tokens(tail + 2, 2)
    relay_weights(tail // 2 + 1)
    take_tokens(tail + 2, 1)
    in_turn(
        project_steps(tail + 2, 1),
        one_by_one(*(advance_steps(c) for c in range(2, tail + 2))),
    )
    take_tokens(tail + 3, 1)
    weights_beside().start()
    in_turn(project_steps(tail + 3, 1))
    for n in range(2):
        units = unit(tail + 2 + n)
    halo_out[...] = units[BLOCK - halo :, :]
    halo_copy = to_sp(
        halo_out, halo_in, halo_send.at[0], halo_recv.at[0], jnp.minimum(place + 1, sp - 1)
    )

    @pl.when(place + 1 < sp)
    def _():
        halo_copy.start()

    in_turn(blocks_steps(tail + 2, 2), one_by_one(conv_steps(tail + 2), conv_steps(tail + 3)))
    for step in range(tail // 2 + 2, line):
        relay_weights(step)

    @pl.when(place >= 1)
    def _():
        halo_copy.wait_recv()

    @pl.when(place < 1)
    def _():
        halo_in[...] = jnp.zeros(halo_in.shape, jnp.bfloat16)

    before = halo_in[...].astype(jnp.float32)
    for g in range(groups):
        padded[g, :halo, :] = before[:, g * lanes : (g + 1) * lanes]
    conv(0)

    for step in range(1, tp):
        ln_copy(step, 1).start()
        ln_copy(step, 2).start()
    in_turn(one_by_one(advance_steps(tail + 2), advance_steps(tail + 3)))
    final_ref[...] = state_ref[...].astype(jnp.bfloat16)

    shift, offset = slice(0, width), slice(width, 2 * width)

    def carry_copy(i, h, cut):
        source = final_ref if i == 0 else sent_s.at[i - 1]
        which = 0 if cut is shift else 1
        return to_sp(
            source.at[h, :, cut], far_s.at[i, h, :, cut],
            far_send.at[i, h, which], far_recv.at[i, h, which],
            jnp.minimum(place + reaches[i], sp - 1),
        )

    def send_carry(i, h, cut):
        if i == last and cut is shift:
            return

        @pl.when(place + reaches[i] < sp)
        def _():
            carry_copy(i, h, cut).start()

    def take_carry(i, h, cut):
        @pl.when(place >= reaches[i])
        def _():
            carry_copy(i, h, cut).wait_recv()

        @pl.when(place < reaches[i])
        def _():
            far_s[i, h, :, cut] = jnp.zeros((width, width), jnp.bfloat16)

    def exchange(i):
        own = final_ref if i == 0 else sent_s.at[i - 1]
        for h in range(heads):
            take_carry(i, h, offset)
            later = mm(own[h, :, shift], far_s[i, h, :, offset])
            later = later + own[h, :, offset].astype(jnp.float32)
            sent_s[i, h, :, offset] = later.astype(jnp.bfloat16)
            send_carry(i + 1, h, offset)
        for h in range(heads):
            take_carry(i, h, shift)
            sent_s[i, h, :, shift] = mm(own[h, :, shift], far_s[i, h, :, shift]).astype(
                jnp.bfloat16
            )
            send_carry(i + 1, h, shift)
        for h in range(heads):
            if i == 0:
                window_s[h] = far_s[i, h].astype(jnp.float32)
            else:
                window = window_s[h]
                moved = mm(window[:, shift], far_s[i, h])
                window_s[h] = jnp.concatenate(
                    [moved[:, shift], moved[:, offset] + window[:, offset]], axis=1
                )

    for h in range(heads):
        send_carry(0, h, offset)
    for h in range(heads):
        send_carry(0, h, shift)
    collect_weights()


    for step in range(1, tp):
        ln_copy(step, 0).wait_recv()
    channels = groups * lanes * tp
    per = tiles // tp

    def mixed_part(buffer, owner, kind):
        if kind == heads:
            return buffer.at[1, owner]
        return buffer.at[0, owner, :, kind * width : (kind + 1) * width]

    def mixed_copy(kind, there):
        return to_tp(
            mixed_part(mixed_out, there, kind), mixed_part(mixed_in, me, kind),
            mix_send.at[kind, there], mix_recv.at[kind, me], there,
        )

    def mixed_wait(kind, source):
        part_in = mixed_part(mixed_in, source, kind)
        to_tp(
            part_in, part_in, mix_send.at[kind, source], mix_recv.at[kind, source], source
        ).wait_recv()

    far_targets = [
        lax.rem(chip + o, chips) * 2 + lax.rem(core + c, 2) for o in range(1, chips) for c in (0, 1)
    ]

    def norm(targets):
        for target, i in [(target, i) for target in targets for i in range(per)]:
            t = target * per + i
            here = pl.ds(i * BLOCK, BLOCK)
            sums = sums_out[t]
            for step in range(1, tp):
                sums = sums + sums_in[step - 1, t]
            sums = jnp.concatenate([sums, jnp.zeros((BLOCK - 8, BLOCK), jnp.float32)], axis=0).T
            center = sums[:, 0:1] / channels
            variance = jnp.maximum(sums[:, 1:2] / channels - center * center, 0.0)
            scale = lax.rsqrt(variance + TINY_VAR)
            for g in range(groups):
                cut = slice(g * lanes, (g + 1) * lanes)
                normed = (filtered[g, at(t), :] - center) * scale
                normed = normed * ln_gain_ref[:, cut] + ln_shift_ref[:, cut]
                gate = proj[CONV_GATE, at(t), cut].astype(jnp.float32)
                mixed_out[1, target, here, cut] = (
                    jax.nn.silu(normed) * jax.nn.silu(gate)
                ).astype(jnp.bfloat16)

    early = [t for t in range(tp) if t * per >= 2 and (t + 1) * per <= tail + 2]

    def norm_far(target):
        @pl.when(target // 2 != chip)
        def _():
            norm([target])
            mixed_copy(heads, target).start()

    for target in early:
        norm_far(target)
    if last > 0:
        exchange(0)
    for step in range(1, tp):
        ln_copy(step, 1).wait_recv()
        ln_copy(step, 2).wait_recv()
    for target in range(tp):
        if target not in early:
            norm_far(target)
    norm([sibling])
    mixed_copy(heads, sibling).start()
    norm([me])
    for i in range(1, last):
        exchange(i)

    def out_columns(n):
        return pl.ds(pl.multiple_of(n * OUT_CUT, OUT_CUT), OUT_CUT)

    cuts = out_ref.shape[1] // OUT_CUT
    sources = [sibling] + far_targets

    def product(terms, head=None, start=False, close=False):
        def part(n, carry):
            total = jnp.zeros((out_ref.shape[0], OUT_CUT), jnp.float32)
            for kind, source, rows_ref in terms:
                total = total + jnp.dot(
                    rows_ref[kind, source], wfull[kind, source, :, out_columns(n)],
                    preferred_element_type=jnp.float32,
                )
            if head is not None:
                cut = slice(head * width, (head + 1) * width)
                total = total + jnp.dot(
                    jnp.concatenate([mixed_in[0, t, :, cut] for t in far_targets], axis=1),
                    jnp.concatenate(
                        [wfull[0, t, cut, out_columns(n)] for t in far_targets], axis=0
                    ),
                    preferred_element_type=jnp.float32,
                )
            if not start:
                total = total + acc_s[:, out_columns(n)]
            if close:
                out_ref[:, out_columns(n)] = total.astype(jnp.bfloat16)
            else:
                acc_s[:, out_columns(n)] = total
            return carry

        lax.fori_loop(0, cuts, part, 0)

    def state_before(h):
        take_carry(last, h, offset)
        earlier = far_s[last, h, :, offset]
        if last > 0:
            window = window_s[h]
            earlier = mm(window[:, shift], earlier) + window[:, offset]
        return earlier.astype(jnp.bfloat16)

    def attend(targets, h, carried):
        cut = slice(h * width, (h + 1) * width)
        for target, i in [(target, i) for target in targets for i in range(per)]:
            t = target * per + i
            here = pl.ds(i * BLOCK, BLOCK)
            result = outb_ref[h, at(t), :] + mm(outa_ref[h, at(t), :], carried)
            result = result * lax.rsqrt(
                jnp.mean(result * result, axis=-1, keepdims=True) + TINY_NORM
            )
            gate = proj[DELTA_GATE, at(t), cut].astype(jnp.float32)
            mixed_out[0, target, here, cut] = (
                result * gain_ref[...] * jax.nn.silu(gate)
            ).astype(jnp.bfloat16)

    weights_beside().wait_recv()
    mixed_wait(heads, sibling)
    product([(1, me, mixed_out), (1, sibling, mixed_in)], start=True)
    carried = []
    for h in range(heads):
        carried.append(state_before(h))
        attend(far_targets, h, carried[h])
        for target in far_targets:
            mixed_copy(h, target).start()
    for h in range(heads):
        attend([sibling, me], h, carried[h])
    for h in range(heads):
        mixed_copy(h, sibling).start()
    for source in far_targets:
        mixed_wait(heads, source)
    for o in range(1, chips):
        weights_forward(o).wait_recv()
    product([(1, source, mixed_in) for source in far_targets])
    for h in range(heads):
        mixed_wait(h, sibling)
    product([(0, me, mixed_out), (0, sibling, mixed_in)])
    for h in range(heads):
        for source in far_targets:
            mixed_wait(h, source)
        product([], head=h, close=h + 1 == heads)

    for r in range(tiles):
        for o in range(1, chips):
            across(o, r).wait_send()
            forward(o, r).wait_send()
        beside(r).wait_send()
    weights_beside().wait_send()
    for o in range(1, chips):
        weights_across(o).wait_send()
        weights_forward(o).wait_send()
        for j in range(line):
            weights_pair(o, j, side).wait_send()
    for origin in range(line):
        for up in (True, False):
            @pl.when((origin <= spot) & (spot + 1 < line) if up else (origin >= spot) & (spot >= 1))
            def _(origin=origin, up=up):
                for o in range(1, chips):
                    weights_along(o, origin, up).wait_send()

    for i in range(last + 1):
        @pl.when(place + reaches[i] < sp)
        def _(i=i):
            for h in range(heads):
                carry_copy(i, h, offset).wait_send()
                if i < last:
                    carry_copy(i, h, shift).wait_send()

    @pl.when(place + 1 < sp)
    def _():
        halo_copy.wait_send()

    for step in range(1, tp):
        for which in range(3):
            ln_copy(step, which).wait_send()
    for kind in range(heads + 1):
        for target in sources:
            mixed_copy(kind, target).wait_send()


def layer(tokens, weights, w_beta, w_decay, decay_log, gain, taps, ln_gain, ln_shift, out_delta, out_conv):
    rows, part = tokens.shape
    width = gain.shape[1]
    features, held = weights[0].shape
    heads = held // width
    channels = taps.shape[1]
    depth, columns = out_delta.shape
    kernel = taps.shape[0]
    halo = (kernel - 1 + 31) // 32 * 32
    lanes = min(channels, 128)
    groups = channels // lanes
    sp, tp = lax.axis_size("sp"), lax.axis_size("tp")
    others = max(tp // 2 - 1, 1)
    line = sp // 2
    steps = 1
    while 2**steps < sp:
        steps += 1
    tiles = rows // BLOCK
    slot = rows // tp
    dma = pltpu.SemaphoreType.DMA
    pair = (heads, width, 2 * width)
    bf16, f32 = jnp.bfloat16, jnp.float32
    vmem = pltpu.VMEM
    return pl.pallas_call(
        functools.partial(layer_kernel, heads, width),
        out_shape=jax.ShapeDtypeStruct((slot, columns), bf16),
        in_specs=[pl.BlockSpec(memory_space=pltpu.HBM)] * 17,
        out_specs=pl.BlockSpec(memory_space=pltpu.VMEM),
        scratch_shapes=[
            vmem((rows, features), bf16),
            vmem((PROJECTIONS, features, held), bf16),
            vmem(w_beta.shape, bf16),
            vmem(w_decay.shape, bf16),
            vmem(decay_log.shape, f32),
            vmem(gain.shape, f32),
            vmem(taps.shape, bf16),
            vmem(ln_gain.shape, f32),
            vmem(ln_shift.shape, f32),
            vmem((BLOCK, features), bf16),
            vmem((1, BLOCK), f32),
            vmem(taps.shape, f32),
            vmem((PROJECTIONS, rows, held), bf16),
            vmem((rows, BLOCK), f32),
            vmem((2, tp, depth, columns), bf16),
            vmem((heads, tiles, 2 * BLOCK, width), bf16),
            vmem((heads, rows, width), f32),
            vmem((heads, rows, BLOCK), bf16),
            vmem((heads, tiles, width, BLOCK), bf16),
            vmem((heads, tiles, 8, BLOCK), f32),
            vmem(pair, f32),
            vmem((heads, rows, width), bf16),
            vmem((heads, rows, width), f32),
            vmem(pair, bf16),
            vmem((groups, halo + rows, lanes), f32),
            vmem((groups, rows, lanes), f32),
            vmem((halo, channels), bf16),
            vmem((halo, channels), bf16),
            vmem((tiles, 8, BLOCK), f32),
            vmem((tp - 1, tiles, 8, BLOCK), f32),
            vmem(pair, f32),
            vmem((steps,) + pair, bf16),
            vmem((steps,) + pair, bf16),
            vmem((2, tp, slot, channels), bf16),
            vmem((2, tp, slot, channels), bf16),
            vmem((slot, columns), f32),
            dma((tiles,)),
            dma((PROJECTIONS,)),
            dma((7,)),
            dma((2,)),
            dma((others, tiles)),
            dma((others, tiles)),
            dma((tiles,)),
            dma((tiles,)),
            dma((others, tiles)),
            dma((others, tiles)),
            dma((1,)),
            dma((1,)),
            dma((others,)),
            dma((others,)),
            dma((others, 2, line)),
            dma((others, line)),
            dma((others, line)),
            dma((others, line)),
            dma((others,)),
            dma((others,)),
            dma((steps, heads, 2)),
            dma((steps, heads, 2)),
            dma((1,)),
            dma((1,)),
            dma((tp - 1, 3)),
            dma((tp - 1, 3)),
            dma((heads + 1, tp)),
            dma((heads + 1, tp)),
        ],
        compiler_params=pltpu.CompilerParams(
            collective_id=0, has_side_effects=True, vmem_limit_bytes=46 * 1024 * 1024
        ),
        cost_estimate=pl.CostEstimate(
            flops=20_000_000_000, bytes_accessed=20_000_000, transcendentals=0
        ),
        name="layer",
    )(
        *(
            pltpu.with_memory_space_constraint(x, pltpu.HBM)
            for x in (
                tokens, *weights, w_beta, w_decay, decay_log, gain, taps, ln_gain, ln_shift,
                out_delta, out_conv,
            )
        )
    )


def local(
    tokens,
    w_query,
    w_key,
    w_value,
    w_delta_gate,
    w_glu_value,
    w_glu_gate,
    w_conv_gate,
    w_beta,
    w_decay,
    decay_log,
    head_gain,
    conv_taps,
    ln_gain,
    ln_shift,
    out_delta,
    out_conv,
):
    weights = (w_query, w_key, w_value, w_delta_gate, w_glu_value, w_glu_gate, w_conv_gate)
    return layer(
        tokens,
        weights,
        w_beta.T,
        w_decay.T,
        decay_log[None, :],
        head_gain[None, :],
        conv_taps,
        ln_gain[None, :],
        ln_shift[None, :],
        out_delta,
        out_conv,
    )


def solution(mesh):
    return jax.shard_map(
        local,
        mesh=mesh,
        in_specs=(
            P("sp", "tp"),
            P(None, "tp"),
            P(None, "tp"),
            P(None, "tp"),
            P(None, "tp"),
            P(None, "tp"),
            P(None, "tp"),
            P(None, "tp"),
            P(),
            P(),
            P(),
            P(),
            P(None, "tp"),
            P("tp"),
            P("tp"),
            P("tp", None),
            P("tp", None),
        ),
        out_specs=P(("sp", "tp"), None),
        check_vma=False,
    )
```

```python
import functools

import jax
import jax.numpy as jnp
from jax import lax
from jax.experimental import pallas as pl
from jax.experimental.pallas import tpu as pltpu
from jax.sharding import PartitionSpec as P

BLOCK = 128
PROJECTIONS = 7
QUERY, KEY, VALUE, DELTA_GATE, GLU_VALUE, GLU_GATE, CONV_GATE = range(PROJECTIONS)
OUT_CUT = 512
TINY_NORM = 1e-06
TINY_VAR = 1e-05
HIGHEST = lax.Precision.HIGHEST
MESH = pl.DeviceIdType.MESH


def nt(a, b):
    return lax.dot_general(a, b, (((1,), (1,)), ((), ())), preferred_element_type=jnp.float32)


def mm(a, b):
    return jnp.dot(
        a.astype(jnp.bfloat16), b.astype(jnp.bfloat16), preferred_element_type=jnp.float32
    )


def slice_shape(rows, columns, pieces):
    high = max(16, rows // pieces)
    across = pieces // (rows // high)
    return high, columns // across, across


def layer_kernel(
    heads, width,
    tok_hbm, wq_hbm, wk_hbm, wv_hbm, wdg_hbm, wgv_hbm, wgg_hbm, wcg_hbm,
    beta_hbm, decay_hbm, rate_hbm, gain_hbm, taps_hbm, ln_gain_hbm, ln_shift_hbm,
    out_delta_hbm, out_conv_hbm,
    out_ref,
    full, w_s, beta_s, decay_s, rate_s, gain_ref, taps_s, ln_gain_ref, ln_shift_ref,
    wg_s, rate_row, taps_ref, proj, gates_s, wfull,
    lhs_s, corr_s, score_s, wt_s, tail_s, state_ref, outa_ref, outb_ref, final_ref,
    padded, filtered, halo_out, halo_in, sums_out, sums_in, window_s, sent_s, far_s,
    mixed_out, mixed_in, acc_s,
    tok_sem, w_sem, small_sem, ow_sem,
    y_send, y_recv, own_send, own_recv, fwd_send, fwd_recv,
    wo_send, wo_recv, wy_send, wy_recv, wl_send, wl_recv, wx_send, wx_recv, wb_send, wb_recv,
    far_send, far_recv, halo_send, halo_recv, ln_send, ln_recv, mix_send, mix_recv,
):
    rows = full.shape[0]
    tp, me = lax.axis_size("tp"), lax.axis_index("tp")
    sp, place = lax.axis_size("sp"), lax.axis_index("sp")
    part = full.shape[1] // tp
    chips = tp // 2
    core = lax.rem(me, 2)
    chip = me // 2
    sibling = me + 1 - 2 * core
    tiles = rows // BLOCK
    halo = halo_in.shape[0]
    lanes = padded.shape[2]
    groups = padded.shape[0]
    kernel = taps_s.shape[0]
    line = sp // 2
    spot = place // 2
    side = lax.rem(place, 2)

    def at(t, count=1):
        return pl.ds(pl.multiple_of(t * BLOCK, BLOCK), count * BLOCK)

    def columns(owner):
        return pl.ds(pl.multiple_of(owner * part, part), part)

    token_loads = [
        pltpu.make_async_copy(
            tok_hbm.at[at(r), :], full.at[at(r), columns(me)], tok_sem.at[r]
        )
        for r in range(tiles)
    ]
    out_loads = [
        pltpu.make_async_copy(src, wfull.at[i, me], ow_sem.at[i])
        for i, src in enumerate((out_delta_hbm, out_conv_hbm))
    ]
    w_loads = [
        pltpu.make_async_copy(src, w_s.at[i], w_sem.at[i])
        for i, src in enumerate((wq_hbm, wk_hbm, wv_hbm, wdg_hbm, wgv_hbm, wgg_hbm, wcg_hbm))
    ]
    small_loads = [
        pltpu.make_async_copy(src, dst, small_sem.at[i])
        for i, (src, dst) in enumerate((
            (beta_hbm, beta_s), (decay_hbm, decay_s), (rate_hbm, rate_s), (gain_hbm, gain_ref),
            (taps_hbm, taps_s), (ln_gain_hbm, ln_gain_ref), (ln_shift_hbm, ln_shift_ref),
        ))
    ]
    for load in out_loads + token_loads + small_loads:
        load.start()

    reaches = [1]
    while 2 * reaches[-1] < sp:
        reaches.append(2 * reaches[-1])
    last = len(reaches) - 1
    barrier = pltpu.get_barrier_semaphore()
    expected = tp - 1
    for step in range(1, tp):
        pl.semaphore_signal(
            barrier, inc=1, device_id={"tp": lax.rem(me + step, tp)}, device_id_type=MESH
        )
    for step in reaches:
        ahead, behind = place + step < sp, place >= step

        @pl.when(ahead)
        def _(step=step):
            pl.semaphore_signal(
                barrier, inc=1, device_id={"sp": place + step}, device_id_type=MESH
            )

        @pl.when(behind)
        def _(step=step):
            pl.semaphore_signal(
                barrier, inc=1, device_id={"sp": place - step}, device_id_type=MESH
            )

        expected = expected + ahead.astype(jnp.int32) + behind.astype(jnp.int32)
    pl.semaphore_wait(barrier, expected)

    def to_tp(src, dst, send, recv, there):
        return pltpu.make_async_remote_copy(
            src_ref=src, dst_ref=dst, send_sem=send, recv_sem=recv,
            device_id={"tp": there}, device_id_type=MESH,
        )

    def to_sp(src, dst, send, recv, there):
        return pltpu.make_async_remote_copy(
            src_ref=src, dst_ref=dst, send_sem=send, recv_sem=recv,
            device_id={"sp": there}, device_id_type=MESH,
        )

    def far_peer(o):
        return lax.rem(chip + o, chips) * 2 + core

    def far_owner(o):
        return lax.rem(chip - o + chips, chips) * 2 + core

    def across(o, r):
        block = full.at[at(r), columns(me)]
        return to_tp(block, block, y_send.at[o - 1, r], y_recv.at[o - 1, r], far_peer(o))

    def beside(r):
        block = full.at[at(r), columns(me)]
        return to_tp(block, block, own_send.at[r], own_recv.at[r], sibling)

    def forward(o, r):
        block = full.at[at(r), columns(far_owner(o))]
        return to_tp(block, block, fwd_send.at[o - 1, r], fwd_recv.at[o - 1, r], sibling)

    high, broad, split = slice_shape(wfull.shape[2], wfull.shape[3], sp)

    def weight_slice(owner, index):
        top = pl.ds(pl.multiple_of(index // split * high, high), high)
        left = pl.ds(pl.multiple_of(lax.rem(index, split) * broad, broad), broad)
        return wfull.at[:, owner, top, left]

    def weights_beside():
        return to_tp(wfull.at[:, me], wfull.at[:, me], wo_send.at[0], wo_recv.at[0], sibling)

    def weights_across(o):
        piece = weight_slice(me, place)
        return to_tp(piece, piece, wy_send.at[o - 1], wy_recv.at[o - 1], far_peer(o))

    def weights_along(o, origin, up):
        piece = weight_slice(far_owner(o), 2 * origin + side)
        there = jnp.clip(spot + (1 if up else -1), 0, line - 1)
        return to_sp(
            piece, piece, wl_send.at[o - 1, int(up), origin], wl_recv.at[o - 1, origin],
            2 * there + side,
        )

    def weights_pair(o, j, parity):
        piece = weight_slice(far_owner(o), 2 * j + parity)
        return to_sp(
            piece, piece, wx_send.at[o - 1, j], wx_recv.at[o - 1, j], place + 1 - 2 * side
        )

    def weights_forward(o):
        block = wfull.at[:, far_owner(o)]
        return to_tp(block, block, wb_send.at[o - 1], wb_recv.at[o - 1], sibling)

    def pass_on(origin, up, arrived):
        for o in range(1, chips):
            if arrived:
                weights_along(o, origin, up).wait_recv()

            @pl.when(spot + 1 < line if up else spot >= 1)
            def _(o=o):
                weights_along(o, origin, up).start()

            if arrived:
                weights_pair(o, origin, side).start()

    def spread_weights():
        for o in range(1, chips):
            weights_across(o).wait_recv()
        pass_on(spot, True, False)
        pass_on(spot, False, False)
        for o in range(1, chips):
            weights_pair(o, spot, side).start()

    def relay_weights(step):
        @pl.when(spot >= step)
        def _():
            pass_on(jnp.maximum(spot - step, 0), True, True)

        @pl.when(spot + step < line)
        def _():
            pass_on(jnp.minimum(spot + step, line - 1), False, True)

    def collect_weights():
        for o in range(1, chips):
            for j in range(line):
                weights_pair(o, j, 1 - side).wait_recv()
            weights_forward(o).start()

    for load in out_loads:
        load.wait()
    for o in range(1, chips):
        weights_across(o).start()
    for r in range(tiles):
        token_loads[r].wait()
        for o in range(1, chips):
            across(o, r).start()
        beside(r).start()
    for load in w_loads:
        load.start()
    for load in small_loads:
        load.wait()

    first_head = me * heads
    total_heads = beta_s.shape[0]
    lane_row = lax.broadcasted_iota(jnp.int32, (1, BLOCK), 1)
    rate = jnp.zeros((1, BLOCK), jnp.float32)
    for h in range(total_heads):
        value = jnp.exp(jnp.broadcast_to(rate_s[:, h : h + 1], (1, BLOCK)))
        rate = jnp.where(lane_row == h - first_head + heads, value, rate)
    rate = jnp.where((lane_row >= heads) & (lane_row < 2 * heads), rate, 0.0)
    rate_row[...] = rate
    pick_row = lax.broadcasted_iota(jnp.int32, (BLOCK, total_heads), 0)
    pick_col = lax.broadcasted_iota(jnp.int32, (BLOCK, total_heads), 1)
    pick_beta = (pick_row < heads) & (pick_col == pick_row + first_head)
    pick_decay = (
        (pick_row >= heads) & (pick_row < 2 * heads) & (pick_col == pick_row - heads + first_head)
    )
    wg_s[...] = (
        mm(jnp.where(pick_beta, 1.0, 0.0), beta_s[...])
        + mm(jnp.where(pick_decay, 1.0, 0.0), decay_s[...])
    ).astype(jnp.bfloat16)
    taps_ref[...] = taps_s[...].astype(jnp.float32)

    def pass_tokens(first, count):
        for i in range(count):
            for o in range(1, chips):
                across(o, first + i).wait_recv()
                forward(o, first + i).start()

    def take_tokens(first, count):
        for i in range(count):
            beside(first + i).wait_recv()
            for o in range(1, chips):
                forward(o, first + i).wait_recv()

    def project_steps(first, count):
        size = count * BLOCK
        here = at(first, count)
        squares = jnp.zeros((size, 1), jnp.float32)
        for b in range(tp):
            piece = full[here, b * part : (b + 1) * part].astype(jnp.float32)
            squares = squares + jnp.sum(piece * piece, axis=1, keepdims=True)
        inv_rms = lax.rsqrt(squares / (part * tp) + TINY_NORM)
        raw = nt(full[here, :], wg_s[...]) * inv_rms
        lane = lax.broadcasted_iota(jnp.int32, raw.shape, 1)
        softplus = jnp.maximum(raw, 0.0) + jnp.log1p(jnp.exp(-jnp.abs(raw)))
        gates_s[here, :] = jnp.where(
            lane < heads, jax.nn.sigmoid(raw), -rate_row[...] * softplus
        )
        yield
        for i in range(PROJECTIONS):
            summed = jnp.dot(full[here, :], w_s[i], preferred_element_type=jnp.float32)
            proj[i, here, :] = (summed * inv_rms).astype(jnp.bfloat16)
            yield

    row_id = lax.broadcasted_iota(jnp.int32, (BLOCK, BLOCK), 0)
    col_id = lax.broadcasted_iota(jnp.int32, (BLOCK, BLOCK), 1)
    causal = row_id >= col_id
    strict = row_id > col_id
    differ = row_id ^ col_id
    eye = jnp.where(row_id == col_id, 1.0, 0.0)
    tril = jnp.where(causal, 1.0, 0.0)

    def prepare(c):
        here = at(c)
        gates = gates_s[here, :]
        sums = jnp.dot(tril, gates, precision=HIGHEST, preferred_element_type=jnp.float32)
        chains = []
        for h in range(heads):
            cut = slice(h * width, (h + 1) * width)
            k, q = proj[KEY, here, cut], proj[QUERY, here, cut]
            v = proj[VALUE, here, cut].astype(jnp.float32)
            kf, qf = k.astype(jnp.float32), q.astype(jnp.float32)
            ik = lax.rsqrt(jnp.sum(kf * kf, axis=-1, keepdims=True) + TINY_NORM)
            iq = lax.rsqrt(jnp.sum(qf * qf, axis=-1, keepdims=True) + TINY_NORM)
            iq = iq * width ** (-0.5)
            beta = gates[:, h : h + 1]
            log_sum = sums[:, heads + h : heads + h + 1]
            log_full = jnp.broadcast_to(log_sum, (BLOCK, BLOCK))
            spread = log_full - log_full.T
            damp = jnp.where(causal, jnp.exp(jnp.where(causal, spread, 0.0)), 0.0)
            damp = damp * jnp.broadcast_to(ik, (BLOCK, BLOCK)).T
            lower = jnp.where(strict, nt(k, k) * damp * (beta * ik), 0.0)
            score_s[h, here, :] = (nt(q, k) * damp * iq).astype(jnp.bfloat16)
            grow = jnp.exp(log_sum)
            right = jnp.concatenate([v * beta, kf * (beta * ik * grow)], axis=1)
            tail = log_full[BLOCK - 1 : BLOCK, :]
            weighted = kf * (ik * jnp.exp(tail[:, :1] - log_sum))
            wt_s[h, c] = weighted.T.astype(jnp.bfloat16)
            tail_s[h, c] = jnp.broadcast_to(jnp.exp(tail), (8, BLOCK))
            lhs_s[h, c, BLOCK:, :] = (qf * (iq * grow)).astype(jnp.bfloat16)
            chains.append([h, lower, right, eye - jnp.where(differ == 1, lower, 0.0)])
        return here, c, chains

    def blocks_steps(first, count):
        prepared = [prepare(first + i) for i in range(count)]
        yield
        size = 2
        while size < BLOCK:
            level = (differ >= size) & (differ < 2 * size)
            parts = [
                [mm(jnp.where(level, ch[1], 0.0), ch[3]) for ch in item[2]] for item in prepared
            ]
            yield
            for item, moves in zip(prepared, parts):
                for ch, moved in zip(item[2], moves):
                    ch[3] = ch[3] - mm(ch[3], moved)
            size *= 2
            yield
        for here, c, chains in prepared:
            for h, lower, right, inverse in chains:
                solved = mm(inverse, right)
                corr_s[h, here, :] = solved[:, :width]
                lhs_s[h, c, :BLOCK, :] = solved[:, width:].astype(jnp.bfloat16)

    def advance_steps(c):
        here = at(c)
        boths = [mm(lhs_s[h, c], state_ref[h]) for h in range(heads)]
        fresh = []
        for h in range(heads):
            first = boths[h][:BLOCK]
            fresh.append(
                jnp.concatenate(
                    [-first[:, :width], corr_s[h, here, :] - first[:, width:]], axis=1
                ).astype(jnp.bfloat16)
            )
        yield
        for h in range(heads):
            decay = tail_s[h, c][:1, :]
            decay = jnp.concatenate([decay, decay], axis=1)
            state_ref[h] = state_ref[h] * decay + mm(wt_s[h, c], fresh[h])
        for h in range(heads):
            out = boths[h][BLOCK:] + mm(score_s[h, here, :], fresh[h])
            outa_ref[h, here, :] = out[:, :width].astype(jnp.bfloat16)
            outb_ref[h, here, :] = out[:, width:]
        yield

    def in_turn(*steps):
        steps = list(steps)
        while steps:
            for step in list(steps):
                if next(step, step) is step:
                    steps.remove(step)

    def one_by_one(*steps):
        for step in steps:
            yield from step

    def unit(t):
        value = proj[GLU_VALUE, at(t), :].astype(jnp.float32)
        gate = proj[GLU_GATE, at(t), :].astype(jnp.float32)
        units = (value * jax.nn.sigmoid(gate)).astype(jnp.bfloat16)
        wide = units.astype(jnp.float32)
        for g in range(groups):
            padded[g, pl.ds(pl.multiple_of(t * BLOCK + halo, halo), BLOCK), :] = wide[
                :, g * lanes : (g + 1) * lanes
            ]
        return units

    def conv_steps(t):
        first = jnp.zeros((BLOCK, 1), jnp.float32)
        second = jnp.zeros((BLOCK, 1), jnp.float32)
        for g in range(groups):
            total = jnp.zeros((BLOCK, lanes), jnp.float32)
            for j in range(kernel):
                start = t * BLOCK + (halo - kernel + 1 + j)
                tap = taps_ref[j : j + 1, g * lanes : (g + 1) * lanes]
                total = total + padded[g, pl.ds(start, BLOCK), :] * tap
            filtered[g, at(t), :] = total
            first = first + jnp.sum(total, axis=1, keepdims=True)
            second = second + jnp.sum(total * total, axis=1, keepdims=True)
            yield
        lane = lax.broadcasted_iota(jnp.int32, (BLOCK, BLOCK), 1)
        sums_out[t] = jnp.where(lane == 0, first, jnp.where(lane == 1, second, 0.0)).T[:8, :]
        yield

    def conv(t):
        for step in conv_steps(t):
            pass

    for h in range(heads):
        state_ref[h] = jnp.concatenate([eye, jnp.zeros((width, width), jnp.float32)], axis=1)
    for load in w_loads:
        load.wait()
    def filter_tiles(first, count):
        for n in range(count):
            unit(first + n)

        def filter_tile(t, carry):
            @pl.when(t > 0)
            def _():
                conv(t)

            return carry

        lax.fori_loop(first, first + count, filter_tile, 0)

    tail = tiles - 4
    ln_parts = (pl.ds(2, tail), pl.ds(0, 2), pl.ds(tail + 2, 2))

    def ln_copy(step, which):
        cut = ln_parts[which]
        return to_tp(
            sums_out.at[cut], sums_in.at[step - 1, cut],
            ln_send.at[step - 1, which], ln_recv.at[step - 1, which], lax.rem(me + step, tp),
        )

    spread_weights()
    pass_tokens(0, 2)
    take_tokens(0, 2)
    in_turn(project_steps(0, 2))
    relay_weights(1)
    filter_tiles(0, 2)
    in_turn(blocks_steps(0, 2))
    in_turn(one_by_one(advance_steps(0), advance_steps(1)))
    pass_tokens(2, 2)

    def pair(i, carry):
        take_tokens(2 * i, 2)
        in_turn(project_steps(2 * i, 2))
        filter_tiles(2 * i, 2)
        pass_tokens(2 * i + 2, 2)
        relay_weights(i + 1)
        return carry

    lax.fori_loop(1, tail // 2, pair, 0)
    take_tokens(tail, 2)
    in_turn(project_steps(tail, 2))
    filter_tiles(tail, 2)
    for step in range(1, tp):
        ln_copy(step, 0).start()
    in_turn(blocks_steps(2, tail))
    pass_tokens(tail + 2, 2)
    relay_weights(tail // 2 + 1)
    take_tokens(tail + 2, 2)
    weights_beside().start()
    in_turn(project_steps(tail + 2, 2))
    for n in range(2):
        units = unit(tail + 2 + n)
    halo_out[...] = units[BLOCK - halo :, :]
    halo_copy = to_sp(
        halo_out, halo_in, halo_send.at[0], halo_recv.at[0], jnp.minimum(place + 1, sp - 1)
    )

    @pl.when(place + 1 < sp)
    def _():
        halo_copy.start()

    in_turn(
        blocks_steps(tail + 2, 2), one_by_one(*(advance_steps(c) for c in range(2, tail + 2)))
    )
    for step in range(tail // 2 + 2, line):
        relay_weights(step)
    in_turn(one_by_one(advance_steps(tail + 2), advance_steps(tail + 3)))
    final_ref[...] = state_ref[...].astype(jnp.bfloat16)

    shift, offset = slice(0, width), slice(width, 2 * width)

    def carry_copy(i, h, cut):
        source = final_ref if i == 0 else sent_s.at[i - 1]
        which = 0 if cut is shift else 1
        return to_sp(
            source.at[h, :, cut], far_s.at[i, h, :, cut],
            far_send.at[i, h, which], far_recv.at[i, h, which],
            jnp.minimum(place + reaches[i], sp - 1),
        )

    def send_carry(i, h, cut):
        if i == last and cut is shift:
            return

        @pl.when(place + reaches[i] < sp)
        def _():
            carry_copy(i, h, cut).start()

    def take_carry(i, h, cut):
        @pl.when(place >= reaches[i])
        def _():
            carry_copy(i, h, cut).wait_recv()

        @pl.when(place < reaches[i])
        def _():
            far_s[i, h, :, cut] = jnp.zeros((width, width), jnp.bfloat16)

    def exchange(i):
        own = final_ref if i == 0 else sent_s.at[i - 1]
        for h in range(heads):
            take_carry(i, h, offset)
            later = mm(own[h, :, shift], far_s[i, h, :, offset])
            later = later + own[h, :, offset].astype(jnp.float32)
            sent_s[i, h, :, offset] = later.astype(jnp.bfloat16)
            send_carry(i + 1, h, offset)
        for h in range(heads):
            take_carry(i, h, shift)
            sent_s[i, h, :, shift] = mm(own[h, :, shift], far_s[i, h, :, shift]).astype(
                jnp.bfloat16
            )
            send_carry(i + 1, h, shift)
        for h in range(heads):
            if i == 0:
                window_s[h] = far_s[i, h].astype(jnp.float32)
            else:
                window = window_s[h]
                moved = mm(window[:, shift], far_s[i, h])
                window_s[h] = jnp.concatenate(
                    [moved[:, shift], moved[:, offset] + window[:, offset]], axis=1
                )

    for h in range(heads):
        send_carry(0, h, offset)
    for h in range(heads):
        send_carry(0, h, shift)
    collect_weights()
    conv(tail + 2)
    conv(tail + 3)

    @pl.when(place >= 1)
    def _():
        halo_copy.wait_recv()

    @pl.when(place < 1)
    def _():
        halo_in[...] = jnp.zeros(halo_in.shape, jnp.bfloat16)

    before = halo_in[...].astype(jnp.float32)
    for g in range(groups):
        padded[g, :halo, :] = before[:, g * lanes : (g + 1) * lanes]
    conv(0)

    for step in range(1, tp):
        ln_copy(step, 1).start()
        ln_copy(step, 2).start()
    for step in range(1, tp):
        ln_copy(step, 0).wait_recv()
    channels = groups * lanes * tp
    per = tiles // tp

    def mixed_part(buffer, owner, kind):
        if kind == heads:
            return buffer.at[1, owner]
        return buffer.at[0, owner, :, kind * width : (kind + 1) * width]

    def mixed_copy(kind, there):
        return to_tp(
            mixed_part(mixed_out, there, kind), mixed_part(mixed_in, me, kind),
            mix_send.at[kind, there], mix_recv.at[kind, me], there,
        )

    def mixed_wait(kind, source):
        part_in = mixed_part(mixed_in, source, kind)
        to_tp(
            part_in, part_in, mix_send.at[kind, source], mix_recv.at[kind, source], source
        ).wait_recv()

    far_targets = [
        lax.rem(chip + o, chips) * 2 + lax.rem(core + c, 2) for o in range(1, chips) for c in (0, 1)
    ]

    def norm(targets):
        for target, i in [(target, i) for target in targets for i in range(per)]:
            t = target * per + i
            here = pl.ds(i * BLOCK, BLOCK)
            sums = sums_out[t]
            for step in range(1, tp):
                sums = sums + sums_in[step - 1, t]
            sums = jnp.concatenate([sums, jnp.zeros((BLOCK - 8, BLOCK), jnp.float32)], axis=0).T
            center = sums[:, 0:1] / channels
            variance = jnp.maximum(sums[:, 1:2] / channels - center * center, 0.0)
            scale = lax.rsqrt(variance + TINY_VAR)
            for g in range(groups):
                cut = slice(g * lanes, (g + 1) * lanes)
                normed = (filtered[g, at(t), :] - center) * scale
                normed = normed * ln_gain_ref[:, cut] + ln_shift_ref[:, cut]
                gate = proj[CONV_GATE, at(t), cut].astype(jnp.float32)
                mixed_out[1, target, here, cut] = (
                    jax.nn.silu(normed) * jax.nn.silu(gate)
                ).astype(jnp.bfloat16)

    early = [t for t in range(tp) if t * per >= 2 and (t + 1) * per <= tail + 2]

    def norm_far(target):
        @pl.when(target // 2 != chip)
        def _():
            norm([target])
            mixed_copy(heads, target).start()

    for target in early:
        norm_far(target)
    if last > 0:
        exchange(0)
    for step in range(1, tp):
        ln_copy(step, 1).wait_recv()
        ln_copy(step, 2).wait_recv()
    for target in range(tp):
        if target not in early:
            norm_far(target)
    norm([sibling])
    mixed_copy(heads, sibling).start()
    norm([me])
    for i in range(1, last):
        exchange(i)

    def out_columns(n):
        return pl.ds(pl.multiple_of(n * OUT_CUT, OUT_CUT), OUT_CUT)

    cuts = out_ref.shape[1] // OUT_CUT
    sources = [sibling] + far_targets

    def product(terms, head=None, start=False, close=False):
        def part(n, carry):
            total = jnp.zeros((out_ref.shape[0], OUT_CUT), jnp.float32)
            for kind, source, rows_ref in terms:
                total = total + jnp.dot(
                    rows_ref[kind, source], wfull[kind, source, :, out_columns(n)],
                    preferred_element_type=jnp.float32,
                )
            if head is not None:
                cut = slice(head * width, (head + 1) * width)
                total = total + jnp.dot(
                    jnp.concatenate([mixed_in[0, t, :, cut] for t in far_targets], axis=1),
                    jnp.concatenate(
                        [wfull[0, t, cut, out_columns(n)] for t in far_targets], axis=0
                    ),
                    preferred_element_type=jnp.float32,
                )
            if not start:
                total = total + acc_s[:, out_columns(n)]
            if close:
                out_ref[:, out_columns(n)] = total.astype(jnp.bfloat16)
            else:
                acc_s[:, out_columns(n)] = total
            return carry

        lax.fori_loop(0, cuts, part, 0, unroll=close)

    def state_before(h):
        take_carry(last, h, offset)
        earlier = far_s[last, h, :, offset]
        if last > 0:
            window = window_s[h]
            earlier = mm(window[:, shift], earlier) + window[:, offset]
        return earlier.astype(jnp.bfloat16)

    def attend(targets, h, carried):
        cut = slice(h * width, (h + 1) * width)
        for target, i in [(target, i) for target in targets for i in range(per)]:
            t = target * per + i
            here = pl.ds(i * BLOCK, BLOCK)
            result = outb_ref[h, at(t), :] + mm(outa_ref[h, at(t), :], carried)
            result = result * lax.rsqrt(
                jnp.mean(result * result, axis=-1, keepdims=True) + TINY_NORM
            )
            gate = proj[DELTA_GATE, at(t), cut].astype(jnp.float32)
            mixed_out[0, target, here, cut] = (
                result * gain_ref[...] * jax.nn.silu(gate)
            ).astype(jnp.bfloat16)

    carried = []
    for h in range(heads):
        carried.append(state_before(h))
        attend(far_targets, h, carried[h])
        for target in far_targets:
            mixed_copy(h, target).start()
    for h in range(heads):
        attend([sibling, me], h, carried[h])
    for h in range(heads):
        mixed_copy(h, sibling).start()
    weights_beside().wait_recv()
    mixed_wait(heads, sibling)
    product([(1, me, mixed_out), (1, sibling, mixed_in)], start=True)
    for source in far_targets:
        mixed_wait(heads, source)
    for o in range(1, chips):
        weights_forward(o).wait_recv()
    product([(1, source, mixed_in) for source in far_targets])
    for h in range(heads):
        mixed_wait(h, sibling)
    product([(0, me, mixed_out), (0, sibling, mixed_in)])
    for r in range(tiles):
        for o in range(1, chips):
            across(o, r).wait_send()
            forward(o, r).wait_send()
        beside(r).wait_send()
    weights_beside().wait_send()
    for o in range(1, chips):
        weights_across(o).wait_send()
        weights_forward(o).wait_send()
        for j in range(line):
            weights_pair(o, j, side).wait_send()
    for origin in range(line):
        for up in (True, False):
            @pl.when((origin <= spot) & (spot + 1 < line) if up else (origin >= spot) & (spot >= 1))
            def _(origin=origin, up=up):
                for o in range(1, chips):
                    weights_along(o, origin, up).wait_send()

    for i in range(last + 1):
        @pl.when(place + reaches[i] < sp)
        def _(i=i):
            for h in range(heads):
                carry_copy(i, h, offset).wait_send()
                if i < last:
                    carry_copy(i, h, shift).wait_send()

    @pl.when(place + 1 < sp)
    def _():
        halo_copy.wait_send()

    for step in range(1, tp):
        for which in range(3):
            ln_copy(step, which).wait_send()
    for h in range(heads):
        for source in far_targets:
            mixed_wait(h, source)
        product([], head=h, close=h + 1 == heads)

    for kind in range(heads + 1):
        for target in sources:
            mixed_copy(kind, target).wait_send()


def layer(tokens, weights, w_beta, w_decay, decay_log, gain, taps, ln_gain, ln_shift, out_delta, out_conv):
    rows, part = tokens.shape
    width = gain.shape[1]
    features, held = weights[0].shape
    heads = held // width
    channels = taps.shape[1]
    depth, columns = out_delta.shape
    kernel = taps.shape[0]
    halo = (kernel - 1 + 31) // 32 * 32
    lanes = min(channels, 128)
    groups = channels // lanes
    sp, tp = lax.axis_size("sp"), lax.axis_size("tp")
    others = max(tp // 2 - 1, 1)
    line = sp // 2
    steps = 1
    while 2**steps < sp:
        steps += 1
    tiles = rows // BLOCK
    slot = rows // tp
    dma = pltpu.SemaphoreType.DMA
    pair = (heads, width, 2 * width)
    bf16, f32 = jnp.bfloat16, jnp.float32
    vmem = pltpu.VMEM
    return pl.pallas_call(
        functools.partial(layer_kernel, heads, width),
        out_shape=jax.ShapeDtypeStruct((slot, columns), bf16),
        in_specs=[pl.BlockSpec(memory_space=pltpu.HBM)] * 17,
        out_specs=pl.BlockSpec(memory_space=pltpu.VMEM),
        scratch_shapes=[
            vmem((rows, features), bf16),
            vmem((PROJECTIONS, features, held), bf16),
            vmem(w_beta.shape, bf16),
            vmem(w_decay.shape, bf16),
            vmem(decay_log.shape, f32),
            vmem(gain.shape, f32),
            vmem(taps.shape, bf16),
            vmem(ln_gain.shape, f32),
            vmem(ln_shift.shape, f32),
            vmem((BLOCK, features), bf16),
            vmem((1, BLOCK), f32),
            vmem(taps.shape, f32),
            vmem((PROJECTIONS, rows, held), bf16),
            vmem((rows, BLOCK), f32),
            vmem((2, tp, depth, columns), bf16),
            vmem((heads, tiles, 2 * BLOCK, width), bf16),
            vmem((heads, rows, width), f32),
            vmem((heads, rows, BLOCK), bf16),
            vmem((heads, tiles, width, BLOCK), bf16),
            vmem((heads, tiles, 8, BLOCK), f32),
            vmem(pair, f32),
            vmem((heads, rows, width), bf16),
            vmem((heads, rows, width), f32),
            vmem(pair, bf16),
            vmem((groups, halo + rows, lanes), f32),
            vmem((groups, rows, lanes), f32),
            vmem((halo, channels), bf16),
            vmem((halo, channels), bf16),
            vmem((tiles, 8, BLOCK), f32),
            vmem((tp - 1, tiles, 8, BLOCK), f32),
            vmem(pair, f32),
            vmem((steps,) + pair, bf16),
            vmem((steps,) + pair, bf16),
            vmem((2, tp, slot, channels), bf16),
            vmem((2, tp, slot, channels), bf16),
            vmem((slot, columns), f32),
            dma((tiles,)),
            dma((PROJECTIONS,)),
            dma((7,)),
            dma((2,)),
            dma((others, tiles)),
            dma((others, tiles)),
            dma((tiles,)),
            dma((tiles,)),
            dma((others, tiles)),
            dma((others, tiles)),
            dma((1,)),
            dma((1,)),
            dma((others,)),
            dma((others,)),
            dma((others, 2, line)),
            dma((others, line)),
            dma((others, line)),
            dma((others, line)),
            dma((others,)),
            dma((others,)),
            dma((steps, heads, 2)),
            dma((steps, heads, 2)),
            dma((1,)),
            dma((1,)),
            dma((tp - 1, 3)),
            dma((tp - 1, 3)),
            dma((heads + 1, tp)),
            dma((heads + 1, tp)),
        ],
        compiler_params=pltpu.CompilerParams(
            collective_id=0, has_side_effects=True, vmem_limit_bytes=46 * 1024 * 1024
        ),
        cost_estimate=pl.CostEstimate(
            flops=20_000_000_000, bytes_accessed=20_000_000, transcendentals=0
        ),
        name="layer",
    )(
        *(
            pltpu.with_memory_space_constraint(x, pltpu.HBM)
            for x in (
                tokens, *weights, w_beta, w_decay, decay_log, gain, taps, ln_gain, ln_shift,
                out_delta, out_conv,
            )
        )
    )


def local(
    tokens,
    w_query,
    w_key,
    w_value,
    w_delta_gate,
    w_glu_value,
    w_glu_gate,
    w_conv_gate,
    w_beta,
    w_decay,
    decay_log,
    head_gain,
    conv_taps,
    ln_gain,
    ln_shift,
    out_delta,
    out_conv,
):
    weights = (w_query, w_key, w_value, w_delta_gate, w_glu_value, w_glu_gate, w_conv_gate)
    return layer(
        tokens,
        weights,
        w_beta.T,
        w_decay.T,
        decay_log[None, :],
        head_gain[None, :],
        conv_taps,
        ln_gain[None, :],
        ln_shift[None, :],
        out_delta,
        out_conv,
    )


def solution(mesh):
    return jax.shard_map(
        local,
        mesh=mesh,
        in_specs=(
            P("sp", "tp"),
            P(None, "tp"),
            P(None, "tp"),
            P(None, "tp"),
            P(None, "tp"),
            P(None, "tp"),
            P(None, "tp"),
            P(None, "tp"),
            P(),
            P(),
            P(),
            P(),
            P(None, "tp"),
            P("tp"),
            P("tp"),
            P("tp", None),
            P("tp", None),
        ),
        out_specs=P(("sp", "tp"), None),
        check_vma=False,
    )
```

```python
import functools

import jax
import jax.numpy as jnp
from jax import lax
from jax.experimental import pallas as pl
from jax.experimental.pallas import tpu as pltpu
from jax.sharding import PartitionSpec as P

BLOCK = 128
PROJECTIONS = 7
QUERY, KEY, VALUE, DELTA_GATE, GLU_VALUE, GLU_GATE, CONV_GATE = range(PROJECTIONS)
OUT_CUT = 512
TINY_NORM = 1e-06
TINY_VAR = 1e-05
HIGHEST = lax.Precision.HIGHEST
MESH = pl.DeviceIdType.MESH


def nt(a, b):
    return lax.dot_general(a, b, (((1,), (1,)), ((), ())), preferred_element_type=jnp.float32)


def mm(a, b):
    return jnp.dot(
        a.astype(jnp.bfloat16), b.astype(jnp.bfloat16), preferred_element_type=jnp.float32
    )


def slice_shape(rows, columns, pieces):
    high = max(16, rows // pieces)
    across = pieces // (rows // high)
    return high, columns // across, across


def layer_kernel(
    heads, width,
    tok_hbm, wq_hbm, wk_hbm, wv_hbm, wdg_hbm, wgv_hbm, wgg_hbm, wcg_hbm,
    beta_hbm, decay_hbm, rate_hbm, gain_hbm, taps_hbm, ln_gain_hbm, ln_shift_hbm,
    out_delta_hbm, out_conv_hbm,
    out_ref,
    full, w_s, beta_s, decay_s, rate_s, gain_ref, taps_s, ln_gain_ref, ln_shift_ref,
    wg_s, rate_row, taps_ref, proj, gates_s, wfull,
    lhs_s, corr_s, score_s, wt_s, tail_s, state_ref, outa_ref, outb_ref, final_ref,
    padded, filtered, halo_out, halo_in, sums_out, sums_in, window_s, sent_s, far_s,
    mixed_out, mixed_in, acc_s,
    tok_sem, w_sem, small_sem, ow_sem,
    y_send, y_recv, own_send, own_recv, fwd_send, fwd_recv,
    wo_send, wo_recv, wy_send, wy_recv, wl_send, wl_recv, wx_send, wx_recv, wb_send, wb_recv,
    far_send, far_recv, halo_send, halo_recv, ln_send, ln_recv, mix_send, mix_recv,
):
    rows = full.shape[0]
    tp, me = lax.axis_size("tp"), lax.axis_index("tp")
    sp, place = lax.axis_size("sp"), lax.axis_index("sp")
    part = full.shape[1] // tp
    chips = tp // 2
    core = lax.rem(me, 2)
    chip = me // 2
    sibling = me + 1 - 2 * core
    tiles = rows // BLOCK
    halo = halo_in.shape[0]
    lanes = padded.shape[2]
    groups = padded.shape[0]
    kernel = taps_s.shape[0]
    line = sp // 2
    spot = place // 2
    side = lax.rem(place, 2)

    def at(t, count=1):
        return pl.ds(pl.multiple_of(t * BLOCK, BLOCK), count * BLOCK)

    def columns(owner):
        return pl.ds(pl.multiple_of(owner * part, part), part)

    token_loads = [
        pltpu.make_async_copy(
            tok_hbm.at[at(r), :], full.at[at(r), columns(me)], tok_sem.at[r]
        )
        for r in range(tiles)
    ]
    out_loads = [
        pltpu.make_async_copy(src, wfull.at[i, me], ow_sem.at[i])
        for i, src in enumerate((out_delta_hbm, out_conv_hbm))
    ]
    w_loads = [
        pltpu.make_async_copy(src, w_s.at[i], w_sem.at[i])
        for i, src in enumerate((wq_hbm, wk_hbm, wv_hbm, wdg_hbm, wgv_hbm, wgg_hbm, wcg_hbm))
    ]
    small_loads = [
        pltpu.make_async_copy(src, dst, small_sem.at[i])
        for i, (src, dst) in enumerate((
            (beta_hbm, beta_s), (decay_hbm, decay_s), (rate_hbm, rate_s), (gain_hbm, gain_ref),
            (taps_hbm, taps_s), (ln_gain_hbm, ln_gain_ref), (ln_shift_hbm, ln_shift_ref),
        ))
    ]
    for load in out_loads + token_loads + small_loads:
        load.start()

    reaches = [1]
    while 2 * reaches[-1] < sp:
        reaches.append(2 * reaches[-1])
    last = len(reaches) - 1
    barrier = pltpu.get_barrier_semaphore()
    expected = tp - 1
    for step in range(1, tp):
        pl.semaphore_signal(
            barrier, inc=1, device_id={"tp": lax.rem(me + step, tp)}, device_id_type=MESH
        )
    for step in reaches:
        ahead, behind = place + step < sp, place >= step

        @pl.when(ahead)
        def _(step=step):
            pl.semaphore_signal(
                barrier, inc=1, device_id={"sp": place + step}, device_id_type=MESH
            )

        @pl.when(behind)
        def _(step=step):
            pl.semaphore_signal(
                barrier, inc=1, device_id={"sp": place - step}, device_id_type=MESH
            )

        expected = expected + ahead.astype(jnp.int32) + behind.astype(jnp.int32)
    pl.semaphore_wait(barrier, expected)

    def to_tp(src, dst, send, recv, there):
        return pltpu.make_async_remote_copy(
            src_ref=src, dst_ref=dst, send_sem=send, recv_sem=recv,
            device_id={"tp": there}, device_id_type=MESH,
        )

    def to_sp(src, dst, send, recv, there):
        return pltpu.make_async_remote_copy(
            src_ref=src, dst_ref=dst, send_sem=send, recv_sem=recv,
            device_id={"sp": there}, device_id_type=MESH,
        )

    def far_peer(o):
        return lax.rem(chip + o, chips) * 2 + core

    def far_owner(o):
        return lax.rem(chip - o + chips, chips) * 2 + core

    def across(o, r):
        block = full.at[at(r), columns(me)]
        return to_tp(block, block, y_send.at[o - 1, r], y_recv.at[o - 1, r], far_peer(o))

    def beside(r):
        block = full.at[at(r), columns(me)]
        return to_tp(block, block, own_send.at[r], own_recv.at[r], sibling)

    def forward(o, r):
        block = full.at[at(r), columns(far_owner(o))]
        return to_tp(block, block, fwd_send.at[o - 1, r], fwd_recv.at[o - 1, r], sibling)

    high, broad, split = slice_shape(wfull.shape[2], wfull.shape[3], sp)

    def weight_slice(owner, index):
        top = pl.ds(pl.multiple_of(index // split * high, high), high)
        left = pl.ds(pl.multiple_of(lax.rem(index, split) * broad, broad), broad)
        return wfull.at[:, owner, top, left]

    def weights_beside():
        return to_tp(wfull.at[:, me], wfull.at[:, me], wo_send.at[0], wo_recv.at[0], sibling)

    def weights_across(o):
        piece = weight_slice(me, place)
        return to_tp(piece, piece, wy_send.at[o - 1], wy_recv.at[o - 1], far_peer(o))

    def weights_along(o, origin, up):
        piece = weight_slice(far_owner(o), 2 * origin + side)
        there = jnp.clip(spot + (1 if up else -1), 0, line - 1)
        return to_sp(
            piece, piece, wl_send.at[o - 1, int(up), origin], wl_recv.at[o - 1, origin],
            2 * there + side,
        )

    def weights_pair(o, j, parity):
        piece = weight_slice(far_owner(o), 2 * j + parity)
        return to_sp(
            piece, piece, wx_send.at[o - 1, j], wx_recv.at[o - 1, j], place + 1 - 2 * side
        )

    def weights_forward(o):
        block = wfull.at[:, far_owner(o)]
        return to_tp(block, block, wb_send.at[o - 1], wb_recv.at[o - 1], sibling)

    def pass_on(origin, up, arrived):
        for o in range(1, chips):
            if arrived:
                weights_along(o, origin, up).wait_recv()

            @pl.when(spot + 1 < line if up else spot >= 1)
            def _(o=o):
                weights_along(o, origin, up).start()

            if arrived:
                weights_pair(o, origin, side).start()

    def spread_weights():
        for o in range(1, chips):
            weights_across(o).wait_recv()
        pass_on(spot, True, False)
        pass_on(spot, False, False)
        for o in range(1, chips):
            weights_pair(o, spot, side).start()

    def relay_weights(step):
        @pl.when(spot >= step)
        def _():
            pass_on(jnp.maximum(spot - step, 0), True, True)

        @pl.when(spot + step < line)
        def _():
            pass_on(jnp.minimum(spot + step, line - 1), False, True)

    def collect_weights():
        for o in range(1, chips):
            for j in range(line):
                weights_pair(o, j, 1 - side).wait_recv()
            weights_forward(o).start()

    for load in out_loads:
        load.wait()
    for o in range(1, chips):
        weights_across(o).start()
    for r in range(tiles):
        token_loads[r].wait()
        for o in range(1, chips):
            across(o, r).start()
        beside(r).start()
    for load in w_loads:
        load.start()
    for load in small_loads:
        load.wait()

    first_head = me * heads
    total_heads = beta_s.shape[0]
    lane_row = lax.broadcasted_iota(jnp.int32, (1, BLOCK), 1)
    rate = jnp.zeros((1, BLOCK), jnp.float32)
    for h in range(total_heads):
        value = jnp.exp(jnp.broadcast_to(rate_s[:, h : h + 1], (1, BLOCK)))
        rate = jnp.where(lane_row == h - first_head + heads, value, rate)
    rate = jnp.where((lane_row >= heads) & (lane_row < 2 * heads), rate, 0.0)
    rate_row[...] = rate
    pick_row = lax.broadcasted_iota(jnp.int32, (BLOCK, total_heads), 0)
    pick_col = lax.broadcasted_iota(jnp.int32, (BLOCK, total_heads), 1)
    pick_beta = (pick_row < heads) & (pick_col == pick_row + first_head)
    pick_decay = (
        (pick_row >= heads) & (pick_row < 2 * heads) & (pick_col == pick_row - heads + first_head)
    )
    wg_s[...] = (
        mm(jnp.where(pick_beta, 1.0, 0.0), beta_s[...])
        + mm(jnp.where(pick_decay, 1.0, 0.0), decay_s[...])
    ).astype(jnp.bfloat16)
    taps_ref[...] = taps_s[...].astype(jnp.float32)

    def pass_tokens(first, count):
        for i in range(count):
            for o in range(1, chips):
                across(o, first + i).wait_recv()
                forward(o, first + i).start()

    def take_tokens(first, count):
        for i in range(count):
            beside(first + i).wait_recv()
            for o in range(1, chips):
                forward(o, first + i).wait_recv()

    def project_steps(first, count):
        size = count * BLOCK
        here = at(first, count)
        squares = jnp.zeros((size, 1), jnp.float32)
        for b in range(tp):
            piece = full[here, b * part : (b + 1) * part].astype(jnp.float32)
            squares = squares + jnp.sum(piece * piece, axis=1, keepdims=True)
        inv_rms = lax.rsqrt(squares / (part * tp) + TINY_NORM)
        raw = nt(full[here, :], wg_s[...]) * inv_rms
        lane = lax.broadcasted_iota(jnp.int32, raw.shape, 1)
        softplus = jnp.maximum(raw, 0.0) + jnp.log1p(jnp.exp(-jnp.abs(raw)))
        gates_s[here, :] = jnp.where(
            lane < heads, jax.nn.sigmoid(raw), -rate_row[...] * softplus
        )
        yield
        for i in range(PROJECTIONS):
            summed = jnp.dot(full[here, :], w_s[i], preferred_element_type=jnp.float32)
            proj[i, here, :] = (summed * inv_rms).astype(jnp.bfloat16)
            yield

    row_id = lax.broadcasted_iota(jnp.int32, (BLOCK, BLOCK), 0)
    col_id = lax.broadcasted_iota(jnp.int32, (BLOCK, BLOCK), 1)
    causal = row_id >= col_id
    strict = row_id > col_id
    differ = row_id ^ col_id
    eye = jnp.where(row_id == col_id, 1.0, 0.0)
    tril = jnp.where(causal, 1.0, 0.0)

    def prepare(c):
        here = at(c)
        gates = gates_s[here, :]
        sums = jnp.dot(tril, gates, precision=HIGHEST, preferred_element_type=jnp.float32)
        chains = []
        for h in range(heads):
            cut = slice(h * width, (h + 1) * width)
            k, q = proj[KEY, here, cut], proj[QUERY, here, cut]
            v = proj[VALUE, here, cut].astype(jnp.float32)
            kf, qf = k.astype(jnp.float32), q.astype(jnp.float32)
            ik = lax.rsqrt(jnp.sum(kf * kf, axis=-1, keepdims=True) + TINY_NORM)
            iq = lax.rsqrt(jnp.sum(qf * qf, axis=-1, keepdims=True) + TINY_NORM)
            iq = iq * width ** (-0.5)
            beta = gates[:, h : h + 1]
            log_sum = sums[:, heads + h : heads + h + 1]
            log_full = jnp.broadcast_to(log_sum, (BLOCK, BLOCK))
            spread = log_full - log_full.T
            damp = jnp.where(causal, jnp.exp(jnp.where(causal, spread, 0.0)), 0.0)
            damp = damp * jnp.broadcast_to(ik, (BLOCK, BLOCK)).T
            lower = jnp.where(strict, nt(k, k) * damp * (beta * ik), 0.0)
            score_s[h, here, :] = (nt(q, k) * damp * iq).astype(jnp.bfloat16)
            grow = jnp.exp(log_sum)
            right = jnp.concatenate([v * beta, kf * (beta * ik * grow)], axis=1)
            tail = log_full[BLOCK - 1 : BLOCK, :]
            weighted = kf * (ik * jnp.exp(tail[:, :1] - log_sum))
            wt_s[h, c] = weighted.T.astype(jnp.bfloat16)
            tail_s[h, c] = jnp.broadcast_to(jnp.exp(tail), (8, BLOCK))
            lhs_s[h, c, BLOCK:, :] = (qf * (iq * grow)).astype(jnp.bfloat16)
            chains.append([h, lower, right, eye - jnp.where(differ == 1, lower, 0.0)])
        return here, c, chains

    def blocks_steps(first, count):
        prepared = [prepare(first + i) for i in range(count)]
        yield
        size = 2
        while size < BLOCK:
            level = (differ >= size) & (differ < 2 * size)
            parts = [
                [mm(jnp.where(level, ch[1], 0.0), ch[3]) for ch in item[2]] for item in prepared
            ]
            yield
            for item, moves in zip(prepared, parts):
                for ch, moved in zip(item[2], moves):
                    ch[3] = ch[3] - mm(ch[3], moved)
            size *= 2
            yield
        for here, c, chains in prepared:
            for h, lower, right, inverse in chains:
                solved = mm(inverse, right)
                corr_s[h, here, :] = solved[:, :width]
                lhs_s[h, c, :BLOCK, :] = solved[:, width:].astype(jnp.bfloat16)

    def advance_steps(c):
        here = at(c)
        boths = [mm(lhs_s[h, c], state_ref[h]) for h in range(heads)]
        fresh = []
        for h in range(heads):
            first = boths[h][:BLOCK]
            fresh.append(
                jnp.concatenate(
                    [-first[:, :width], corr_s[h, here, :] - first[:, width:]], axis=1
                ).astype(jnp.bfloat16)
            )
        yield
        for h in range(heads):
            decay = tail_s[h, c][:1, :]
            decay = jnp.concatenate([decay, decay], axis=1)
            state_ref[h] = state_ref[h] * decay + mm(wt_s[h, c], fresh[h])
        for h in range(heads):
            out = boths[h][BLOCK:] + mm(score_s[h, here, :], fresh[h])
            outa_ref[h, here, :] = out[:, :width].astype(jnp.bfloat16)
            outb_ref[h, here, :] = out[:, width:]
        yield

    def in_turn(*steps):
        steps = list(steps)
        while steps:
            for step in list(steps):
                if next(step, step) is step:
                    steps.remove(step)

    def one_by_one(*steps):
        for step in steps:
            yield from step

    def unit(t):
        value = proj[GLU_VALUE, at(t), :].astype(jnp.float32)
        gate = proj[GLU_GATE, at(t), :].astype(jnp.float32)
        units = (value * jax.nn.sigmoid(gate)).astype(jnp.bfloat16)
        wide = units.astype(jnp.float32)
        for g in range(groups):
            padded[g, pl.ds(pl.multiple_of(t * BLOCK + halo, halo), BLOCK), :] = wide[
                :, g * lanes : (g + 1) * lanes
            ]
        return units

    def conv_steps(t):
        first = jnp.zeros((BLOCK, 1), jnp.float32)
        second = jnp.zeros((BLOCK, 1), jnp.float32)
        for g in range(groups):
            total = jnp.zeros((BLOCK, lanes), jnp.float32)
            for j in range(kernel):
                start = t * BLOCK + (halo - kernel + 1 + j)
                tap = taps_ref[j : j + 1, g * lanes : (g + 1) * lanes]
                total = total + padded[g, pl.ds(start, BLOCK), :] * tap
            filtered[g, at(t), :] = total
            first = first + jnp.sum(total, axis=1, keepdims=True)
            second = second + jnp.sum(total * total, axis=1, keepdims=True)
            yield
        lane = lax.broadcasted_iota(jnp.int32, (BLOCK, BLOCK), 1)
        sums_out[t] = jnp.where(lane == 0, first, jnp.where(lane == 1, second, 0.0)).T[:8, :]
        yield

    def conv(t):
        for step in conv_steps(t):
            pass

    for h in range(heads):
        state_ref[h] = jnp.concatenate([eye, jnp.zeros((width, width), jnp.float32)], axis=1)
    for load in w_loads:
        load.wait()
    def filter_tiles(first, count):
        for n in range(count):
            unit(first + n)

        def filter_tile(t, carry):
            @pl.when(t > 0)
            def _():
                conv(t)

            return carry

        lax.fori_loop(first, first + count, filter_tile, 0)

    tail = tiles - 4
    ln_parts = (pl.ds(2, tail), pl.ds(0, 2), pl.ds(tail + 2, 2))

    def ln_copy(step, which):
        cut = ln_parts[which]
        return to_tp(
            sums_out.at[cut], sums_in.at[step - 1, cut],
            ln_send.at[step - 1, which], ln_recv.at[step - 1, which], lax.rem(me + step, tp),
        )

    spread_weights()
    pass_tokens(0, 2)
    take_tokens(0, 2)
    in_turn(project_steps(0, 2))
    relay_weights(1)
    filter_tiles(0, 2)
    in_turn(blocks_steps(0, 2))
    in_turn(one_by_one(advance_steps(0), advance_steps(1)))
    pass_tokens(2, 2)

    def pair(i, carry):
        take_tokens(2 * i, 2)
        in_turn(project_steps(2 * i, 2))
        filter_tiles(2 * i, 2)
        pass_tokens(2 * i + 2, 2)
        relay_weights(i + 1)
        return carry

    lax.fori_loop(1, tail // 2, pair, 0)
    take_tokens(tail, 2)
    in_turn(project_steps(tail, 2))
    filter_tiles(tail, 2)
    for step in range(1, tp):
        ln_copy(step, 0).start()
    in_turn(blocks_steps(2, tail))
    pass_tokens(tail + 2, 2)
    relay_weights(tail // 2 + 1)
    take_tokens(tail + 2, 2)
    weights_beside().start()
    in_turn(project_steps(tail + 2, 2))
    for n in range(2):
        units = unit(tail + 2 + n)
    halo_out[...] = units[BLOCK - halo :, :]
    halo_copy = to_sp(
        halo_out, halo_in, halo_send.at[0], halo_recv.at[0], jnp.minimum(place + 1, sp - 1)
    )

    @pl.when(place + 1 < sp)
    def _():
        halo_copy.start()

    in_turn(
        blocks_steps(tail + 2, 2), one_by_one(*(advance_steps(c) for c in range(2, tail + 2)))
    )
    for step in range(tail // 2 + 2, line):
        relay_weights(step)
    in_turn(one_by_one(advance_steps(tail + 2), advance_steps(tail + 3)))
    final_ref[...] = state_ref[...].astype(jnp.bfloat16)

    shift, offset = slice(0, width), slice(width, 2 * width)

    def carry_copy(i, h, cut):
        source = final_ref if i == 0 else sent_s.at[i - 1]
        which = 0 if cut is shift else 1
        return to_sp(
            source.at[h, :, cut], far_s.at[i, h, :, cut],
            far_send.at[i, h, which], far_recv.at[i, h, which],
            jnp.minimum(place + reaches[i], sp - 1),
        )

    def send_carry(i, h, cut):
        if i == last and cut is shift:
            return

        @pl.when(place + reaches[i] < sp)
        def _():
            carry_copy(i, h, cut).start()

    def take_carry(i, h, cut):
        @pl.when(place >= reaches[i])
        def _():
            carry_copy(i, h, cut).wait_recv()

        @pl.when(place < reaches[i])
        def _():
            far_s[i, h, :, cut] = jnp.zeros((width, width), jnp.bfloat16)

    def exchange(i):
        own = final_ref if i == 0 else sent_s.at[i - 1]
        for h in range(heads):
            take_carry(i, h, offset)
            later = mm(own[h, :, shift], far_s[i, h, :, offset])
            later = later + own[h, :, offset].astype(jnp.float32)
            sent_s[i, h, :, offset] = later.astype(jnp.bfloat16)
            send_carry(i + 1, h, offset)
        for h in range(heads):
            take_carry(i, h, shift)
            sent_s[i, h, :, shift] = mm(own[h, :, shift], far_s[i, h, :, shift]).astype(
                jnp.bfloat16
            )
            send_carry(i + 1, h, shift)
        for h in range(heads):
            if i == 0:
                window_s[h] = far_s[i, h].astype(jnp.float32)
            else:
                window = window_s[h]
                moved = mm(window[:, shift], far_s[i, h])
                window_s[h] = jnp.concatenate(
                    [moved[:, shift], moved[:, offset] + window[:, offset]], axis=1
                )

    for h in range(heads):
        send_carry(0, h, offset)
    for h in range(heads):
        send_carry(0, h, shift)
    collect_weights()
    conv(tail + 2)
    conv(tail + 3)

    @pl.when(place >= 1)
    def _():
        halo_copy.wait_recv()

    @pl.when(place < 1)
    def _():
        halo_in[...] = jnp.zeros(halo_in.shape, jnp.bfloat16)

    before = halo_in[...].astype(jnp.float32)
    for g in range(groups):
        padded[g, :halo, :] = before[:, g * lanes : (g + 1) * lanes]
    conv(0)

    for step in range(1, tp):
        ln_copy(step, 1).start()
        ln_copy(step, 2).start()
    for step in range(1, tp):
        ln_copy(step, 0).wait_recv()
    channels = groups * lanes * tp
    per = tiles // tp

    def mixed_part(buffer, owner, kind):
        if kind == heads:
            return buffer.at[1, owner]
        return buffer.at[0, owner, :, kind * width : (kind + 1) * width]

    def mixed_copy(kind, there):
        return to_tp(
            mixed_part(mixed_out, there, kind), mixed_part(mixed_in, me, kind),
            mix_send.at[kind, there], mix_recv.at[kind, me], there,
        )

    def mixed_wait(kind, source):
        part_in = mixed_part(mixed_in, source, kind)
        to_tp(
            part_in, part_in, mix_send.at[kind, source], mix_recv.at[kind, source], source
        ).wait_recv()

    far_targets = [
        lax.rem(chip + o, chips) * 2 + lax.rem(core + c, 2) for o in range(1, chips) for c in (0, 1)
    ]

    def norm(targets):
        for target, i in [(target, i) for target in targets for i in range(per)]:
            t = target * per + i
            here = pl.ds(i * BLOCK, BLOCK)
            sums = sums_out[t]
            for step in range(1, tp):
                sums = sums + sums_in[step - 1, t]
            sums = jnp.concatenate([sums, jnp.zeros((BLOCK - 8, BLOCK), jnp.float32)], axis=0).T
            center = sums[:, 0:1] / channels
            variance = jnp.maximum(sums[:, 1:2] / channels - center * center, 0.0)
            scale = lax.rsqrt(variance + TINY_VAR)
            for g in range(groups):
                cut = slice(g * lanes, (g + 1) * lanes)
                normed = (filtered[g, at(t), :] - center) * scale
                normed = normed * ln_gain_ref[:, cut] + ln_shift_ref[:, cut]
                gate = proj[CONV_GATE, at(t), cut].astype(jnp.float32)
                mixed_out[1, target, here, cut] = (
                    jax.nn.silu(normed) * jax.nn.silu(gate)
                ).astype(jnp.bfloat16)

    early = [t for t in range(tp) if t * per >= 2 and (t + 1) * per <= tail + 2]

    def norm_far(target):
        @pl.when(target // 2 != chip)
        def _():
            norm([target])
            mixed_copy(heads, target).start()

    for target in early:
        norm_far(target)
    if last > 0:
        exchange(0)
    for step in range(1, tp):
        ln_copy(step, 1).wait_recv()
        ln_copy(step, 2).wait_recv()
    for target in range(tp):
        if target not in early:
            norm_far(target)
    for i in range(1, last):
        exchange(i)
    norm([sibling])
    mixed_copy(heads, sibling).start()
    norm([me])

    def out_columns(n):
        return pl.ds(pl.multiple_of(n * OUT_CUT, OUT_CUT), OUT_CUT)

    cuts = out_ref.shape[1] // OUT_CUT
    sources = [sibling] + far_targets

    def product(terms, head=None, start=False, close=False):
        def part(n, carry):
            total = jnp.zeros((out_ref.shape[0], OUT_CUT), jnp.float32)
            for kind, source, rows_ref in terms:
                total = total + jnp.dot(
                    rows_ref[kind, source], wfull[kind, source, :, out_columns(n)],
                    preferred_element_type=jnp.float32,
                )
            if head is not None:
                cut = slice(head * width, (head + 1) * width)
                total = total + jnp.dot(
                    jnp.concatenate([mixed_in[0, t, :, cut] for t in far_targets], axis=1),
                    jnp.concatenate(
                        [wfull[0, t, cut, out_columns(n)] for t in far_targets], axis=0
                    ),
                    preferred_element_type=jnp.float32,
                )
            if not start:
                total = total + acc_s[:, out_columns(n)]
            if close:
                out_ref[:, out_columns(n)] = total.astype(jnp.bfloat16)
            else:
                acc_s[:, out_columns(n)] = total
            return carry

        lax.fori_loop(0, cuts, part, 0, unroll=True)

    def state_before(h):
        take_carry(last, h, offset)
        earlier = far_s[last, h, :, offset]
        if last > 0:
            window = window_s[h]
            earlier = mm(window[:, shift], earlier) + window[:, offset]
        return earlier.astype(jnp.bfloat16)

    def attend(targets, h, carried):
        cut = slice(h * width, (h + 1) * width)
        for target, i in [(target, i) for target in targets for i in range(per)]:
            t = target * per + i
            here = pl.ds(i * BLOCK, BLOCK)
            result = outb_ref[h, at(t), :] + mm(outa_ref[h, at(t), :], carried)
            result = result * lax.rsqrt(
                jnp.mean(result * result, axis=-1, keepdims=True) + TINY_NORM
            )
            gate = proj[DELTA_GATE, at(t), cut].astype(jnp.float32)
            mixed_out[0, target, here, cut] = (
                result * gain_ref[...] * jax.nn.silu(gate)
            ).astype(jnp.bfloat16)

    carried = []
    for h in range(heads):
        carried.append(state_before(h))
        attend(far_targets, h, carried[h])
        for target in far_targets:
            mixed_copy(h, target).start()
    for h in range(heads):
        attend([sibling, me], h, carried[h])
    for h in range(heads):
        mixed_copy(h, sibling).start()
    for source in far_targets:
        mixed_wait(heads, source)
    for o in range(1, chips):
        weights_forward(o).wait_recv()
    product([(1, source, mixed_in) for source in far_targets], start=True)
    weights_beside().wait_recv()
    mixed_wait(heads, sibling)
    product([(1, me, mixed_out), (1, sibling, mixed_in)])
    for h in range(heads):
        mixed_wait(h, sibling)
    product([(0, me, mixed_out), (0, sibling, mixed_in)])
    for r in range(tiles):
        for o in range(1, chips):
            across(o, r).wait_send()
            forward(o, r).wait_send()
        beside(r).wait_send()
    weights_beside().wait_send()
    for o in range(1, chips):
        weights_across(o).wait_send()
        weights_forward(o).wait_send()
        for j in range(line):
            weights_pair(o, j, side).wait_send()
    for origin in range(line):
        for up in (True, False):
            @pl.when((origin <= spot) & (spot + 1 < line) if up else (origin >= spot) & (spot >= 1))
            def _(origin=origin, up=up):
                for o in range(1, chips):
                    weights_along(o, origin, up).wait_send()

    for i in range(last + 1):
        @pl.when(place + reaches[i] < sp)
        def _(i=i):
            for h in range(heads):
                carry_copy(i, h, offset).wait_send()
                if i < last:
                    carry_copy(i, h, shift).wait_send()

    @pl.when(place + 1 < sp)
    def _():
        halo_copy.wait_send()

    for step in range(1, tp):
        for which in range(3):
            ln_copy(step, which).wait_send()
    for h in range(heads):
        for source in far_targets:
            mixed_wait(h, source)
        product([], head=h, close=h + 1 == heads)

    for kind in range(heads + 1):
        for target in sources:
            mixed_copy(kind, target).wait_send()


def layer(tokens, weights, w_beta, w_decay, decay_log, gain, taps, ln_gain, ln_shift, out_delta, out_conv):
    rows, part = tokens.shape
    width = gain.shape[1]
    features, held = weights[0].shape
    heads = held // width
    channels = taps.shape[1]
    depth, columns = out_delta.shape
    kernel = taps.shape[0]
    halo = (kernel - 1 + 31) // 32 * 32
    lanes = min(channels, 128)
    groups = channels // lanes
    sp, tp = lax.axis_size("sp"), lax.axis_size("tp")
    others = max(tp // 2 - 1, 1)
    line = sp // 2
    steps = 1
    while 2**steps < sp:
        steps += 1
    tiles = rows // BLOCK
    slot = rows // tp
    dma = pltpu.SemaphoreType.DMA
    pair = (heads, width, 2 * width)
    bf16, f32 = jnp.bfloat16, jnp.float32
    vmem = pltpu.VMEM
    return pl.pallas_call(
        functools.partial(layer_kernel, heads, width),
        out_shape=jax.ShapeDtypeStruct((slot, columns), bf16),
        in_specs=[pl.BlockSpec(memory_space=pltpu.HBM)] * 17,
        out_specs=pl.BlockSpec(memory_space=pltpu.VMEM),
        scratch_shapes=[
            vmem((rows, features), bf16),
            vmem((PROJECTIONS, features, held), bf16),
            vmem(w_beta.shape, bf16),
            vmem(w_decay.shape, bf16),
            vmem(decay_log.shape, f32),
            vmem(gain.shape, f32),
            vmem(taps.shape, bf16),
            vmem(ln_gain.shape, f32),
            vmem(ln_shift.shape, f32),
            vmem((BLOCK, features), bf16),
            vmem((1, BLOCK), f32),
            vmem(taps.shape, f32),
            vmem((PROJECTIONS, rows, held), bf16),
            vmem((rows, BLOCK), f32),
            vmem((2, tp, depth, columns), bf16),
            vmem((heads, tiles, 2 * BLOCK, width), bf16),
            vmem((heads, rows, width), f32),
            vmem((heads, rows, BLOCK), bf16),
            vmem((heads, tiles, width, BLOCK), bf16),
            vmem((heads, tiles, 8, BLOCK), f32),
            vmem(pair, f32),
            vmem((heads, rows, width), bf16),
            vmem((heads, rows, width), f32),
            vmem(pair, bf16),
            vmem((groups, halo + rows, lanes), f32),
            vmem((groups, rows, lanes), f32),
            vmem((halo, channels), bf16),
            vmem((halo, channels), bf16),
            vmem((tiles, 8, BLOCK), f32),
            vmem((tp - 1, tiles, 8, BLOCK), f32),
            vmem(pair, f32),
            vmem((steps,) + pair, bf16),
            vmem((steps,) + pair, bf16),
            vmem((2, tp, slot, channels), bf16),
            vmem((2, tp, slot, channels), bf16),
            vmem((slot, columns), f32),
            dma((tiles,)),
            dma((PROJECTIONS,)),
            dma((7,)),
            dma((2,)),
            dma((others, tiles)),
            dma((others, tiles)),
            dma((tiles,)),
            dma((tiles,)),
            dma((others, tiles)),
            dma((others, tiles)),
            dma((1,)),
            dma((1,)),
            dma((others,)),
            dma((others,)),
            dma((others, 2, line)),
            dma((others, line)),
            dma((others, line)),
            dma((others, line)),
            dma((others,)),
            dma((others,)),
            dma((steps, heads, 2)),
            dma((steps, heads, 2)),
            dma((1,)),
            dma((1,)),
            dma((tp - 1, 3)),
            dma((tp - 1, 3)),
            dma((heads + 1, tp)),
            dma((heads + 1, tp)),
        ],
        compiler_params=pltpu.CompilerParams(
            collective_id=0, has_side_effects=True, vmem_limit_bytes=46 * 1024 * 1024
        ),
        cost_estimate=pl.CostEstimate(
            flops=20_000_000_000, bytes_accessed=20_000_000, transcendentals=0
        ),
        name="layer",
    )(
        *(
            pltpu.with_memory_space_constraint(x, pltpu.HBM)
            for x in (
                tokens, *weights, w_beta, w_decay, decay_log, gain, taps, ln_gain, ln_shift,
                out_delta, out_conv,
            )
        )
    )


def local(
    tokens,
    w_query,
    w_key,
    w_value,
    w_delta_gate,
    w_glu_value,
    w_glu_gate,
    w_conv_gate,
    w_beta,
    w_decay,
    decay_log,
    head_gain,
    conv_taps,
    ln_gain,
    ln_shift,
    out_delta,
    out_conv,
):
    weights = (w_query, w_key, w_value, w_delta_gate, w_glu_value, w_glu_gate, w_conv_gate)
    return layer(
        tokens,
        weights,
        w_beta.T,
        w_decay.T,
        decay_log[None, :],
        head_gain[None, :],
        conv_taps,
        ln_gain[None, :],
        ln_shift[None, :],
        out_delta,
        out_conv,
    )


def solution(mesh):
    return jax.shard_map(
        local,
        mesh=mesh,
        in_specs=(
            P("sp", "tp"),
            P(None, "tp"),
            P(None, "tp"),
            P(None, "tp"),
            P(None, "tp"),
            P(None, "tp"),
            P(None, "tp"),
            P(None, "tp"),
            P(),
            P(),
            P(),
            P(),
            P(None, "tp"),
            P("tp"),
            P("tp"),
            P("tp", None),
            P("tp", None),
        ),
        out_specs=P(("sp", "tp"), None),
        check_vma=False,
    )
```
